512 devices in a mesh: sp: 64 (over z, y), tp: 8 (over x, core).
Axes of the slice: x: 4, y: 4, z: 16, core: 2. Of those that a mesh axis runs over, the one named last changes fastest.
Arguments:
- tokens: bfloat16 [16384, 2048], P('sp'), may hold values from -6 to 6
- input_norm_gain: float32 [2048], replicated, may hold values from 0.1 to 1.9
- mq_weight: bfloat16 [2048, 1024], P('sp', 'tp'), may hold values from -0.125 to 0.125
- mk_weight: bfloat16 [2048, 1024], P('sp', 'tp'), may hold values from -0.125 to 0.125
- mv_weight: bfloat16 [2048, 1024], P('sp', 'tp'), may hold values from -0.125 to 0.125
- mo_weight: bfloat16 [2048, 1024], P('sp', 'tp'), may hold values from -0.125 to 0.125
- gate_weight: bfloat16 [2048, 4, 8], P('sp', None, 'tp'), may hold values from -0.125 to 0.125
- gate_bias: float32 [4, 8], P(None, 'tp'), may hold values from -3 to 100
- decay_extra: float32 [2, 8, 16384], P(None, 'tp', 'sp'), may hold values from -1 to 0
- m_gain: float32 [1024], P('tp'), may hold values from 0.1 to 1.9
- aq_weight: bfloat16 [2048, 1024], P('sp', 'tp'), may hold values from -0.125 to 0.125
- ak_weight: bfloat16 [2048, 512], P('sp', 'tp'), may hold values from -8.838835 to 8.838835
- av_weight: bfloat16 [2048, 512], P('sp', 'tp'), may hold values from -0.125 to 0.125
- sink_logit: float32 [16], P('tp'), may hold values from 3 to 6
- out_m_weight: bfloat16 [1024, 2048], P('sp', 'tp'), may hold values from -0.1875 to 0.1875
- out_a_weight: bfloat16 [1024, 2048], P('sp', 'tp'), may hold values from -1.5 to 1.5
Outputs:
- mixed: bfloat16 [16384, 2048], P('sp', 'tp')
- log_total: float32 [16, 16384], P('tp', 'sp')
The draws below stay inside these ranges and needn't reach their ends.
All inputs are finite; a program needn't handle non-finite values.
Results may differ from the reference program's by a relative error of at most 0.015.
The reference program's roundings to bfloat16 on the way count: a program that leaves them out, or rounds other values in their place, can miss the bound.
Values may be sent and summed in bfloat16 or wider, within the bound.
A program may use at most 64 MiB of HBM per device.

```python
import math
import jax
import jax.numpy as jnp
from jax import lax

D = 2048
M_HEADS = 8
M_DIM = 128
W_HEADS = 16
KEY_VALUE_HEADS = 8
W_DIM = 64
WINDOW = 128
M_BLOCK = 64
TOK_DEV = 256
SEQUENCE_STEPS = 16384
M_WIDTH = 1024
W_WIDTH = 1024
KV_WIDTH = 512


def draw_gate_bias(key, part):
    keys_all = jax.random.split(jax.random.fold_in(key, 11), 4)
    inputs_gate = jax.random.truncated_normal(keys_all[0], -3.0, 3.0, (2, M_HEADS), jnp.float32)
    fast_share = 0.5
    fast_heads = jax.random.uniform(keys_all[1], (2, M_HEADS), jnp.float32) < fast_share
    fast_value = jax.random.uniform(keys_all[2], (2, M_HEADS), jnp.float32, 2.5, 3.5)
    slow_value = math.log(SEQUENCE_STEPS) + jax.random.uniform(keys_all[3], (2, M_HEADS), jnp.float32, 1.0, 2.0)
    forget_bias = jnp.where(fast_heads, fast_value, slow_value)
    return jnp.stack([inputs_gate[0], forget_bias[0], inputs_gate[1], forget_bias[1]])


def draw_decay_extra(key, part):
    keys_all = jax.random.split(jax.random.fold_in(key, 23), 3)
    block_total = SEQUENCE_STEPS // TOK_DEV
    rates = jnp.exp(jax.random.uniform(keys_all[0], (2, M_HEADS, block_total), jnp.float32, math.log(0.2), math.log(2.0))) / SEQUENCE_STEPS
    reference_speed = -jnp.repeat(rates, TOK_DEV, axis=2)
    spots = jax.random.randint(keys_all[1], (2, M_HEADS, 2), 0, SEQUENCE_STEPS)
    stacked_level = jnp.log(jax.random.uniform(keys_all[2], (2, M_HEADS, 2), jnp.float32, 0.5, 0.8))
    places = jnp.arange(SEQUENCE_STEPS, dtype=jnp.int32)
    equality_detected = places[None, None, :, None] == spots[:, :, None, :]
    clustered_spikes = jnp.sum(jnp.where(equality_detected, stacked_level[:, :, None, :], 0.0), axis=-1)
    return reference_speed + clustered_spikes


def draw_ak_weight(key, part):
    base_draw = jax.random.truncated_normal(jax.random.fold_in(key, 5), -4.0, 4.0, (D, KV_WIDTH), jnp.float32) * D ** (-0.5)
    return base_draw.astype(jnp.bfloat16)


def block_levels(key, extent, shards, smallest, high):
    gain = 1.0
    for dim, parts in shards:
        steps = jax.random.uniform(jax.random.fold_in(jax.random.fold_in(key, 6), dim), (parts,), jnp.float32, smallest / len(shards), high / len(shards))
        gain = gain * jnp.repeat(jnp.exp(steps), extent[dim] // parts).reshape((-1,) + (1,) * (len(extent) - 1 - dim))
    return gain


def centred(own_key, extent, deviation, bound, pieces=(), kind=jnp.bfloat16):
    loudness = block_levels(own_key, extent, pieces, -0.22, 0.18) if pieces else 1.0
    drawn = jax.random.normal(own_key, extent, jnp.float32) * deviation * loudness
    return jnp.minimum(jnp.maximum(drawn, -bound), bound).astype(kind)


def setup_inputs(seed: int = 0) -> dict:
    key_list = jax.random.split(jax.random.key(seed), 17)
    return {
        "tokens": centred(key_list[0], (SEQUENCE_STEPS, D), 1.0, 6.0, ((0, 64),)),
        "input_norm_gain": jnp.clip(1.0 + 0.18 * jax.random.normal(key_list[1], (D,), jnp.float32), 0.1, 1.9),
        "mq_weight": centred(key_list[2], (D, M_WIDTH), D ** -0.5, 0.125, ((0, 64), (1, 8))),
        "mk_weight": centred(key_list[3], (D, M_WIDTH), D ** -0.5, 0.125, ((0, 64), (1, 8))),
        "mv_weight": centred(key_list[4], (D, M_WIDTH), D ** -0.5, 0.125, ((0, 64), (1, 8))),
        "mo_weight": centred(key_list[5], (D, M_WIDTH), D ** -0.5, 0.125, ((0, 64), (1, 8))),
        "gate_weight": centred(key_list[6], (D, 4, M_HEADS), D ** -0.5, 0.125, ((0, 64), (2, 8))),
        "gate_bias": draw_gate_bias(jax.random.fold_in(key_list[16], 71), 0),
        "decay_extra": draw_decay_extra(jax.random.fold_in(key_list[16], 71), 0),
        "m_gain": jnp.clip(1.0 + 0.18 * jax.random.normal(key_list[9], (M_WIDTH,), jnp.float32), 0.1, 1.9),
        "aq_weight": centred(key_list[10], (D, W_WIDTH), D ** -0.5, 0.125, ((0, 64), (1, 8))),
        "ak_weight": draw_ak_weight(jax.random.fold_in(key_list[16], 71), 0),
        "av_weight": centred(key_list[12], (D, KV_WIDTH), D ** -0.5, 0.125, ((0, 64), (1, 8))),
        "sink_logit": jnp.clip(3.0 + 3.0 * jax.random.uniform(key_list[13], (W_HEADS,), jnp.float32) ** block_levels(key_list[13], (W_HEADS,), ((0, 8),), -0.2, 0.2), 3.0, 6.0),
        "out_m_weight": centred(key_list[14], (M_WIDTH, D), M_WIDTH ** -0.5, 0.1875, ((0, 64), (1, 8))),
        "out_a_weight": centred(key_list[15], (W_WIDTH, D), (W_WIDTH // 64) ** -0.5, 1.5, ((0, 64), (1, 8))),
    }


EPS = 1e-06
HIGHEST = lax.Precision.HIGHEST

def rms_rows(inputs, gain_vec):
    return inputs * lax.rsqrt(lax.optimization_barrier(jnp.mean(inputs * inputs, axis=-1, keepdims=True)) + EPS) * gain_vec

def stored(result):
    return lax.optimization_barrier(result.astype(jnp.bfloat16))

def block_pass(queries, key_vecs, value_vecs, in_gate, log_forget, start_state):
    head_count, length, head_width = queries.shape
    block_count = length // M_BLOCK

    def blocks(array_in):
        return jnp.moveaxis(array_in.reshape((head_count, block_count, M_BLOCK) + array_in.shape[2:]), 1, 0)
    lower_mask = jnp.tril(jnp.ones((M_BLOCK, M_BLOCK), dtype=bool))

    def advance(state_in, block_in):
        cell_mat, norm_vec, stab_max = state_in
        q_blk, k_blk, v_blk, i_blk, f_blk = block_in
        cum_log = jnp.cumsum(f_blk, axis=-1)
        seg_total = cum_log[:, -1]
        log_end = seg_total[:, None] - cum_log + i_blk
        max_next = jnp.maximum(seg_total + stab_max, lax.optimization_barrier(jnp.max(log_end, axis=-1)))
        w_end = jnp.exp(log_end - max_next[:, None])
        fade_old = jnp.exp(seg_total + stab_max - max_next)
        cell_next = fade_old[:, None, None] * cell_mat + jnp.einsum('hsv,hsk->hvk', w_end[:, :, None] * v_blk, k_blk, precision=HIGHEST)
        norm_next = fade_old[:, None] * norm_vec + jnp.einsum('hs,hsk->hk', w_end, k_blk, precision=HIGHEST)
        log_w = jnp.where(lower_mask, cum_log[:, :, None] - cum_log[:, None, :] + i_blk[:, None, :], -jnp.inf)
        log_inter = cum_log + stab_max[:, None]
        row_max = jnp.maximum(log_inter, lax.optimization_barrier(jnp.max(log_w, axis=-1)))
        w_intra = jnp.exp(log_w - row_max[:, :, None])
        w_inter = jnp.exp(log_inter - row_max)
        scores = jnp.einsum('htk,hsk->hts', q_blk, k_blk, precision=HIGHEST) * w_intra
        numerator = jnp.einsum('hts,hsv->htv', scores, v_blk, precision=HIGHEST) + w_inter[..., None] * jnp.einsum('hvk,htk->htv', cell_mat, q_blk, precision=HIGHEST)
        denominator = lax.optimization_barrier(jnp.sum(scores, axis=-1)) + w_inter * jnp.einsum('hk,htk->ht', norm_vec, q_blk, precision=HIGHEST)
        result_rows = numerator / jnp.maximum(jnp.abs(denominator), jnp.exp(-row_max))[..., None]
        return ((cell_next, norm_next, max_next), result_rows)
    final_state, outputs = lax.scan(advance, start_state, tuple((blocks(array_in) for array_in in (queries, key_vecs, value_vecs, in_gate, log_forget))))
    return (jnp.moveaxis(outputs, 0, 1).reshape(head_count, length, head_width), final_state)

def flip_tokens(array_in):
    return jnp.flip(array_in, axis=1)

def window_attention(a_query, a_key, a_value, sink_logit):
    length = a_query.shape[0]
    block_count = length // WINDOW
    groups = W_HEADS // KEY_VALUE_HEADS
    query_blocks = a_query.reshape(block_count, WINDOW, KEY_VALUE_HEADS, groups, W_DIM)
    border = ((WINDOW, WINDOW), (0, 0))
    key_pad = jnp.pad(a_key, border).reshape(length + 2 * WINDOW, KEY_VALUE_HEADS, W_DIM)
    value_pad = jnp.pad(a_value, border).reshape(length + 2 * WINDOW, KEY_VALUE_HEADS, W_DIM)
    query_off = jnp.arange(WINDOW, dtype=jnp.int32)
    key_off = jnp.arange(3 * WINDOW, dtype=jnp.int32) - WINDOW
    in_window = jnp.abs(query_off[:, None] - key_off[None, :]) <= WINDOW
    sink_col = sink_logit.reshape(KEY_VALUE_HEADS, groups, 1)

    def one_block(block_in):
        index, query_rows = block_in
        first = (index * WINDOW).astype(jnp.int32)
        key_rows = lax.dynamic_slice_in_dim(key_pad, first, 3 * WINDOW, 0).astype(jnp.float32)
        value_rows = lax.dynamic_slice_in_dim(value_pad, first, 3 * WINDOW, 0).astype(jnp.float32)
        key_place = first + key_off
        usable = in_window & ((key_place >= 0) & (key_place < length))[None, :]
        scores = jnp.einsum('qgrd,kgd->grqk', query_rows.astype(jnp.float32), key_rows) * W_DIM ** (-0.5)
        scores = jnp.where(usable, scores, -jnp.inf)
        peak_log = jnp.maximum(sink_col, lax.optimization_barrier(jnp.max(scores, axis=-1)))
        weights_exp = jnp.exp(scores - peak_log[..., None])
        weight_total_sum = jnp.exp(sink_col - peak_log) + lax.optimization_barrier(jnp.sum(weights_exp, axis=-1))
        rounded = weights_exp.astype(jnp.bfloat16).astype(jnp.float32)
        weighted = jnp.einsum('grqk,kgd->qgrd', rounded, value_rows)
        mixed_rows = (weighted / jnp.transpose(weight_total_sum, (2, 0, 1))[..., None]).astype(jnp.bfloat16)
        return (mixed_rows.reshape(WINDOW, W_HEADS * W_DIM), (peak_log + jnp.log(weight_total_sum)).reshape(W_HEADS, WINDOW))
    mixed_blocks, log_blocks = lax.map(one_block, (jnp.arange(block_count, dtype=jnp.int32), query_blocks))
    return (mixed_blocks.reshape(length, W_HEADS * W_DIM), jnp.transpose(log_blocks, (1, 0, 2)).reshape(W_HEADS, length))

def reference(tokens, input_norm_gain, mq_weight, mk_weight, mv_weight, mo_weight, gate_weight, gate_bias, decay_extra, m_gain, aq_weight, ak_weight, av_weight, sink_logit, out_m_weight, out_a_weight):
    length = tokens.shape[0]
    normed = rms_rows(tokens.astype(jnp.float32), input_norm_gain).astype(jnp.bfloat16)

    def project(weight_mat):
        return jnp.dot(normed, weight_mat, preferred_element_type=jnp.float32)
    m_query = stored(project(mq_weight))
    m_key = stored(project(mk_weight))
    m_value = stored(project(mv_weight))
    m_out = stored(project(mo_weight))
    gates = project(gate_weight.reshape(D, 4 * M_HEADS)).reshape(length, 4, M_HEADS) + gate_bias[None]

    def heads_first(matrix):
        return jnp.transpose(matrix.astype(jnp.float32).reshape(length, M_HEADS, M_DIM), (1, 0, 2))
    queries = heads_first(m_query)
    key_vecs = heads_first(m_key) * M_DIM ** (-0.5)
    value_vecs = heads_first(m_value)
    in_fwd = gates[:, 0, :].T
    forget_fwd = jax.nn.log_sigmoid(gates[:, 1, :].T) + decay_extra[0]
    in_bwd = gates[:, 2, :].T
    forget_bwd = jax.nn.log_sigmoid(gates[:, 3, :].T) + decay_extra[1]
    zero_state = (jnp.zeros((M_HEADS, M_DIM, M_DIM), jnp.float32), jnp.zeros((M_HEADS, M_DIM), jnp.float32), jnp.zeros((M_HEADS,), jnp.float32))
    hidden_fwd, forward_unused = block_pass(queries, key_vecs, value_vecs, in_fwd, forget_fwd, zero_state)
    hidden_bwd, unused_bwd = block_pass(flip_tokens(queries), flip_tokens(key_vecs), flip_tokens(value_vecs), flip_tokens(in_bwd), flip_tokens(forget_bwd), zero_state)
    cell_out = hidden_fwd + flip_tokens(hidden_bwd)
    gate_open = jax.nn.sigmoid(m_out.astype(jnp.float32)).reshape(length, M_HEADS, M_DIM)
    cell_rows = jnp.transpose(cell_out, (1, 0, 2)) * gate_open
    mixed_m = rms_rows(cell_rows, m_gain.reshape(M_HEADS, M_DIM)).astype(jnp.bfloat16).reshape(length, M_WIDTH)
    a_query = stored(project(aq_weight))
    a_key = stored(project(ak_weight))
    a_value = stored(project(av_weight))
    mixed_a, log_total = window_attention(a_query, a_key, a_value, sink_logit)
    mixed = jnp.dot(mixed_m, out_m_weight, preferred_element_type=jnp.float32) + jnp.dot(mixed_a, out_a_weight, preferred_element_type=jnp.float32)
    return (mixed.astype(jnp.bfloat16), log_total)
```

```python
import functools

import jax
import jax.numpy as jnp
from jax import lax
from jax.experimental import pallas as pl
from jax.experimental.pallas import tpu as pltpu
from jax.sharding import Mesh
from jax.sharding import PartitionSpec as P

M_DIM = 128
W_DIM = 64
WINDOW = 128
EPS = 1e-06
FLOOR_LOG = -1e30
NZ = 16
NY = 4
NT = 8
TOK = 256
D = 2048
SP = ("z", "y")
MESH = pl.DeviceIdType.MESH
VMEM = pltpu.VMEM
F32 = jnp.float32
BF16 = jnp.bfloat16


def mod(a, n):
    return lax.rem(a + n, n)


def remote(src, dst, ssem, rsem, **where):
    return pltpu.make_async_remote_copy(
        src_ref=src,
        dst_ref=dst,
        send_sem=ssem,
        recv_sem=rsem,
        device_id=where,
        device_id_type=MESH,
    )


def gather_body(a_ref, b_ref, ga, gb, ssem, az, ay, ah, bz, by, bh):
    z = lax.axis_index("z")
    y = lax.axis_index("y")
    zu, zd = mod(z + 1, NZ), mod(z - 1, NZ)
    yu, yd = mod(y + 1, NY), mod(y - 1, NY)
    yo = mod(y + 2, NY)
    me = z * NY + y
    barrier = pltpu.get_barrier_semaphore()
    pl.semaphore_signal(barrier, inc=1, device_id={"z": zu}, device_id_type=MESH)
    pl.semaphore_signal(barrier, inc=1, device_id={"z": zd}, device_id_type=MESH)
    pl.semaphore_signal(barrier, inc=1, device_id={"y": yu}, device_id_type=MESH)
    pl.semaphore_signal(barrier, inc=1, device_id={"y": yd}, device_id_type=MESH)
    pl.semaphore_wait(barrier, 4)

    sa, sb = ssem.at[0], ssem.at[1]

    def a_up(src, slot, s):
        return remote(src, ga.at[slot], sa, az.at[0, s], z=zu)

    def a_down(src, slot, s):
        return remote(src, ga.at[slot], sa, az.at[1, s], z=zd)

    def a_side(src, zz):
        slot = zz * NY + y
        remote(src, ga.at[slot], sa, ay.at[0, zz], y=yu).start()
        remote(src, ga.at[slot], sa, ay.at[1, zz], y=yd).start()

    def b_up(src, slot, s, j):
        return remote(src, gb.at[slot], sb, bz.at[0, s, j], z=zu)

    def b_down(src, slot, s, j):
        return remote(src, gb.at[slot], sb, bz.at[1, s, j], z=zd)

    remote(b_ref, gb.at[me], sb, by.at[0], y=yu).start()
    remote(b_ref, gb.at[me], sb, by.at[1], y=yd).start()
    a_up(a_ref, me, 1).start()
    a_down(a_ref, me, 1).start()
    b_up(b_ref, me, 1, y).start()
    b_down(b_ref, me, 1, y).start()
    a_side(a_ref, z)
    ga[me] = a_ref[...]
    gb[me] = b_ref[...]

    slot_d, slot_u, slot_o = z * NY + yd, z * NY + yu, z * NY + yo
    lo, hi = pl.ds(0, 16), pl.ds(16, 16)
    remote(b_ref, gb.at[slot_d], sb, by.at[0], y=yd).wait_recv()
    remote(gb.at[slot_d, lo], gb.at[slot_d, lo], sb, bh.at[0], y=yu).start()
    b_up(gb.at[slot_d], slot_d, 1, yd).start()
    b_down(gb.at[slot_d], slot_d, 1, yd).start()
    remote(b_ref, gb.at[slot_u], sb, by.at[1], y=yd).wait_recv()
    remote(gb.at[slot_u, hi], gb.at[slot_u, hi], sb, bh.at[1], y=yd).start()
    b_up(gb.at[slot_u], slot_u, 1, yu).start()
    b_down(gb.at[slot_u], slot_u, 1, yu).start()
    remote(gb.at[slot_o, lo], gb.at[slot_o, lo], sb, bh.at[0], y=yd).wait_recv()
    remote(gb.at[slot_o, hi], gb.at[slot_o, hi], sb, bh.at[1], y=yd).wait_recv()
    b_up(gb.at[slot_o], slot_o, 1, yo).start()
    b_down(gb.at[slot_o], slot_o, 1, yo).start()

    def side_forward(zz):
        sd, su = zz * NY + yd, zz * NY + yu
        remote(ga.at[sd], ga.at[sd], sa, ay.at[0, zz], y=yd).wait_recv()
        remote(ga.at[sd, lo], ga.at[sd, lo], sa, ah.at[0, zz], y=yu).start()
        remote(ga.at[su], ga.at[su], sa, ay.at[1, zz], y=yd).wait_recv()
        remote(ga.at[su, hi], ga.at[su, hi], sa, ah.at[1, zz], y=yd).start()

    half = NZ // 2

    def step(s, carry):
        z_lo, z_hi = mod(z - s, NZ), mod(z + s, NZ)
        slot = z_lo * NY + y
        a_up(ga.at[slot], slot, s).wait_recv()

        @pl.when(s < half)
        def _():
            a_up(ga.at[slot], slot, s + 1).start()

        a_side(ga.at[slot], z_lo)

        @pl.when(s < half)
        def _():
            slot2 = z_hi * NY + y
            a_down(ga.at[slot2], slot2, s).wait_recv()

            @pl.when(s < half - 1)
            def _():
                a_down(ga.at[slot2], slot2, s + 1).start()

            a_side(ga.at[slot2], z_hi)

        for j in (y, yd, yu, yo):
            sl = z_lo * NY + j
            b_up(gb.at[sl], sl, s, j).wait_recv()

            @pl.when(s < half)
            def _():
                b_up(gb.at[sl], sl, s + 1, j).start()

            @pl.when(s < half)
            def _():
                sl2 = z_hi * NY + j
                b_down(gb.at[sl2], sl2, s, j).wait_recv()

                @pl.when(s < half - 1)
                def _():
                    b_down(gb.at[sl2], sl2, s + 1, j).start()

        side_forward(mod(z - s + 1, NZ))

        @pl.when(s > 1)
        def _():
            side_forward(mod(z + s - 1, NZ))

        return carry

    lax.fori_loop(1, half + 1, step, 0)
    side_forward(mod(z + half, NZ))

    def finish(zz, carry):
        so = zz * NY + yo
        remote(ga.at[so, lo], ga.at[so, lo], sa, ah.at[0, zz], y=yd).wait_recv()
        remote(ga.at[so, hi], ga.at[so, hi], sa, ah.at[1, zz], y=yd).wait_recv()
        return carry

    lax.fori_loop(0, NZ, finish, 0)
    n = NZ * NY - 1
    every = pl.ds(0, n)
    remote(ga.at[every], ga.at[every], sa, az.at[0, 0], y=yd).wait_send()
    remote(gb.at[every], gb.at[every], sb, az.at[0, 0], y=yd).wait_send()


def gather_weights(a, b):
    n = NZ * NY
    dma = pltpu.SemaphoreType.DMA
    return pl.pallas_call(
        gather_body,
        name="gather_weights",
        out_shape=(
            jax.ShapeDtypeStruct((n,) + a.shape, BF16),
            jax.ShapeDtypeStruct((n,) + b.shape, BF16),
        ),
        in_specs=[pl.BlockSpec(memory_space=VMEM)] * 2,
        out_specs=[pl.BlockSpec(memory_space=VMEM)] * 2,
        scratch_shapes=[
            dma((2,)),
            dma((2, NZ // 2 + 1)),
            dma((2, NZ)),
            dma((2, NZ)),
            dma((2, NZ // 2 + 1, NY)),
            dma((2,)),
            dma((2,)),
        ],
        compiler_params=pltpu.CompilerParams(collective_id=0, has_side_effects=True),
    )(a, b)


def log1p_of(e):
    poly = e * (
        1.0
        + e * (-0.5 + e * (1 / 3 + e * (-0.25 + e * (0.2 + e * (-1 / 6 + e * (1 / 7))))))
    )
    return jnp.where(e < 0.0625, poly, jnp.log(1.0 + e))


def log_sigmoid(x):
    return jnp.minimum(x, 0.0) - log1p_of(jnp.exp(-jnp.abs(x)))


def split3(x):
    hi = x.astype(BF16).astype(F32)
    mid = (x - hi).astype(BF16).astype(F32)
    return hi, mid, x - hi - mid


def project_body(
    tok_ref, gain_ref, ga, gb, bias_ref, decay_ref, qkvo, aq, kv, pk, rows_ref, cols_ref, normed
):
    x = tok_ref[...].astype(F32)
    scale = lax.rsqrt(jnp.mean(x * x, axis=-1, keepdims=True) + EPS)
    normed[...] = (x * scale * gain_ref[...]).astype(BF16)
    gates = (
        jnp.dot(normed[...], gb[...].reshape(D, -1)[:, 0:128], preferred_element_type=F32)
        + bias_ref[...]
    )
    for c in range(3):
        out = jnp.dot(
            normed[...],
            ga[:, :, c * 256 : c * 256 + 256].reshape(D, 256),
            preferred_element_type=F32,
        ).astype(BF16)
        if c < 2:
            qkvo[:, c * 256 : c * 256 + 256] = out
        else:
            aq[...] = out[:, 0:128]
            kv[...] = out[:, 128:256]
    gt = jnp.transpose(gates)
    in_f, in_b = gt[0:1], gt[2:3]
    lf_f = log_sigmoid(gt[1:2]) + decay_ref[0:1]
    lf_b = log_sigmoid(gt[3:4]) + decay_ref[1:2]
    lane = lax.broadcasted_iota(jnp.int32, (1, TOK), 1)
    cum, rev = lf_f, lf_b
    k = 1
    while k < TOK:
        cum = cum + jnp.where(lane >= k, pltpu.roll(cum, k, 1), 0.0)
        rev = rev + jnp.where(lane < TOK - k, pltpu.roll(rev, TOK - k, 1), 0.0)
        k *= 2
    tot_f = jnp.max(jnp.where(lane == TOK - 1, cum, -jnp.inf), axis=1, keepdims=True)
    tot_b = jnp.max(jnp.where(lane == 0, rev, -jnp.inf), axis=1, keepdims=True)
    end_f = tot_f - cum + in_f
    end_b = tot_b - rev + in_b
    m_f = jnp.max(end_f, axis=1, keepdims=True)
    m_b = jnp.max(end_b, axis=1, keepdims=True)
    w_f, w_b = jnp.exp(end_f - m_f), jnp.exp(end_b - m_b)
    zero = jnp.zeros((2, TOK), F32)
    rows = jnp.concatenate([in_f, cum, in_b, rev, w_f, w_b, zero], axis=0)
    rows_ref[...] = rows
    cols = jnp.transpose(jnp.concatenate([rows, jnp.zeros((120, TOK), F32)], axis=0))
    cols_ref[...] = cols
    key = qkvo[:, 128:256]
    val = qkvo[:, 256:384].astype(F32)
    wide = (1, 128)
    tail = []
    mats = []
    norms = jnp.dot(rows.astype(BF16), key, preferred_element_type=F32)
    for c in (4, 5):
        wv = (cols[:, c : c + 1] * val).astype(BF16)
        mats.append(
            lax.dot_general(key, wv, (((0,), (0,)), ((), ())), preferred_element_type=F32)
        )
        tail.append(norms[c : c + 1])
    for v in (m_f, tot_f, m_b, tot_b):
        tail.extend(jnp.broadcast_to(p, wide) for p in split3(v))
    tail.append(jnp.zeros((2, 128), F32))
    last = jnp.concatenate(tail, axis=0).astype(BF16)
    for q in range(NY):
        pk[q, 0:32] = mats[0][q * 32 : q * 32 + 32].astype(BF16)
        pk[q, 32:64] = mats[1][q * 32 : q * 32 + 32].astype(BF16)
        pk[q, 64:80] = last


def project(tokens, gain, ga, gb, bias, decay):
    sds = jax.ShapeDtypeStruct
    return pl.pallas_call(
        project_body,
        name="project",
        out_shape=(
            sds((TOK, 512), BF16),
            sds((TOK, 128), BF16),
            sds((TOK, 128), BF16),
            sds((NY, 80, 128), BF16),
            sds((8, TOK), F32),
            sds((TOK, 128), F32),
        ),
        in_specs=[pl.BlockSpec(memory_space=VMEM)] * 6,
        out_specs=[pl.BlockSpec(memory_space=VMEM)] * 6,
        scratch_shapes=[pltpu.VMEM((TOK, D), BF16)],
    )(tokens, gain, ga, gb, bias, decay)


def step_state(state, piece):
    peak, mat, norm = state
    p_peak, p_decay, p_mat, p_norm = piece
    new = jnp.maximum(peak + p_decay, p_peak)
    old_s, new_s = jnp.exp(peak + p_decay - new), jnp.exp(p_peak - new)
    return new, mat * old_s + p_mat * new_s, norm * old_s + p_norm * new_s


def joined(tail, at):
    return tail[at : at + 1] + tail[at + 1 : at + 2] + tail[at + 2 : at + 3]


def scan_body(pk, kv, st, nm, halo, p1, zp, p2, p3, keep, s1, r1, s2, r2, s3, r3, sh, rh):
    z = lax.axis_index("z")
    y = lax.axis_index("y")
    me = z * NY + y
    nxt, prv = mod(me + 1, NZ * NY), mod(me - 1, NZ * NY)
    zn, yn = lax.div(nxt, NY), lax.rem(nxt, NY)
    zq, yq = lax.div(prv, NY), lax.rem(prv, NY)
    barrier = pltpu.get_barrier_semaphore()
    for d in range(1, NZ):
        pl.semaphore_signal(
            barrier, inc=1, device_id={"z": mod(z + d, NZ)}, device_id_type=MESH
        )
    for d in range(1, NY):
        pl.semaphore_signal(
            barrier, inc=1, device_id={"y": mod(y + d, NY)}, device_id_type=MESH
        )
    pl.semaphore_signal(barrier, inc=1, device_id={"z": zn, "y": yn}, device_id_type=MESH)
    pl.semaphore_signal(barrier, inc=1, device_id={"z": zq, "y": yq}, device_id_type=MESH)
    pl.semaphore_wait(barrier, NZ + NY)

    for d in (2, 1, 3):
        t = mod(y + d, NY)
        remote(pk.at[t], p1.at[y], s1.at[d - 1], r1.at[y], y=t).start()
    first, last = pl.ds(0, WINDOW), pl.ds(TOK - WINDOW, WINDOW)
    to_next = remote(kv.at[last], halo.at[0], sh.at[0], rh.at[0], z=zn, y=yn)
    to_prev = remote(kv.at[first], halo.at[1], sh.at[1], rh.at[1], z=zq, y=yq)
    to_next.start()
    to_prev.start()
    p1[y] = pk[y]
    for d in range(1, NY):
        t = mod(y + d, NY)
        remote(p1.at[t], p1.at[t], s1.at[0], r1.at[t], y=t).wait_recv()

    def local_piece(j, back):
        tail = p1[j, 64:80].astype(F32)
        if back:
            return joined(tail, 8), joined(tail, 11), p1[j, 32:64].astype(F32), tail[1:2]
        return joined(tail, 2), joined(tail, 5), p1[j, 0:32].astype(F32), tail[0:1]

    def empty():
        return (
            jnp.full((1, 128), FLOOR_LOG, F32),
            jnp.zeros((32, 128), F32),
            jnp.zeros((1, 128), F32),
        )

    for back in (0, 1):
        state, decay = empty(), jnp.zeros((1, 128), F32)
        for j in reversed(range(NY)) if back else range(NY):
            piece = local_piece(j, back)
            state = step_state(state, piece)
            decay = decay + piece[1]
        zp[back, 0:32] = state[1].astype(BF16)
        zp[back, 32:48] = jnp.concatenate(
            [state[2], *split3(state[0]), *split3(decay), jnp.zeros((9, 128), F32)], axis=0
        ).astype(BF16)
    for d in (8, 7, 9, 6, 10, 5, 11, 4, 12, 3, 13, 2, 14, 1, 15):
        t = mod(z + d, NZ)
        remote(
            zp.at[lax.div(z + d, NZ)], p2.at[z], s2.at[d - 1], r2.at[z], z=t
        ).start()
    for d in range(1, NZ):
        t = mod(z + d, NZ)
        remote(p2.at[t], p2.at[t], s2.at[0], r2.at[t], z=t).wait_recv()

    def far(i, state):
        tail = p2[i, 32:48].astype(F32)
        return step_state(
            state, (joined(tail, 1), joined(tail, 4), p2[i, 0:32].astype(F32), tail[0:1])
        )

    fwd = lax.fori_loop(0, z, far, empty())
    bwd = lax.fori_loop(0, NZ - 1 - z, lambda i, s: far(NZ - 1 - i, s), empty())
    for j in range(NY):
        p3[j, 0:32] = fwd[1].astype(BF16)
        keep[j, 0:1] = fwd[2]
        keep[j, 2:3] = fwd[0]
        fwd = step_state(fwd, local_piece(j, 0))
    for j in reversed(range(NY)):
        p3[j, 32:64] = bwd[1].astype(BF16)
        keep[j, 1:2] = bwd[2]
        keep[j, 3:4] = bwd[0]
        bwd = step_state(bwd, local_piece(j, 1))
    for d in (2, 1, 3):
        t = mod(y + d, NY)
        remote(p3.at[t], st.at[y], s3.at[d - 1], r3.at[y], y=t).start()
    st[y] = p3[y]
    nm[0:4] = keep[y, 0:4]
    nm[4:8] = jnp.zeros((4, 128), F32)
    for d in range(1, NY):
        t = mod(y + d, NY)
        remote(st.at[t], st.at[t], s3.at[0], r3.at[t], y=t).wait_recv()
    to_next.wait_recv()
    to_prev.wait_recv()
    for d in range(1, NY):
        remote(pk.at[0], p1.at[0], s1.at[d - 1], r1.at[0], y=y).wait_send()
        remote(p3.at[0], st.at[0], s3.at[d - 1], r3.at[0], y=y).wait_send()
    for d in range(1, NZ):
        remote(zp.at[0], p2.at[0], s2.at[d - 1], r2.at[0], z=z).wait_send()
    to_next.wait_send()
    to_prev.wait_send()


def scan_states(pk, kv):
    sds = jax.ShapeDtypeStruct
    dma = pltpu.SemaphoreType.DMA
    return pl.pallas_call(
        scan_body,
        name="scan_states",
        out_shape=(
            sds((NY, 64, 128), BF16),
            sds((8, 128), F32),
            sds((2, WINDOW, 128), BF16),
        ),
        in_specs=[pl.BlockSpec(memory_space=VMEM)] * 2,
        out_specs=[pl.BlockSpec(memory_space=VMEM)] * 3,
        scratch_shapes=[
            pltpu.VMEM((NY, 80, 128), BF16),
            pltpu.VMEM((2, 48, 128), BF16),
            pltpu.VMEM((NZ, 48, 128), BF16),
            pltpu.VMEM((NY, 64, 128), BF16),
            pltpu.VMEM((NY, 8, 128), F32),
            dma((NY - 1,)),
            dma((NY,)),
            dma((NZ - 1,)),
            dma((NZ,)),
            dma((NY - 1,)),
            dma((NY,)),
            dma((2,)),
            dma((2,)),
        ],
        compiler_params=pltpu.CompilerParams(collective_id=1, has_side_effects=True),
    )(pk, kv)


def mix_body(qkvo, aq, kv, rows_ref, cols_ref, st, nm, halo, mgain, sink, mix, logs, win):
    z = lax.axis_index("z")
    y = lax.axis_index("y")
    me = z * NY + y
    query, key, value = qkvo[:, 0:128], qkvo[:, 128:256], qkvo[:, 256:384]
    scale = M_DIM**-0.5
    across = (((1,), (1,)), ((), ()))
    dots = lax.dot_general(query, key, across, preferred_element_type=F32) * scale
    ti = lax.broadcasted_iota(jnp.int32, (TOK, TOK), 0)
    si = lax.broadcasted_iota(jnp.int32, (TOK, TOK), 1)
    qf = query.astype(F32) * scale
    total = None
    for back in (0, 1):
        ins = rows_ref[2 * back : 2 * back + 1]
        cum = rows_ref[2 * back + 1 : 2 * back + 2]
        cum_t = cols_ref[:, 2 * back + 1 : 2 * back + 2]
        keep = (si >= ti) if back else (si <= ti)
        log_w = jnp.where(keep, cum_t + (ins - cum), -jnp.inf)
        inter = cum_t + nm[2 + back : 3 + back, 0:1]
        top = jnp.maximum(inter, jnp.max(log_w, axis=1, keepdims=True))
        scores = dots * jnp.exp(log_w - top)
        w_inter = jnp.exp(inter - top)
        mat = st[:, 32 * back : 32 * back + 32].reshape(128, 128)
        numer = jnp.dot(scores.astype(BF16), value, preferred_element_type=F32) + (
            w_inter * scale
        ) * jnp.dot(query, mat, preferred_element_type=F32)
        denom = jnp.sum(scores, axis=1, keepdims=True) + w_inter * jnp.sum(
            qf * nm[back : back + 1], axis=1, keepdims=True
        )
        part = numer / jnp.maximum(jnp.abs(denom), jnp.exp(-top))
        total = part if total is None else total + part
    gate = qkvo[:, 384:512].astype(F32)
    u = total / (1.0 + jnp.exp(-gate))
    norm = lax.rsqrt(jnp.mean(u * u, axis=1, keepdims=True) + EPS)
    mix[:, 0:128] = (u * norm * mgain[...]).astype(BF16)

    win[0:WINDOW] = halo[0]
    win[WINDOW : WINDOW + TOK] = kv[...]
    win[WINDOW + TOK :] = halo[1]
    lane = lax.broadcasted_iota(jnp.int32, (WINDOW, 128), 1)
    two = lax.broadcasted_iota(jnp.int32, (2 * WINDOW, 3 * WINDOW), 0)
    col = lax.broadcasted_iota(jnp.int32, (2 * WINDOW, 3 * WINDOW), 1)
    head = two >= WINDOW
    off = col - jnp.where(head, two - WINDOW, two)
    in_window = (off >= 0) & (off <= 2 * WINDOW)
    head_row = lax.broadcasted_iota(jnp.int32, (2 * WINDOW, 1), 0) >= WINDOW
    sink_col = jnp.where(head_row, sink[0:1, 1:2], sink[0:1, 0:1])
    for b in range(2):
        qb = aq[b * WINDOW : b * WINDOW + WINDOW].astype(F32)
        q0 = jnp.where(lane < W_DIM, qb, 0.0)
        q1 = jnp.where(lane < W_DIM, pltpu.roll(qb, W_DIM, 1), 0.0)
        qq = jnp.concatenate([q0, q1], axis=0).astype(BF16)
        keys = win[b * WINDOW : b * WINDOW + 3 * WINDOW]
        scores = lax.dot_general(qq, keys, across, preferred_element_type=F32) * W_DIM**-0.5
        place = me * TOK + (b - 1) * WINDOW + col
        usable = in_window & (place >= 0) & (place < NZ * NY * TOK)
        scores = jnp.where(usable, scores, -jnp.inf)
        peak = jnp.maximum(sink_col, jnp.max(scores, axis=1, keepdims=True))
        weights = jnp.exp(scores - peak)
        tot = jnp.exp(sink_col - peak) + jnp.sum(weights, axis=1, keepdims=True)
        out = jnp.dot(weights.astype(BF16), keys, preferred_element_type=F32) / tot
        o0 = pltpu.roll(out[0:WINDOW], W_DIM, 1)
        o1 = out[WINDOW:]
        mix[b * WINDOW : b * WINDOW + WINDOW, 128:256] = jnp.where(
            lane < W_DIM, o0, o1
        ).astype(BF16)
        logt = jnp.transpose(jnp.broadcast_to(peak + jnp.log(tot), (2 * WINDOW, 128)))
        logs[0:1, b * WINDOW : b * WINDOW + WINDOW] = logt[0:1, 0:WINDOW]
        logs[1:2, b * WINDOW : b * WINDOW + WINDOW] = logt[0:1, WINDOW:]


def mix_local(*args):
    sds = jax.ShapeDtypeStruct
    return pl.pallas_call(
        mix_body,
        name="mix",
        out_shape=(sds((TOK, 256), BF16), sds((2, TOK), F32)),
        in_specs=[pl.BlockSpec(memory_space=VMEM)] * len(args),
        out_specs=[pl.BlockSpec(memory_space=VMEM)] * 2,
        scratch_shapes=[pltpu.VMEM((TOK + 2 * WINDOW, 128), BF16)],
    )(*args)


def heads_body(mix, full, ssem, rx, rh, rc):
    t = lax.axis_index("tp")
    x, c = lax.div(t, 2), lax.rem(t, 2)
    o = 1 - c
    xu, xd, xo = mod(x + 1, 4), mod(x - 1, 4), mod(x + 2, 4)
    partner, up, down = 2 * x + o, 2 * xu + c, 2 * xd + c
    far = 2 * xo + c
    barrier = pltpu.get_barrier_semaphore()
    for p in (partner, up, down):
        pl.semaphore_signal(barrier, inc=1, device_id={"tp": p}, device_id_type=MESH)
    pl.semaphore_wait(barrier, 3)
    lo, hi = pl.ds(0, TOK // 2), pl.ds(TOK // 2, TOK // 2)
    remote(mix, full.at[t], ssem, rx.at[0], tp=up).start()
    remote(mix, full.at[t], ssem, rx.at[1], tp=down).start()
    remote(mix, full.at[t], ssem, rc.at[0], tp=partner).start()
    full[t] = mix[...]
    remote(mix, full.at[down], ssem, rx.at[0], tp=up).wait_recv()
    remote(full.at[down, lo], full.at[down, lo], ssem, rh.at[0], tp=up).start()
    remote(full.at[down], full.at[down], ssem, rc.at[1], tp=partner).start()
    remote(mix, full.at[up], ssem, rx.at[1], tp=up).wait_recv()
    remote(full.at[up, hi], full.at[up, hi], ssem, rh.at[1], tp=down).start()
    remote(full.at[up], full.at[up], ssem, rc.at[2], tp=partner).start()
    remote(full.at[far, lo], full.at[far, lo], ssem, rh.at[0], tp=up).wait_recv()
    remote(full.at[far, lo], full.at[far, lo], ssem, rc.at[3], tp=partner).start()
    remote(full.at[far, hi], full.at[far, hi], ssem, rh.at[1], tp=up).wait_recv()
    remote(full.at[far, hi], full.at[far, hi], ssem, rc.at[4], tp=partner).start()
    remote(mix, full.at[partner], ssem, rc.at[0], tp=partner).wait_recv()
    remote(mix, full.at[2 * xd + o], ssem, rc.at[1], tp=partner).wait_recv()
    remote(mix, full.at[2 * xu + o], ssem, rc.at[2], tp=partner).wait_recv()
    other = 2 * xo + o
    remote(full.at[other, lo], full.at[other, lo], ssem, rc.at[3], tp=partner).wait_recv()
    remote(full.at[other, hi], full.at[other, hi], ssem, rc.at[4], tp=partner).wait_recv()
    every = pl.ds(0, NT - 1)
    remote(full.at[every], full.at[every], ssem, rc.at[0], tp=partner).wait_send()


def gather_heads(mix):
    dma = pltpu.SemaphoreType.DMA
    return pl.pallas_call(
        heads_body,
        name="gather_heads",
        out_shape=jax.ShapeDtypeStruct((NT, TOK, 256), BF16),
        in_specs=[pl.BlockSpec(memory_space=VMEM)],
        out_specs=pl.BlockSpec(memory_space=VMEM),
        scratch_shapes=[dma, dma((2,)), dma((2,)), dma((5,))],
        compiler_params=pltpu.CompilerParams(collective_id=2, has_side_effects=True),
    )(mix)


def last_body(full, gb, out):
    acc = None
    for t in range(NT):
        for part in (0, 1):
            w = gb[8 * t : 8 * t + 8, 16 * part : 16 * part + 16, 128:384].reshape(128, 256)
            term = jnp.dot(
                full[t, :, 128 * part : 128 * part + 128], w, preferred_element_type=F32
            )
            acc = term if acc is None else acc + term
    out[...] = acc.astype(BF16)


def project_out(full, gb):
    return pl.pallas_call(
        last_body,
        name="project_out",
        out_shape=jax.ShapeDtypeStruct((TOK, 256), BF16),
        in_specs=[pl.BlockSpec(memory_space=VMEM)] * 2,
        out_specs=pl.BlockSpec(memory_space=VMEM),
    )(full, gb)


def on_device(
    tokens,
    input_norm_gain,
    mq_weight,
    mk_weight,
    mv_weight,
    mo_weight,
    gate_weight,
    gate_bias,
    decay_extra,
    m_gain,
    aq_weight,
    ak_weight,
    av_weight,
    sink_logit,
    out_m_weight,
    out_a_weight,
):
    a = jnp.concatenate(
        [mq_weight, mk_weight, mv_weight, mo_weight, aq_weight, ak_weight, av_weight], axis=1
    )
    gate = jnp.pad(gate_weight[:, :, 0], ((0, 0), (0, 124)))
    b = jnp.concatenate(
        [gate, jnp.concatenate([out_m_weight, out_a_weight], axis=0)], axis=1
    )
    ga, gb = gather_weights(a, b)
    bias = jnp.pad(gate_bias.T, ((0, 0), (0, 124)))
    qkvo, aq, kv, pk, rows, cols = project(
        tokens, input_norm_gain[None], ga, gb, bias, decay_extra[:, 0]
    )
    st, nm, halo = scan_states(pk, kv)
    mix, logs = mix_local(
        qkvo, aq, kv, rows, cols, st, nm, halo, m_gain[None], sink_logit[None]
    )
    full = gather_heads(mix)
    return project_out(full, gb), logs


def solution(mesh):
    split = Mesh(mesh.devices.reshape(NZ, NY, NT), ("z", "y", "tp"))
    return jax.shard_map(
        on_device,
        mesh=split,
        in_specs=(
            P(SP, None),
            P(),
            P(SP, "tp"),
            P(SP, "tp"),
            P(SP, "tp"),
            P(SP, "tp"),
            P(SP, None, "tp"),
            P(None, "tp"),
            P(None, "tp", SP),
            P("tp"),
            P(SP, "tp"),
            P(SP, "tp"),
            P(SP, "tp"),
            P("tp"),
            P(SP, "tp"),
            P(SP, "tp"),
        ),
        out_specs=(P(SP, "tp"), P("tp", SP)),
        check_vma=False,
    )
```

```python
import jax
import jax.numpy as jnp
from jax import lax
from jax.experimental import pallas as pl
from jax.experimental.pallas import tpu as pltpu
from jax.sharding import Mesh
from jax.sharding import PartitionSpec as P

M_DIM = 128
W_DIM = 64
WINDOW = 128
EPS = 1e-06
FLOOR_LOG = -1e30
NZ = 16
NY = 4
NX = 4
NT = 8
TOK = 256
D = 2048
HALF = NZ // 2
A_COLS = 640
B_ROWS = 104
SP = ("z", "y")
MESH = pl.DeviceIdType.MESH
F32 = jnp.float32
BF16 = jnp.bfloat16
ACROSS = (((1,), (1,)), ((), ()))


def mod(a, n):
    return lax.rem(a + n, n)


def remote(src, dst, ssem, rsem, **where):
    return pltpu.make_async_remote_copy(
        src_ref=src,
        dst_ref=dst,
        send_sem=ssem,
        recv_sem=rsem,
        device_id=where,
        device_id_type=MESH,
    )


def log1p_of(e):
    poly = e * (
        1.0
        + e * (-0.5 + e * (1 / 3 + e * (-0.25 + e * (0.2 + e * (-1 / 6 + e * (1 / 7))))))
    )
    return jnp.where(e < 0.0625, poly, jnp.log(1.0 + e))


def log_sigmoid(x):
    return jnp.minimum(x, 0.0) - log1p_of(jnp.exp(-jnp.abs(x)))


def split3(x):
    hi = x.astype(BF16).astype(F32)
    mid = (x - hi).astype(BF16).astype(F32)
    return hi, mid, x - hi - mid


def joined(tail, at):
    return tail[at : at + 1] + tail[at + 1 : at + 2] + tail[at + 2 : at + 3]


def step_state(state, piece):
    peak, mat, norm = state
    p_peak, p_decay, p_mat, p_norm = piece
    new = jnp.maximum(peak + p_decay, p_peak)
    old_s, new_s = jnp.exp(peak + p_decay - new), jnp.exp(p_peak - new)
    return new, mat * old_s + p_mat * new_s, norm * old_s + p_norm * new_s


def empty_state():
    return (
        jnp.full((1, 128), FLOOR_LOG, F32),
        jnp.zeros((32, 128), F32),
        jnp.zeros((1, 128), F32),
    )


def layer_body(
    tok_hbm,
    gain,
    mq,
    mk,
    mv,
    mo,
    gate_t,
    bias,
    decay,
    mgain,
    aq_w,
    ak_w,
    av_w,
    sink,
    om,
    oa,
    out,
    logs,
    tok,
    wa,
    wb,
    ga,
    gb,
    normed,
    acc_a,
    acc_b,
    qkvo,
    aq,
    kv,
    halo,
    win,
    pk,
    p1,
    zp,
    p2,
    p3,
    st,
    keep,
    mixes,
    full,
    local_sem,
    ssem,
    az,
    ay,
    ah,
    bz,
    by,
    bh,
    s1,
    r1,
    s2,
    r2,
    s3,
    r3,
    sh,
    rh,
    hs,
    hx,
    hh,
    hc,
):
    z = lax.axis_index("z")
    y = lax.axis_index("y")
    t = lax.axis_index("tp")
    me = z * NY + y
    zu, zd = mod(z + 1, NZ), mod(z - 1, NZ)
    yu, yd = mod(y + 1, NY), mod(y - 1, NY)
    yo = mod(y + 2, NY)
    nxt, prv = mod(me + 1, NZ * NY), mod(me - 1, NZ * NY)
    zn, yn = lax.div(nxt, NY), lax.rem(nxt, NY)
    zq, yq = lax.div(prv, NY), lax.rem(prv, NY)
    x, c = lax.div(t, 2), lax.rem(t, 2)
    o = 1 - c
    xu, xd, xo = mod(x + 1, NX), mod(x - 1, NX), mod(x + 2, NX)
    partner, t_up, t_down, t_far = 2 * x + o, 2 * xu + c, 2 * xd + c, 2 * xo + c

    loads = []

    def load(src, dst):
        copy = pltpu.make_async_copy(src, dst, local_sem.at[len(loads)])
        copy.start()
        loads.append(copy)

    for i, w in enumerate((mq, mk, mv, mo, aq_w)):
        load(w, wa.at[:, 128 * i : 128 * i + 128])
    for i, w in enumerate((om, oa)):
        for part in (0, 1):
            at = 32 + 32 * i + 16 * part
            load(w.at[:, 128 * part : 128 * part + 128], wb.at[at : at + 16])
    load(tok_hbm, tok)
    barrier = pltpu.get_barrier_semaphore()
    hello = [{"z": zu}, {"z": zd}, {"y": yu}, {"y": yd}, {"y": yo}]
    hello += [{"z": zn, "y": yn}, {"z": zq, "y": yq}]
    hello += [{"tp": partner}, {"tp": t_up}, {"tp": t_down}]
    for where in hello:
        pl.semaphore_signal(barrier, inc=1, device_id=where, device_id_type=MESH)
    wb[0:32] = jnp.concatenate([ak_w[...], av_w[...]], axis=1)
    gate_rows = jnp.concatenate([gate_t[...].astype(F32), jnp.zeros((4, 96), F32)], axis=1)
    gate_row = gate_rows[0:1]
    for g in range(1, 4):
        gate_row = gate_row + pltpu.roll(gate_rows[g : g + 1], 32 * g, 1)
    wb[96:104] = jnp.concatenate([gate_row, jnp.zeros((7, 128), F32)], axis=0).astype(BF16)
    for copy in loads[:-1]:
        copy.wait()
    pl.semaphore_wait(barrier, len(hello))

    sa, sb = ssem.at[0], ssem.at[1]

    def a_up(src, slot, s):
        return remote(src, ga.at[slot], sa, az.at[0, s], z=zu)

    def a_down(src, slot, s):
        return remote(src, ga.at[slot], sa, az.at[1, s], z=zd)

    def a_side(src, zz):
        slot = zz * NY + y
        remote(src, ga.at[slot], sa, ay.at[0, zz], y=yu).start()
        remote(src, ga.at[slot], sa, ay.at[1, zz], y=yd).start()

    def b_up(src, slot, s, j):
        return remote(src, gb.at[slot], sb, bz.at[0, s, j], z=zu)

    def b_down(src, slot, s, j):
        return remote(src, gb.at[slot], sb, bz.at[1, s, j], z=zd)

    remote(wb, gb.at[me], sb, by.at[0], y=yu).start()
    remote(wb, gb.at[me], sb, by.at[1], y=yd).start()
    a_up(wa, me, 1).start()
    a_down(wa, me, 1).start()
    b_up(wb, me, 1, y).start()
    b_down(wb, me, 1, y).start()
    a_side(wa, z)
    ga[me] = wa[...]
    gb[me] = wb[...]

    loads[-1].wait()
    xs = tok[...].astype(F32)
    xs = xs * lax.rsqrt(jnp.mean(xs * xs, axis=-1, keepdims=True) + EPS) * gain[...]
    for i in range(NZ):
        normed[i] = xs[:, 128 * i : 128 * i + 128].astype(BF16)
    acc_a[...] = jnp.zeros_like(acc_a)
    acc_b[...] = jnp.zeros_like(acc_b)

    slot_d, slot_u, slot_o = z * NY + yd, z * NY + yu, z * NY + yo
    lo, hi = pl.ds(0, 16), pl.ds(16, 16)
    blo, bhi = pl.ds(0, 48), pl.ds(48, 56)
    remote(wb, gb.at[slot_d], sb, by.at[0], y=yd).wait_recv()
    remote(gb.at[slot_d, blo], gb.at[slot_d, blo], sb, bh.at[0], y=yu).start()
    b_up(gb.at[slot_d], slot_d, 1, yd).start()
    b_down(gb.at[slot_d], slot_d, 1, yd).start()
    remote(wb, gb.at[slot_u], sb, by.at[1], y=yd).wait_recv()
    remote(gb.at[slot_u, bhi], gb.at[slot_u, bhi], sb, bh.at[1], y=yd).start()
    b_up(gb.at[slot_u], slot_u, 1, yu).start()
    b_down(gb.at[slot_u], slot_u, 1, yu).start()
    remote(gb.at[slot_o, blo], gb.at[slot_o, blo], sb, bh.at[0], y=yd).wait_recv()
    remote(gb.at[slot_o, bhi], gb.at[slot_o, bhi], sb, bh.at[1], y=yd).wait_recv()
    b_up(gb.at[slot_o], slot_o, 1, yo).start()
    b_down(gb.at[slot_o], slot_o, 1, yo).start()

    def side_forward(zz):
        sd, su = zz * NY + yd, zz * NY + yu
        remote(ga.at[sd], ga.at[sd], sa, ay.at[0, zz], y=yd).wait_recv()
        remote(ga.at[sd, lo], ga.at[sd, lo], sa, ah.at[0, zz], y=yu).start()
        remote(ga.at[su], ga.at[su], sa, ay.at[1, zz], y=yd).wait_recv()
        remote(ga.at[su, hi], ga.at[su, hi], sa, ah.at[1, zz], y=yd).start()

    spread = lax.broadcasted_iota(jnp.int32, (32, 128), 0) == lax.rem(
        lax.broadcasted_iota(jnp.int32, (32, 128), 1), 32
    )

    def level(zz):
        so = zz * NY + yo
        remote(ga.at[so, lo], ga.at[so, lo], sa, ah.at[0, zz], y=yd).wait_recv()
        remote(ga.at[so, hi], ga.at[so, hi], sa, ah.at[1, zz], y=yd).wait_recv()
        rows = normed[zz]
        first = zz * NY
        for at, width in ((0, 256), (256, 256), (512, 128)):
            w = jnp.concatenate(
                [ga[first + j, :, at : at + width] for j in range(NY)], axis=0
            )
            acc_a[:, at : at + width] += jnp.dot(rows, w, preferred_element_type=F32)
        w = jnp.concatenate([gb[first + j, 0:32] for j in range(NY)], axis=0)
        g = jnp.concatenate(
            [
                jnp.where(spread, gb[first + j, 96:104].astype(F32)[0:1], 0.0).astype(BF16)
                for j in range(NY)
            ],
            axis=0,
        )
        acc_b[...] += jnp.dot(
            rows, jnp.concatenate([w, g], axis=1), preferred_element_type=F32
        )

    def both(d, what):
        what(mod(z - d, NZ))

        @pl.when((d > 0) & (d < HALF))
        def _():
            what(mod(z + d, NZ))

    def step(s, carry):
        z_lo, z_hi = mod(z - s, NZ), mod(z + s, NZ)
        slot = z_lo * NY + y
        a_up(ga.at[slot], slot, s).wait_recv()

        @pl.when(s < HALF)
        def _():
            a_up(ga.at[slot], slot, s + 1).start()

        a_side(ga.at[slot], z_lo)

        @pl.when(s < HALF)
        def _():
            slot2 = z_hi * NY + y
            a_down(ga.at[slot2], slot2, s).wait_recv()

            @pl.when(s < HALF - 1)
            def _():
                a_down(ga.at[slot2], slot2, s + 1).start()

            a_side(ga.at[slot2], z_hi)

        for j in (y, yd, yu, yo):
            sl = z_lo * NY + j
            b_up(gb.at[sl], sl, s, j).wait_recv()

            @pl.when(s < HALF)
            def _():
                b_up(gb.at[sl], sl, s + 1, j).start()

            @pl.when(s < HALF)
            def _():
                sl2 = z_hi * NY + j
                b_down(gb.at[sl2], sl2, s, j).wait_recv()

                @pl.when(s < HALF - 1)
                def _():
                    b_down(gb.at[sl2], sl2, s + 1, j).start()

        @pl.when(s >= 2)
        def _():
            both(s - 2, side_forward)

        @pl.when(s >= 4)
        def _():
            both(s - 4, level)

        return carry

    lax.fori_loop(1, HALF + 1, step, 0)

    def tail_step(d, carry):
        @pl.when(d < HALF + 1)
        def _():
            both(d, side_forward)

        both(d - 2, level)
        return carry

    lax.fori_loop(HALF - 1, HALF + 3, tail_step, 0)

    qkvo[...] = acc_a[:, 0:512].astype(BF16)
    aq[...] = acc_a[:, 512:640].astype(BF16)
    kv[...] = acc_b[:, 0:128].astype(BF16)
    first, last = pl.ds(0, WINDOW), pl.ds(TOK - WINDOW, WINDOW)
    to_next = remote(kv.at[last], halo.at[0], sh.at[0], rh.at[0], z=zn, y=yn)
    to_prev = remote(kv.at[first], halo.at[1], sh.at[1], rh.at[1], z=zq, y=yq)
    gt = jnp.sum(jnp.transpose(acc_b[:, 128:256]).reshape(4, 32, TOK), axis=1)
    in_f, in_b = gt[0:1] + bias[0:1, 0:1], gt[2:3] + bias[0:1, 2:3]
    lf_f = log_sigmoid(gt[1:2] + bias[0:1, 1:2]) + decay[0]
    lf_b = log_sigmoid(gt[3:4] + bias[0:1, 3:4]) + decay[1]
    to_next.start()
    to_prev.start()
    lane = lax.broadcasted_iota(jnp.int32, (1, TOK), 1)
    cum, rev = lf_f, lf_b
    k = 1
    while k < TOK:
        cum = cum + jnp.where(lane >= k, pltpu.roll(cum, k, 1), 0.0)
        rev = rev + jnp.where(lane < TOK - k, pltpu.roll(rev, TOK - k, 1), 0.0)
        k *= 2
    tot_f = jnp.max(jnp.where(lane == TOK - 1, cum, -jnp.inf), axis=1, keepdims=True)
    tot_b = jnp.max(jnp.where(lane == 0, rev, -jnp.inf), axis=1, keepdims=True)
    end_f = tot_f - cum + in_f
    end_b = tot_b - rev + in_b
    m_f = jnp.max(end_f, axis=1, keepdims=True)
    m_b = jnp.max(end_b, axis=1, keepdims=True)
    w_f, w_b = jnp.exp(end_f - m_f), jnp.exp(end_b - m_b)
    rows = jnp.concatenate([in_f, cum, in_b, rev, w_f, w_b, jnp.zeros((2, TOK), F32)], axis=0)
    cols = jnp.transpose(jnp.concatenate([rows, jnp.zeros((120, TOK), F32)], axis=0))
    query, key, value = qkvo[:, 0:128], qkvo[:, 128:256], qkvo[:, 256:384]
    val = value.astype(F32)
    tail, mats = [], []
    norms = jnp.dot(rows.astype(BF16), key, preferred_element_type=F32)
    for i in (4, 5):
        wv = (cols[:, i : i + 1] * val).astype(BF16)
        mats.append(
            lax.dot_general(key, wv, (((0,), (0,)), ((), ())), preferred_element_type=F32)
        )
        tail.append(norms[i : i + 1])
    for v in (m_f, tot_f, m_b, tot_b):
        tail.extend(jnp.broadcast_to(p, (1, 128)) for p in split3(v))
    tail.append(jnp.zeros((2, 128), F32))
    summary_tail = jnp.concatenate(tail, axis=0).astype(BF16)
    for q in range(NY):
        pk[q, 0:32] = mats[0][q * 32 : q * 32 + 32].astype(BF16)
        pk[q, 32:64] = mats[1][q * 32 : q * 32 + 32].astype(BF16)
        pk[q, 64:80] = summary_tail

    for d in (2, 1, 3):
        j = mod(y + d, NY)
        remote(pk.at[j], p1.at[y], s1.at[d - 1], r1.at[y], y=j).start()
    p1[y] = pk[y]

    scale = M_DIM**-0.5
    dots = lax.dot_general(query, key, ACROSS, preferred_element_type=F32) * scale
    ti = lax.broadcasted_iota(jnp.int32, (TOK, TOK), 0)
    si = lax.broadcasted_iota(jnp.int32, (TOK, TOK), 1)
    inside = []
    for back in (0, 1):
        cum_t = cols[:, 2 * back + 1 : 2 * back + 2]
        log_in = rows[2 * back : 2 * back + 1] - rows[2 * back + 1 : 2 * back + 2]
        usable = (si >= ti) if back else (si <= ti)
        log_w = jnp.where(usable, cum_t + log_in, -jnp.inf)
        top = jnp.max(log_w, axis=1, keepdims=True)
        scores = dots * jnp.exp(log_w - top)
        numer = jnp.dot(scores.astype(BF16), value, preferred_element_type=F32)
        denom = jnp.sum(scores, axis=1, keepdims=True)
        inside.append((cum_t, top, numer, denom))

    for d in range(1, NY):
        j = mod(y + d, NY)
        remote(p1.at[j], p1.at[j], s1.at[0], r1.at[j], y=j).wait_recv()

    def local_piece(j, back):
        ends = p1[j, 64:80].astype(F32)
        if back:
            return joined(ends, 8), joined(ends, 11), p1[j, 32:64].astype(F32), ends[1:2]
        return joined(ends, 2), joined(ends, 5), p1[j, 0:32].astype(F32), ends[0:1]

    for back in (0, 1):
        state, total_decay = empty_state(), jnp.zeros((1, 128), F32)
        for j in reversed(range(NY)) if back else range(NY):
            piece = local_piece(j, back)
            state = step_state(state, piece)
            total_decay = total_decay + piece[1]
        zp[back, 0:32] = state[1].astype(BF16)
        zp[back, 32:48] = jnp.concatenate(
            [state[2], *split3(state[0]), *split3(total_decay), jnp.zeros((9, 128), F32)],
            axis=0,
        ).astype(BF16)
    for d in (8, 7, 9, 6, 10, 5, 11, 4, 12, 3, 13, 2, 14, 1, 15):
        remote(
            zp.at[lax.div(z + d, NZ)],
            p2.at[z],
            s2.at[d - 1],
            r2.at[z],
            z=mod(z + d, NZ),
        ).start()

    mid, end = pl.ds(0, TOK // 2), pl.ds(TOK // 2, TOK // 2)

    def heads_start(i):
        mix, dst = mixes.at[i], full.at[i]
        remote(mix, dst.at[t], hs.at[i], hx.at[i, 0], tp=t_up).start()
        remote(mix, dst.at[t], hs.at[i], hx.at[i, 1], tp=t_down).start()
        remote(mix, dst.at[t], hs.at[i], hc.at[i, 0], tp=partner).start()
        full[i, t] = mixes[i]

    def heads_middle(i):
        mix, dst = mixes.at[i], full.at[i]
        remote(mix, dst.at[t_down], hs.at[i], hx.at[i, 0], tp=t_up).wait_recv()
        src = dst.at[t_down]
        remote(src.at[mid], src.at[mid], hs.at[i], hh.at[i, 0], tp=t_up).start()
        remote(src, src, hs.at[i], hc.at[i, 1], tp=partner).start()
        remote(mix, dst.at[t_up], hs.at[i], hx.at[i, 1], tp=t_up).wait_recv()
        src = dst.at[t_up]
        remote(src.at[end], src.at[end], hs.at[i], hh.at[i, 1], tp=t_down).start()
        remote(src, src, hs.at[i], hc.at[i, 2], tp=partner).start()

    def heads_end(i):
        mix, dst = mixes.at[i], full.at[i]
        for n, part in enumerate((mid, end)):
            src = dst.at[t_far, part]
            remote(src, src, hs.at[i], hh.at[i, n], tp=t_up).wait_recv()
            remote(src, src, hs.at[i], hc.at[i, 3 + n], tp=partner).start()
        remote(mix, dst.at[partner], hs.at[i], hc.at[i, 0], tp=partner).wait_recv()
        remote(mix, dst.at[2 * xd + o], hs.at[i], hc.at[i, 1], tp=partner).wait_recv()
        remote(mix, dst.at[2 * xu + o], hs.at[i], hc.at[i, 2], tp=partner).wait_recv()
        for n, part in enumerate((mid, end)):
            src = dst.at[2 * xo + o, part]
            remote(src, src, hs.at[i], hc.at[i, 3 + n], tp=partner).wait_recv()

    def heads_product(i):
        total = None
        for n in range(NT):
            w = jnp.concatenate(
                [
                    gb[8 * n : 8 * n + 8, at : at + 16].reshape(128, 128)
                    for at in (32 + 32 * i, 48 + 32 * i)
                ],
                axis=1,
            )
            term = jnp.dot(full[i, n], w, preferred_element_type=F32)
            total = term if total is None else total + term
        return total

    to_next.wait_recv()
    to_prev.wait_recv()
    win[0:WINDOW] = halo[0]
    win[WINDOW : WINDOW + TOK] = kv[...]
    win[WINDOW + TOK :] = halo[1]
    low = lax.broadcasted_iota(jnp.int32, (WINDOW, 128), 1) < W_DIM
    two = lax.broadcasted_iota(jnp.int32, (2 * WINDOW, 3 * WINDOW), 0)
    col = lax.broadcasted_iota(jnp.int32, (2 * WINDOW, 3 * WINDOW), 1)
    off = col - jnp.where(two >= WINDOW, two - WINDOW, two)
    in_window = (off >= 0) & (off <= 2 * WINDOW)
    second = lax.broadcasted_iota(jnp.int32, (2 * WINDOW, 1), 0) >= WINDOW
    sink_col = jnp.where(second, sink[0:1, 1:2], sink[0:1, 0:1])
    for b in range(2):
        block = pl.ds(b * WINDOW, WINDOW)
        qb = aq[b * WINDOW : b * WINDOW + WINDOW].astype(F32)
        q0 = jnp.where(low, qb, 0.0)
        q1 = jnp.where(low, pltpu.roll(qb, W_DIM, 1), 0.0)
        qq = jnp.concatenate([q0, q1], axis=0).astype(BF16)
        keys = win[b * WINDOW : b * WINDOW + 3 * WINDOW]
        scores = lax.dot_general(qq, keys, ACROSS, preferred_element_type=F32) * W_DIM**-0.5
        place = me * TOK + (b - 1) * WINDOW + col
        usable = in_window & (place >= 0) & (place < NZ * NY * TOK)
        scores = jnp.where(usable, scores, -jnp.inf)
        peak = jnp.maximum(sink_col, jnp.max(scores, axis=1, keepdims=True))
        weights = jnp.exp(scores - peak)
        tot = jnp.exp(sink_col - peak) + jnp.sum(weights, axis=1, keepdims=True)
        res = jnp.dot(weights.astype(BF16), keys, preferred_element_type=F32) / tot
        mixes[1, block] = jnp.where(
            low, pltpu.roll(res[0:WINDOW], W_DIM, 1), res[WINDOW:]
        ).astype(BF16)
        logt = jnp.transpose(jnp.broadcast_to(peak + jnp.log(tot), (2 * WINDOW, 128)))
        logs[0:1, block] = logt[0:1, 0:WINDOW]
        logs[1:2, block] = logt[0:1, WINDOW:]
    heads_start(1)
    gate_open = 1.0 / (1.0 + jnp.exp(-qkvo[:, 384:512].astype(F32)))
    heads_middle(1)

    for d in range(1, NZ):
        j = mod(z + d, NZ)
        remote(p2.at[j], p2.at[j], s2.at[0], r2.at[j], z=j).wait_recv()

    def far(i, state):
        ends = p2[i, 32:48].astype(F32)
        return step_state(
            state, (joined(ends, 1), joined(ends, 4), p2[i, 0:32].astype(F32), ends[0:1])
        )

    fwd = lax.fori_loop(0, z, far, empty_state())
    bwd = lax.fori_loop(0, NZ - 1 - z, lambda i, s: far(NZ - 1 - i, s), empty_state())
    for j in range(NY):
        p3[j, 0:32] = fwd[1].astype(BF16)
        keep[j, 0:1] = fwd[2]
        keep[j, 2:3] = fwd[0]
        fwd = step_state(fwd, local_piece(j, 0))
    for j in reversed(range(NY)):
        p3[j, 32:64] = bwd[1].astype(BF16)
        keep[j, 1:2] = bwd[2]
        keep[j, 3:4] = bwd[0]
        bwd = step_state(bwd, local_piece(j, 1))
    for d in (2, 1, 3):
        j = mod(y + d, NY)
        remote(p3.at[j], st.at[y], s3.at[d - 1], r3.at[y], y=j).start()
    st[y] = p3[y]
    nm = keep[y]
    heads_end(1)
    acc_b[...] = heads_product(1)
    qf = query.astype(F32) * scale
    for d in range(1, NY):
        j = mod(y + d, NY)
        remote(st.at[j], st.at[j], s3.at[0], r3.at[j], y=j).wait_recv()

    cell = None
    for back in (0, 1):
        cum_t, top_in, numer, denom = inside[back]
        inter = cum_t + nm[2 + back : 3 + back, 0:1]
        top = jnp.maximum(inter, top_in)
        w_in, w_inter = jnp.exp(top_in - top), jnp.exp(inter - top)
        mat = st[:, 32 * back : 32 * back + 32].reshape(128, 128)
        numer = w_in * numer + (w_inter * scale) * jnp.dot(
            query, mat, preferred_element_type=F32
        )
        denom = w_in * denom + w_inter * jnp.sum(
            qf * nm[back : back + 1], axis=1, keepdims=True
        )
        part = numer / jnp.maximum(jnp.abs(denom), jnp.exp(-top))
        cell = part if cell is None else cell + part
    u = cell * gate_open
    norm = lax.rsqrt(jnp.mean(u * u, axis=1, keepdims=True) + EPS)
    mixes[0] = (u * norm * mgain[...]).astype(BF16)
    heads_start(0)
    heads_middle(0)
    heads_end(0)
    out[...] = (acc_b[...] + heads_product(0)).astype(BF16)

    n = NZ * NY - 1
    every = pl.ds(0, n)
    remote(ga.at[every], ga.at[every], sa, az.at[0, 0], y=yd).wait_send()
    remote(gb.at[every], gb.at[every], sb, az.at[0, 0], y=yd).wait_send()
    for d in range(1, NY):
        remote(pk.at[0], p1.at[0], s1.at[d - 1], r1.at[0], y=yd).wait_send()
        remote(p3.at[0], st.at[0], s3.at[d - 1], r3.at[0], y=yd).wait_send()
    for d in range(1, NZ):
        remote(zp.at[0], p2.at[0], s2.at[d - 1], r2.at[0], z=zd).wait_send()
    to_next.wait_send()
    to_prev.wait_send()
    most = pl.ds(0, NT - 1)
    for i in (0, 1):
        src = full.at[i, most]
        remote(src, src, hs.at[i], hc.at[i, 0], tp=partner).wait_send()


def on_device(
    tokens,
    input_norm_gain,
    mq_weight,
    mk_weight,
    mv_weight,
    mo_weight,
    gate_weight,
    gate_bias,
    decay_extra,
    m_gain,
    aq_weight,
    ak_weight,
    av_weight,
    sink_logit,
    out_m_weight,
    out_a_weight,
):
    sds = jax.ShapeDtypeStruct
    dma = pltpu.SemaphoreType.DMA
    vm = pltpu.VMEM
    hbm = pl.BlockSpec(memory_space=pl.ANY)
    local = pl.BlockSpec(memory_space=pltpu.VMEM)
    n = NZ * NY
    return pl.pallas_call(
        layer_body,
        name="layer",
        out_shape=(sds((TOK, 256), BF16), sds((2, TOK), F32)),
        in_specs=[hbm, local, hbm, hbm, hbm, hbm, local, local, local, local]
        + [hbm, local, local, local, hbm, hbm],
        out_specs=[local] * 2,
        scratch_shapes=[
            vm((TOK, D), BF16),
            vm((32, A_COLS), BF16),
            vm((B_ROWS, 128), BF16),
            vm((n, 32, A_COLS), BF16),
            vm((n, B_ROWS, 128), BF16),
            vm((NZ, TOK, 128), BF16),
            vm((TOK, A_COLS), F32),
            vm((TOK, 256), F32),
            vm((TOK, 512), BF16),
            vm((TOK, 128), BF16),
            vm((TOK, 128), BF16),
            vm((2, WINDOW, 128), BF16),
            vm((TOK + 2 * WINDOW, 128), BF16),
            vm((NY, 80, 128), BF16),
            vm((NY, 80, 128), BF16),
            vm((2, 48, 128), BF16),
            vm((NZ, 48, 128), BF16),
            vm((NY, 64, 128), BF16),
            vm((NY, 64, 128), BF16),
            vm((NY, 8, 128), F32),
            vm((2, TOK, 128), BF16),
            vm((2, NT, TOK, 128), BF16),
            dma((10,)),
            dma((2,)),
            dma((2, HALF + 1)),
            dma((2, NZ)),
            dma((2, NZ)),
            dma((2, HALF + 1, NY)),
            dma((2,)),
            dma((2,)),
            dma((NY - 1,)),
            dma((NY,)),
            dma((NZ - 1,)),
            dma((NZ,)),
            dma((NY - 1,)),
            dma((NY,)),
            dma((2,)),
            dma((2,)),
            dma((2,)),
            dma((2, 2)),
            dma((2, 2)),
            dma((2, 5)),
        ],
        compiler_params=pltpu.CompilerParams(collective_id=0, has_side_effects=True),
    )(
        tokens,
        input_norm_gain[None],
        mq_weight,
        mk_weight,
        mv_weight,
        mo_weight,
        gate_weight[:, :, 0].T,
        gate_bias.T,
        decay_extra,
        m_gain[None],
        aq_weight,
        ak_weight,
        av_weight,
        sink_logit[None],
        out_m_weight,
        out_a_weight,
    )


def solution(mesh):
    split = Mesh(mesh.devices.reshape(NZ, NY, NT), ("z", "y", "tp"))
    return jax.shard_map(
        on_device,
        mesh=split,
        in_specs=(
            P(SP, None),
            P(),
            P(SP, "tp"),
            P(SP, "tp"),
            P(SP, "tp"),
            P(SP, "tp"),
            P(SP, None, "tp"),
            P(None, "tp"),
            P(None, "tp", SP),
            P("tp"),
            P(SP, "tp"),
            P(SP, "tp"),
            P(SP, "tp"),
            P("tp"),
            P(SP, "tp"),
            P(SP, "tp"),
        ),
        out_specs=(P(SP, "tp"), P("tp", SP)),
        check_vma=False,
    )
```

```python
import jax
import jax.numpy as jnp
from jax import lax
from jax.experimental import pallas as pl
from jax.experimental.pallas import tpu as pltpu
from jax.sharding import Mesh
from jax.sharding import PartitionSpec as P

M_DIM = 128
W_DIM = 64
WINDOW = 128
EPS = 1e-06
FLOOR_LOG = -1e30
NZ = 16
NY = 4
NX = 4
NT = 8
TOK = 256
D = 2048
HALF = NZ // 2
A_ROWS = 160
B_ROWS = 104
SP = ("z", "y")
MESH = pl.DeviceIdType.MESH
F32 = jnp.float32
BF16 = jnp.bfloat16
ACROSS = (((1,), (1,)), ((), ()))


def mod(a, n):
    return lax.rem(a + n, n)


def remote(src, dst, ssem, rsem, **where):
    return pltpu.make_async_remote_copy(
        src_ref=src,
        dst_ref=dst,
        send_sem=ssem,
        recv_sem=rsem,
        device_id=where,
        device_id_type=MESH,
    )


def log1p_of(e):
    poly = e * (
        1.0
        + e * (-0.5 + e * (1 / 3 + e * (-0.25 + e * (0.2 + e * (-1 / 6 + e * (1 / 7))))))
    )
    return jnp.where(e < 0.0625, poly, jnp.log(1.0 + e))


def log_sigmoid(x):
    return jnp.minimum(x, 0.0) - log1p_of(jnp.exp(-jnp.abs(x)))


def split3(x):
    hi = x.astype(BF16).astype(F32)
    mid = (x - hi).astype(BF16).astype(F32)
    return hi, mid, x - hi - mid


def joined(tail, at):
    return tail[at : at + 1] + tail[at + 1 : at + 2] + tail[at + 2 : at + 3]


def step_state(state, piece):
    peak, mat, norm = state
    p_peak, p_decay, p_mat, p_norm = piece
    new = jnp.maximum(peak + p_decay, p_peak)
    old_s, new_s = jnp.exp(peak + p_decay - new), jnp.exp(p_peak - new)
    return new, mat * old_s + p_mat * new_s, norm * old_s + p_norm * new_s


def empty_state():
    return (
        jnp.full((1, 128), FLOOR_LOG, F32),
        jnp.zeros((32, 128), F32),
        jnp.zeros((1, 128), F32),
    )


def layer_body(
    tok_hbm,
    gain,
    mq,
    mk,
    mv,
    mo,
    gate_t,
    bias,
    decay,
    mgain,
    aq_w,
    ak_w,
    av_w,
    sink,
    om,
    oa,
    out,
    logs,
    tok,
    wa,
    wb,
    ga,
    gb,
    normed,
    acc_a,
    acc_b,
    kv,
    halo,
    win,
    pk,
    p1,
    zp,
    p2,
    p3,
    st,
    keep,
    mixes,
    full,
    local_sem,
    ssem,
    az,
    ay,
    ah,
    bz,
    by,
    bh,
    s1,
    r1,
    s2,
    r2,
    s3,
    r3,
    sh,
    rh,
    hs,
    hx,
    hh,
    hc,
):
    z = lax.axis_index("z")
    y = lax.axis_index("y")
    t = lax.axis_index("tp")
    me = z * NY + y
    zu, zd = mod(z + 1, NZ), mod(z - 1, NZ)
    yu, yd = mod(y + 1, NY), mod(y - 1, NY)
    yo = mod(y + 2, NY)
    nxt, prv = mod(me + 1, NZ * NY), mod(me - 1, NZ * NY)
    zn, yn = lax.div(nxt, NY), lax.rem(nxt, NY)
    zq, yq = lax.div(prv, NY), lax.rem(prv, NY)
    x, c = lax.div(t, 2), lax.rem(t, 2)
    o = 1 - c
    xu, xd, xo = mod(x + 1, NX), mod(x - 1, NX), mod(x + 2, NX)
    partner, t_up, t_down, t_far = 2 * x + o, 2 * xu + c, 2 * xd + c, 2 * xo + c

    loads = []

    def load(src, dst):
        copy = pltpu.make_async_copy(src, dst, local_sem.at[len(loads)])
        copy.start()
        loads.append(copy)
        return copy

    for i, w in enumerate((mk, mv)):
        load(w, wb.at[32 * i : 32 * i + 32])
    for i, w in enumerate((mq, mo, aq_w)):
        load(w, wa.at[32 * i : 32 * i + 32])
    for i, w in enumerate((om, oa)):
        for part in (0, 1):
            at = 96 + 32 * i + 16 * part
            load(w.at[:, 128 * part : 128 * part + 128], wa.at[at : at + 16])
    tok_load = load(tok_hbm, tok)
    barrier = pltpu.get_barrier_semaphore()
    hello = [{"z": zu}, {"z": zd}, {"y": yu}, {"y": yd}, {"y": yo}]
    hello += [{"z": zn, "y": yn}, {"z": zq, "y": yq}]
    hello += [{"tp": partner}, {"tp": t_up}, {"tp": t_down}]
    for where in hello:
        pl.semaphore_signal(barrier, inc=1, device_id=where, device_id_type=MESH)
    wb[64:96] = jnp.concatenate([ak_w[...], av_w[...]], axis=1)
    gate_rows = jnp.concatenate([gate_t[...].astype(F32), jnp.zeros((4, 96), F32)], axis=1)
    gate_row = gate_rows[0:1]
    for g in range(1, 4):
        gate_row = gate_row + pltpu.roll(gate_rows[g : g + 1], 32 * g, 1)
    wb[96:104] = jnp.concatenate([gate_row, jnp.zeros((7, 128), F32)], axis=0).astype(BF16)
    for copy in loads[:-1]:
        copy.wait()
    pl.semaphore_wait(barrier, len(hello))

    sa, sb = ssem.at[0], ssem.at[1]

    def a_up(src, slot, s):
        return remote(src, ga.at[slot], sa, az.at[0, s], z=zu)

    def a_down(src, slot, s):
        return remote(src, ga.at[slot], sa, az.at[1, s], z=zd)

    def a_side(src, zz):
        slot = zz * NY + y
        remote(src, ga.at[slot], sa, ay.at[0, zz], y=yu).start()
        remote(src, ga.at[slot], sa, ay.at[1, zz], y=yd).start()

    def b_up(src, slot, s, j):
        return remote(src, gb.at[slot], sb, bz.at[0, s, j], z=zu)

    def b_down(src, slot, s, j):
        return remote(src, gb.at[slot], sb, bz.at[1, s, j], z=zd)

    remote(wb, gb.at[me], sb, by.at[0], y=yu).start()
    remote(wb, gb.at[me], sb, by.at[1], y=yd).start()
    b_up(wb, me, 1, y).start()
    b_down(wb, me, 1, y).start()
    a_up(wa, me, 1).start()
    a_down(wa, me, 1).start()
    ga[me] = wa[...]
    gb[me] = wb[...]

    slot_d, slot_u, slot_o = z * NY + yd, z * NY + yu, z * NY + yo
    lo, hi = pl.ds(0, A_ROWS // 2), pl.ds(A_ROWS // 2, A_ROWS // 2)
    blo, bhi = pl.ds(0, 48), pl.ds(48, 56)
    remote(wb, gb.at[slot_d], sb, by.at[0], y=yd).wait_recv()
    remote(gb.at[slot_d, blo], gb.at[slot_d, blo], sb, bh.at[0], y=yu).start()
    b_up(gb.at[slot_d], slot_d, 1, yd).start()
    b_down(gb.at[slot_d], slot_d, 1, yd).start()
    remote(wb, gb.at[slot_u], sb, by.at[1], y=yd).wait_recv()
    remote(gb.at[slot_u, bhi], gb.at[slot_u, bhi], sb, bh.at[1], y=yd).start()
    b_up(gb.at[slot_u], slot_u, 1, yu).start()
    b_down(gb.at[slot_u], slot_u, 1, yu).start()
    a_side(wa, z)

    def norm():
        tok_load.wait()
        xs = tok[...].astype(F32)
        xs = xs * lax.rsqrt(jnp.mean(xs * xs, axis=-1, keepdims=True) + EPS) * gain[...]
        for i in range(NZ):
            normed[i] = xs[:, 128 * i : 128 * i + 128].astype(BF16)
        acc_a[...] = jnp.zeros_like(acc_a)
        acc_b[...] = jnp.zeros_like(acc_b)

    def opposite():
        remote(gb.at[slot_o, blo], gb.at[slot_o, blo], sb, bh.at[0], y=yd).wait_recv()
        remote(gb.at[slot_o, bhi], gb.at[slot_o, bhi], sb, bh.at[1], y=yd).wait_recv()
        b_up(gb.at[slot_o], slot_o, 1, yo).start()
        b_down(gb.at[slot_o], slot_o, 1, yo).start()

    def side_forward(zz):
        sd, su = zz * NY + yd, zz * NY + yu
        remote(ga.at[sd], ga.at[sd], sa, ay.at[0, zz], y=yd).wait_recv()
        remote(ga.at[sd, lo], ga.at[sd, lo], sa, ah.at[0, zz], y=yu).start()
        remote(ga.at[su], ga.at[su], sa, ay.at[1, zz], y=yd).wait_recv()
        remote(ga.at[su, hi], ga.at[su, hi], sa, ah.at[1, zz], y=yd).start()

    spread = lax.broadcasted_iota(jnp.int32, (32, 128), 0) == lax.rem(
        lax.broadcasted_iota(jnp.int32, (32, 128), 1), 32
    )

    def stacked(ref, zz, at):
        return jnp.concatenate([ref[zz * NY + j, at : at + 32] for j in range(NY)], axis=0)

    def level_a(zz):
        so = zz * NY + yo
        remote(ga.at[so, lo], ga.at[so, lo], sa, ah.at[0, zz], y=yd).wait_recv()
        remote(ga.at[so, hi], ga.at[so, hi], sa, ah.at[1, zz], y=yd).wait_recv()
        rows = normed[zz]
        w = jnp.concatenate([stacked(ga, zz, 0), stacked(ga, zz, 32)], axis=1)
        acc_a[:, 0:256] += jnp.dot(rows, w, preferred_element_type=F32)
        acc_a[:, 256:384] += jnp.dot(rows, stacked(ga, zz, 64), preferred_element_type=F32)

    def level_b(zz):
        rows = normed[zz]
        w = jnp.concatenate([stacked(gb, zz, 0), stacked(gb, zz, 32)], axis=1)
        acc_b[:, 0:256] += jnp.dot(rows, w, preferred_element_type=F32)
        g = jnp.concatenate(
            [
                jnp.where(
                    spread, gb[zz * NY + j, 96:104].astype(F32)[0:1], 0.0
                ).astype(BF16)
                for j in range(NY)
            ],
            axis=0,
        )
        w = jnp.concatenate([stacked(gb, zz, 64), g], axis=1)
        acc_b[:, 256:512] += jnp.dot(rows, w, preferred_element_type=F32)

    def both(d, what):
        what(mod(z - d, NZ))

        @pl.when((d > 0) & (d < HALF))
        def _():
            what(mod(z + d, NZ))

    def step(s, carry):
        z_lo, z_hi = mod(z - s, NZ), mod(z + s, NZ)

        def b_step(j, far_up):
            sl, sl2 = z_lo * NY + j, z_hi * NY + j
            up_from, down_from = (HALF, HALF - 1) if far_up else (HALF - 1, HALF)

            @pl.when(s <= up_from)
            def _():
                b_up(gb.at[sl], sl, s, j).wait_recv()

                @pl.when(s < up_from)
                def _():
                    b_up(gb.at[sl], sl, s + 1, j).start()

            @pl.when(s <= down_from)
            def _():
                b_down(gb.at[sl2], sl2, s, j).wait_recv()

                @pl.when(s < down_from)
                def _():
                    b_down(gb.at[sl2], sl2, s + 1, j).start()

        b_step(y, True)
        slot = z_lo * NY + y
        a_up(ga.at[slot], slot, s).wait_recv()

        @pl.when(s < HALF)
        def _():
            a_up(ga.at[slot], slot, s + 1).start()

        a_side(ga.at[slot], z_lo)

        @pl.when(s < HALF)
        def _():
            slot2 = z_hi * NY + y
            a_down(ga.at[slot2], slot2, s).wait_recv()

            @pl.when(s < HALF - 1)
            def _():
                a_down(ga.at[slot2], slot2, s + 1).start()

            a_side(ga.at[slot2], z_hi)

        @pl.when(s == 1)
        def _():
            opposite()
            norm()

        b_step(yd, True)
        b_step(yu, False)
        b_step(yo, False)

        @pl.when(s >= 2)
        def _():
            both(s - 2, side_forward)
            both(s - 2, level_b)

        @pl.when(s >= 4)
        def _():
            both(s - 4, level_a)

        return carry

    lax.fori_loop(1, HALF + 1, step, 0)
    both(HALF - 1, level_b)
    level_b(mod(z - HALF, NZ))

    kv[...] = acc_b[:, 256:384].astype(BF16)
    first, last = pl.ds(0, WINDOW), pl.ds(TOK - WINDOW, WINDOW)
    to_next = remote(kv.at[last], halo.at[0], sh.at[0], rh.at[0], z=zn, y=yn)
    to_prev = remote(kv.at[first], halo.at[1], sh.at[1], rh.at[1], z=zq, y=yq)
    gt = jnp.sum(jnp.transpose(acc_b[:, 384:512]).reshape(4, 32, TOK), axis=1)
    in_f, in_b = gt[0:1] + bias[0:1, 0:1], gt[2:3] + bias[0:1, 2:3]
    lf_f = log_sigmoid(gt[1:2] + bias[0:1, 1:2]) + decay[0]
    lf_b = log_sigmoid(gt[3:4] + bias[0:1, 3:4]) + decay[1]
    to_next.start()
    to_prev.start()
    lane = lax.broadcasted_iota(jnp.int32, (1, TOK), 1)
    cum, rev = lf_f, lf_b
    k = 1
    while k < TOK:
        cum = cum + jnp.where(lane >= k, pltpu.roll(cum, k, 1), 0.0)
        rev = rev + jnp.where(lane < TOK - k, pltpu.roll(rev, TOK - k, 1), 0.0)
        k *= 2
    tot_f = jnp.max(jnp.where(lane == TOK - 1, cum, -jnp.inf), axis=1, keepdims=True)
    tot_b = jnp.max(jnp.where(lane == 0, rev, -jnp.inf), axis=1, keepdims=True)
    end_f = tot_f - cum + in_f
    end_b = tot_b - rev + in_b
    m_f = jnp.max(end_f, axis=1, keepdims=True)
    m_b = jnp.max(end_b, axis=1, keepdims=True)
    w_f, w_b = jnp.exp(end_f - m_f), jnp.exp(end_b - m_b)
    rows = jnp.concatenate([in_f, cum, in_b, rev, w_f, w_b, jnp.zeros((2, TOK), F32)], axis=0)
    cols = jnp.transpose(jnp.concatenate([rows, jnp.zeros((120, TOK), F32)], axis=0))
    key, value = acc_b[:, 0:128].astype(BF16), acc_b[:, 128:256].astype(BF16)
    val = value.astype(F32)
    tail, mats = [], []
    norms = jnp.dot(rows.astype(BF16), key, preferred_element_type=F32)
    for i in (4, 5):
        wv = (cols[:, i : i + 1] * val).astype(BF16)
        mats.append(
            lax.dot_general(key, wv, (((0,), (0,)), ((), ())), preferred_element_type=F32)
        )
        tail.append(norms[i : i + 1])
    for v in (m_f, tot_f, m_b, tot_b):
        tail.extend(jnp.broadcast_to(p, (1, 128)) for p in split3(v))
    tail.append(jnp.zeros((2, 128), F32))
    summary_tail = jnp.concatenate(tail, axis=0).astype(BF16)
    for q in range(NY):
        pk[q, 0:32] = mats[0][q * 32 : q * 32 + 32].astype(BF16)
        pk[q, 32:64] = mats[1][q * 32 : q * 32 + 32].astype(BF16)
        pk[q, 64:80] = summary_tail

    for d in (2, 1, 3):
        j = mod(y + d, NY)
        remote(pk.at[j], p1.at[y], s1.at[d - 1], r1.at[y], y=j).start()
    p1[y] = pk[y]

    both(HALF - 1, side_forward)
    level_a(mod(z - 5, NZ))
    level_a(mod(z + 5, NZ))
    side_forward(mod(z - HALF, NZ))
    level_a(mod(z - 6, NZ))
    level_a(mod(z + 6, NZ))

    for d in range(1, NY):
        j = mod(y + d, NY)
        remote(p1.at[j], p1.at[j], s1.at[0], r1.at[j], y=j).wait_recv()

    def local_piece(j, back):
        ends = p1[j, 64:80].astype(F32)
        if back:
            return joined(ends, 8), joined(ends, 11), p1[j, 32:64].astype(F32), ends[1:2]
        return joined(ends, 2), joined(ends, 5), p1[j, 0:32].astype(F32), ends[0:1]

    for back in (0, 1):
        state, total_decay = empty_state(), jnp.zeros((1, 128), F32)
        for j in reversed(range(NY)) if back else range(NY):
            piece = local_piece(j, back)
            state = step_state(state, piece)
            total_decay = total_decay + piece[1]
        zp[back, 0:32] = state[1].astype(BF16)
        zp[back, 32:40] = jnp.concatenate(
            [state[2], *split3(state[0]), *split3(total_decay), jnp.zeros((1, 128), F32)],
            axis=0,
        ).astype(BF16)
    for d in (8, 7, 9, 6, 10, 5, 11, 4, 12, 3, 13, 2, 14, 1, 15):
        remote(
            zp.at[lax.div(z + d, NZ)],
            p2.at[z],
            s2.at[d - 1],
            r2.at[z],
            z=mod(z + d, NZ),
        ).start()

    level_a(mod(z - 7, NZ))
    level_a(mod(z + 7, NZ))
    level_a(mod(z - HALF, NZ))
    query = acc_a[:, 0:128].astype(BF16)
    gate_in = acc_a[:, 128:256].astype(BF16)
    a_query = acc_a[:, 256:384].astype(BF16).astype(F32)

    mid, end = pl.ds(0, TOK // 2), pl.ds(TOK // 2, TOK // 2)

    def heads_start(i):
        mix, dst = mixes.at[i], full.at[i]
        remote(mix, dst.at[t], hs.at[i], hx.at[i, 0], tp=t_up).start()
        remote(mix, dst.at[t], hs.at[i], hx.at[i, 1], tp=t_down).start()
        remote(mix, dst.at[t], hs.at[i], hc.at[i, 0], tp=partner).start()
        full[i, t] = mixes[i]

    def heads_middle(i):
        mix, dst = mixes.at[i], full.at[i]
        remote(mix, dst.at[t_down], hs.at[i], hx.at[i, 0], tp=t_up).wait_recv()
        src = dst.at[t_down]
        remote(src.at[mid], src.at[mid], hs.at[i], hh.at[i, 0], tp=t_up).start()
        remote(src, src, hs.at[i], hc.at[i, 1], tp=partner).start()
        remote(mix, dst.at[t_up], hs.at[i], hx.at[i, 1], tp=t_up).wait_recv()
        src = dst.at[t_up]
        remote(src.at[end], src.at[end], hs.at[i], hh.at[i, 1], tp=t_down).start()
        remote(src, src, hs.at[i], hc.at[i, 2], tp=partner).start()

    def heads_end(i):
        mix, dst = mixes.at[i], full.at[i]
        for n, part in enumerate((mid, end)):
            src = dst.at[t_far, part]
            remote(src, src, hs.at[i], hh.at[i, n], tp=t_up).wait_recv()
            remote(src, src, hs.at[i], hc.at[i, 3 + n], tp=partner).start()
        remote(mix, dst.at[partner], hs.at[i], hc.at[i, 0], tp=partner).wait_recv()
        remote(mix, dst.at[2 * xd + o], hs.at[i], hc.at[i, 1], tp=partner).wait_recv()
        remote(mix, dst.at[2 * xu + o], hs.at[i], hc.at[i, 2], tp=partner).wait_recv()
        for n, part in enumerate((mid, end)):
            src = dst.at[2 * xo + o, part]
            remote(src, src, hs.at[i], hc.at[i, 3 + n], tp=partner).wait_recv()

    def heads_product(i):
        total = None
        for n in range(NT):
            w = jnp.concatenate(
                [
                    ga[8 * n : 8 * n + 8, at : at + 16].reshape(128, 128)
                    for at in (96 + 32 * i, 112 + 32 * i)
                ],
                axis=1,
            )
            term = jnp.dot(full[i, n], w, preferred_element_type=F32)
            total = term if total is None else total + term
        return total

    to_next.wait_recv()
    to_prev.wait_recv()
    win[0:WINDOW] = halo[0]
    win[WINDOW : WINDOW + TOK] = kv[...]
    win[WINDOW + TOK :] = halo[1]
    low = lax.broadcasted_iota(jnp.int32, (WINDOW, 128), 1) < W_DIM
    two = lax.broadcasted_iota(jnp.int32, (2 * WINDOW, 3 * WINDOW), 0)
    col = lax.broadcasted_iota(jnp.int32, (2 * WINDOW, 3 * WINDOW), 1)
    off = col - jnp.where(two >= WINDOW, two - WINDOW, two)
    in_window = (off >= 0) & (off <= 2 * WINDOW)
    second = lax.broadcasted_iota(jnp.int32, (2 * WINDOW, 1), 0) >= WINDOW
    sink_col = jnp.where(second, sink[0:1, 1:2], sink[0:1, 0:1])
    for b in range(2):
        block = pl.ds(b * WINDOW, WINDOW)
        qb = a_query[b * WINDOW : b * WINDOW + WINDOW]
        q0 = jnp.where(low, qb, 0.0)
        q1 = jnp.where(low, pltpu.roll(qb, W_DIM, 1), 0.0)
        qq = jnp.concatenate([q0, q1], axis=0).astype(BF16)
        keys = win[b * WINDOW : b * WINDOW + 3 * WINDOW]
        scores = lax.dot_general(qq, keys, ACROSS, preferred_element_type=F32) * W_DIM**-0.5
        place = me * TOK + (b - 1) * WINDOW + col
        usable = in_window & (place >= 0) & (place < NZ * NY * TOK)
        scores = jnp.where(usable, scores, -jnp.inf)
        peak = jnp.maximum(sink_col, jnp.max(scores, axis=1, keepdims=True))
        weights = jnp.exp(scores - peak)
        tot = jnp.exp(sink_col - peak) + jnp.sum(weights, axis=1, keepdims=True)
        res = jnp.dot(weights.astype(BF16), keys, preferred_element_type=F32) / tot
        mixes[1, block] = jnp.where(
            low, pltpu.roll(res[0:WINDOW], W_DIM, 1), res[WINDOW:]
        ).astype(BF16)
        logt = jnp.transpose(jnp.broadcast_to(peak + jnp.log(tot), (2 * WINDOW, 128)))
        logs[0:1, block] = logt[0:1, 0:WINDOW]
        logs[1:2, block] = logt[0:1, WINDOW:]
    heads_start(1)
    gate_open = 1.0 / (1.0 + jnp.exp(-gate_in.astype(F32)))

    scale = M_DIM**-0.5
    dots = lax.dot_general(query, key, ACROSS, preferred_element_type=F32) * scale
    ti = lax.broadcasted_iota(jnp.int32, (TOK, TOK), 0)
    si = lax.broadcasted_iota(jnp.int32, (TOK, TOK), 1)
    inside = []
    for back in (0, 1):
        cum_t = cols[:, 2 * back + 1 : 2 * back + 2]
        log_in = rows[2 * back : 2 * back + 1] - rows[2 * back + 1 : 2 * back + 2]
        usable = (si >= ti) if back else (si <= ti)
        log_w = jnp.where(usable, cum_t + log_in, -jnp.inf)
        top = jnp.max(log_w, axis=1, keepdims=True)
        scores = dots * jnp.exp(log_w - top)
        numer = jnp.dot(scores.astype(BF16), value, preferred_element_type=F32)
        denom = jnp.sum(scores, axis=1, keepdims=True)
        inside.append((cum_t, top, numer, denom))

    heads_middle(1)

    for d in range(1, NZ):
        j = mod(z + d, NZ)
        remote(p2.at[j], p2.at[j], s2.at[0], r2.at[j], z=j).wait_recv()

    def far(i, state):
        ends = p2[i, 32:40].astype(F32)
        return step_state(
            state, (joined(ends, 1), joined(ends, 4), p2[i, 0:32].astype(F32), ends[0:1])
        )

    fwd = lax.fori_loop(0, z, far, empty_state())
    bwd = lax.fori_loop(0, NZ - 1 - z, lambda i, s: far(NZ - 1 - i, s), empty_state())
    for j in range(NY):
        p3[j, 0:32] = fwd[1].astype(BF16)
        keep[j, 0:1] = fwd[2]
        keep[j, 2:3] = fwd[0]
        fwd = step_state(fwd, local_piece(j, 0))
    for j in reversed(range(NY)):
        p3[j, 32:64] = bwd[1].astype(BF16)
        keep[j, 1:2] = bwd[2]
        keep[j, 3:4] = bwd[0]
        bwd = step_state(bwd, local_piece(j, 1))
    for d in (2, 1, 3):
        j = mod(y + d, NY)
        remote(p3.at[j], st.at[y], s3.at[d - 1], r3.at[y], y=j).start()
    st[y] = p3[y]
    nm = keep[y]
    heads_end(1)
    acc_b[:, 0:256] = heads_product(1)
    qf = query.astype(F32) * scale
    for d in range(1, NY):
        j = mod(y + d, NY)
        remote(st.at[j], st.at[j], s3.at[0], r3.at[j], y=j).wait_recv()

    cell = None
    for back in (0, 1):
        cum_t, top_in, numer, denom = inside[back]
        inter = cum_t + nm[2 + back : 3 + back, 0:1]
        top = jnp.maximum(inter, top_in)
        w_in, w_inter = jnp.exp(top_in - top), jnp.exp(inter - top)
        mat = st[:, 32 * back : 32 * back + 32].reshape(128, 128)
        numer = w_in * numer + (w_inter * scale) * jnp.dot(
            query, mat, preferred_element_type=F32
        )
        denom = w_in * denom + w_inter * jnp.sum(
            qf * nm[back : back + 1], axis=1, keepdims=True
        )
        part = numer / jnp.maximum(jnp.abs(denom), jnp.exp(-top))
        cell = part if cell is None else cell + part
    u = cell * gate_open
    norm = lax.rsqrt(jnp.mean(u * u, axis=1, keepdims=True) + EPS)
    mixes[0] = (u * norm * mgain[...]).astype(BF16)
    heads_start(0)
    heads_middle(0)
    heads_end(0)
    out[...] = (acc_b[:, 0:256] + heads_product(0)).astype(BF16)

    n = NZ * NY - 1
    every = pl.ds(0, n)
    remote(ga.at[every], ga.at[every], sa, az.at[0, 0], y=yd).wait_send()
    remote(gb.at[every], gb.at[every], sb, az.at[0, 0], y=yd).wait_send()
    for d in range(1, NY):
        remote(pk.at[0], p1.at[0], s1.at[d - 1], r1.at[0], y=yd).wait_send()
        remote(p3.at[0], st.at[0], s3.at[d - 1], r3.at[0], y=yd).wait_send()
    for d in range(1, NZ):
        remote(zp.at[0], p2.at[0], s2.at[d - 1], r2.at[0], z=zd).wait_send()
    to_next.wait_send()
    to_prev.wait_send()
    most = pl.ds(0, NT - 1)
    for i in (0, 1):
        src = full.at[i, most]
        remote(src, src, hs.at[i], hc.at[i, 0], tp=partner).wait_send()


def on_device(
    tokens,
    input_norm_gain,
    mq_weight,
    mk_weight,
    mv_weight,
    mo_weight,
    gate_weight,
    gate_bias,
    decay_extra,
    m_gain,
    aq_weight,
    ak_weight,
    av_weight,
    sink_logit,
    out_m_weight,
    out_a_weight,
):
    sds = jax.ShapeDtypeStruct
    dma = pltpu.SemaphoreType.DMA
    vm = pltpu.VMEM
    hbm = pl.BlockSpec(memory_space=pl.ANY)
    local = pl.BlockSpec(memory_space=pltpu.VMEM)
    n = NZ * NY
    return pl.pallas_call(
        layer_body,
        name="layer",
        out_shape=(sds((TOK, 256), BF16), sds((2, TOK), F32)),
        in_specs=[hbm, local, hbm, hbm, hbm, hbm, local, local, local, local]
        + [hbm, local, local, local, hbm, hbm],
        out_specs=[local] * 2,
        scratch_shapes=[
            vm((TOK, D), BF16),
            vm((A_ROWS, 128), BF16),
            vm((B_ROWS, 128), BF16),
            vm((n, A_ROWS, 128), BF16),
            vm((n, B_ROWS, 128), BF16),
            vm((NZ, TOK, 128), BF16),
            vm((TOK, 384), F32),
            vm((TOK, 512), F32),
            vm((TOK, 128), BF16),
            vm((2, WINDOW, 128), BF16),
            vm((TOK + 2 * WINDOW, 128), BF16),
            vm((NY, 80, 128), BF16),
            vm((NY, 80, 128), BF16),
            vm((2, 40, 128), BF16),
            vm((NZ, 40, 128), BF16),
            vm((NY, 64, 128), BF16),
            vm((NY, 64, 128), BF16),
            vm((NY, 8, 128), F32),
            vm((2, TOK, 128), BF16),
            vm((2, NT, TOK, 128), BF16),
            dma((10,)),
            dma((2,)),
            dma((2, HALF + 1)),
            dma((2, NZ)),
            dma((2, NZ)),
            dma((2, HALF + 1, NY)),
            dma((2,)),
            dma((2,)),
            dma((NY - 1,)),
            dma((NY,)),
            dma((NZ - 1,)),
            dma((NZ,)),
            dma((NY - 1,)),
            dma((NY,)),
            dma((2,)),
            dma((2,)),
            dma((2,)),
            dma((2, 2)),
            dma((2, 2)),
            dma((2, 5)),
        ],
        compiler_params=pltpu.CompilerParams(collective_id=0, has_side_effects=True),
    )(
        tokens,
        input_norm_gain[None],
        mq_weight,
        mk_weight,
        mv_weight,
        mo_weight,
        gate_weight[:, :, 0].T,
        gate_bias.T,
        decay_extra,
        m_gain[None],
        aq_weight,
        ak_weight,
        av_weight,
        sink_logit[None],
        out_m_weight,
        out_a_weight,
    )


def solution(mesh):
    split = Mesh(mesh.devices.reshape(NZ, NY, NT), ("z", "y", "tp"))
    return jax.shard_map(
        on_device,
        mesh=split,
        in_specs=(
            P(SP, None),
            P(),
            P(SP, "tp"),
            P(SP, "tp"),
            P(SP, "tp"),
            P(SP, "tp"),
            P(SP, None, "tp"),
            P(None, "tp"),
            P(None, "tp", SP),
            P("tp"),
            P(SP, "tp"),
            P(SP, "tp"),
            P(SP, "tp"),
            P("tp"),
            P(SP, "tp"),
            P(SP, "tp"),
        ),
        out_specs=(P(SP, "tp"), P("tp", SP)),
        check_vma=False,
    )
```

```python
import jax
import jax.numpy as jnp
from jax import lax
from jax.experimental import pallas as pl
from jax.experimental.pallas import tpu as pltpu
from jax.sharding import Mesh
from jax.sharding import PartitionSpec as P

M_DIM = 128
W_DIM = 64
WINDOW = 128
EPS = 1e-06
FLOOR_LOG = -1e30
NZ = 16
NY = 4
NX = 4
NT = 8
TOK = 256
D = 2048
HALF = NZ // 2
A_ROWS = 160
B_ROWS = 104
SP = ("z", "y")
MESH = pl.DeviceIdType.MESH
F32 = jnp.float32
BF16 = jnp.bfloat16
ACROSS = (((1,), (1,)), ((), ()))


def mod(a, n):
    return lax.rem(a + n, n)


def remote(src, dst, ssem, rsem, **where):
    return pltpu.make_async_remote_copy(
        src_ref=src,
        dst_ref=dst,
        send_sem=ssem,
        recv_sem=rsem,
        device_id=where,
        device_id_type=MESH,
    )


def log1p_of(e):
    poly = e * (
        1.0
        + e * (-0.5 + e * (1 / 3 + e * (-0.25 + e * (0.2 + e * (-1 / 6 + e * (1 / 7))))))
    )
    return jnp.where(e < 0.0625, poly, jnp.log(1.0 + e))


def log_sigmoid(x):
    return jnp.minimum(x, 0.0) - log1p_of(jnp.exp(-jnp.abs(x)))


def split3(x):
    hi = x.astype(BF16).astype(F32)
    mid = (x - hi).astype(BF16).astype(F32)
    return hi, mid, x - hi - mid


def joined(tail, at):
    return tail[at : at + 1] + tail[at + 1 : at + 2] + tail[at + 2 : at + 3]


def step_state(state, piece):
    peak, mat, norm = state
    p_peak, p_decay, p_mat, p_norm = piece
    new = jnp.maximum(peak + p_decay, p_peak)
    old_s, new_s = jnp.exp(peak + p_decay - new), jnp.exp(p_peak - new)
    return new, mat * old_s + p_mat * new_s, norm * old_s + p_norm * new_s


def empty_state():
    return (
        jnp.full((1, 128), FLOOR_LOG, F32),
        jnp.zeros((32, 128), F32),
        jnp.zeros((1, 128), F32),
    )


def layer_body(
    tok_hbm,
    gain,
    mq,
    mk,
    mv,
    mo,
    gate_t,
    bias,
    decay,
    mgain,
    aq_w,
    ak_w,
    av_w,
    sink,
    om,
    oa,
    out,
    logs,
    tok,
    wa,
    wb,
    ga,
    gb,
    normed,
    acc_a,
    acc_b,
    kv,
    halo,
    win,
    pk,
    p1,
    zp,
    p2,
    p3,
    st,
    keep,
    mixes,
    full,
    local_sem,
    ssem,
    az,
    ay,
    ah,
    bz,
    by,
    bh,
    s1,
    r1,
    s2,
    r2,
    s3,
    r3,
    sh,
    rh,
    hs,
    hx,
    hh,
    hc,
):
    z = lax.axis_index("z")
    y = lax.axis_index("y")
    t = lax.axis_index("tp")
    me = z * NY + y
    zu, zd = mod(z + 1, NZ), mod(z - 1, NZ)
    yu, yd = mod(y + 1, NY), mod(y - 1, NY)
    yo = mod(y + 2, NY)
    nxt, prv = mod(me + 1, NZ * NY), mod(me - 1, NZ * NY)
    zn, yn = lax.div(nxt, NY), lax.rem(nxt, NY)
    zq, yq = lax.div(prv, NY), lax.rem(prv, NY)
    x, c = lax.div(t, 2), lax.rem(t, 2)
    o = 1 - c
    xu, xd, xo = mod(x + 1, NX), mod(x - 1, NX), mod(x + 2, NX)
    partner, t_up, t_down, t_far = 2 * x + o, 2 * xu + c, 2 * xd + c, 2 * xo + c

    loads = []

    def load(src, dst):
        copy = pltpu.make_async_copy(src, dst, local_sem.at[len(loads)])
        copy.start()
        loads.append(copy)
        return copy

    for i, w in enumerate((mk, mv)):
        load(w, wb.at[32 * i : 32 * i + 32])
    for i, w in enumerate((mq, mo, aq_w)):
        load(w, wa.at[32 * i : 32 * i + 32])
    for i, w in enumerate((om, oa)):
        for part in (0, 1):
            at = 96 + 32 * i + 16 * part
            load(w.at[:, 128 * part : 128 * part + 128], wa.at[at : at + 16])
    tok_load = load(tok_hbm, tok)
    barrier = pltpu.get_barrier_semaphore()
    hello = [{"z": zu}, {"z": zd}, {"y": yu}, {"y": yd}, {"y": yo}]
    hello += [{"z": zn, "y": yn}, {"z": zq, "y": yq}]
    hello += [{"tp": partner}, {"tp": t_up}, {"tp": t_down}, {"tp": t_far}]
    for where in hello:
        pl.semaphore_signal(barrier, inc=1, device_id=where, device_id_type=MESH)
    wb[64:96] = jnp.concatenate([ak_w[...], av_w[...]], axis=1)
    gate_rows = jnp.concatenate([gate_t[...].astype(F32), jnp.zeros((4, 96), F32)], axis=1)
    gate_row = gate_rows[0:1]
    for g in range(1, 4):
        gate_row = gate_row + pltpu.roll(gate_rows[g : g + 1], 32 * g, 1)
    wb[96:104] = jnp.concatenate([gate_row, jnp.zeros((7, 128), F32)], axis=0).astype(BF16)
    for copy in loads[:-1]:
        copy.wait()
    pl.semaphore_wait(barrier, len(hello))

    sa, sb = ssem.at[0], ssem.at[1]

    parts = (pl.ds(0, A_ROWS // 2), pl.ds(A_ROWS // 2, A_ROWS // 2))

    def a_up(ref, slot, s, h):
        return remote(ref.at[parts[h]], ga.at[slot, parts[h]], sa, az.at[0, s, h], z=zu)

    def a_down(ref, slot, s, h):
        return remote(ref.at[parts[h]], ga.at[slot, parts[h]], sa, az.at[1, s, h], z=zd)

    def a_side(src, zz):
        slot = zz * NY + y
        remote(src, ga.at[slot], sa, ay.at[0, zz], y=yu).start()
        remote(src, ga.at[slot], sa, ay.at[1, zz], y=yd).start()

    def b_up(src, slot, s, j):
        return remote(src, gb.at[slot], sb, bz.at[0, s, j], z=zu)

    def b_down(src, slot, s, j):
        return remote(src, gb.at[slot], sb, bz.at[1, s, j], z=zd)

    remote(wb, gb.at[me], sb, by.at[0], y=yu).start()
    remote(wb, gb.at[me], sb, by.at[1], y=yd).start()
    b_up(wb, me, 1, y).start()
    b_down(wb, me, 1, y).start()
    for h in (0, 1):
        a_up(wa, me, 1, h).start()
        a_down(wa, me, 1, h).start()
    ga[me] = wa[...]
    gb[me] = wb[...]

    tok_load.wait()
    xs = tok[...].astype(F32)
    xs = xs * lax.rsqrt(jnp.mean(xs * xs, axis=-1, keepdims=True) + EPS) * gain[...]
    for i in range(NZ):
        normed[i] = xs[:, 128 * i : 128 * i + 128].astype(BF16)
    acc_a[...] = jnp.zeros_like(acc_a)
    acc_b[...] = jnp.zeros_like(acc_b)

    slot_d, slot_u, slot_o = z * NY + yd, z * NY + yu, z * NY + yo
    lo, hi = pl.ds(0, A_ROWS // 2), pl.ds(A_ROWS // 2, A_ROWS // 2)
    blo, bhi = pl.ds(0, 48), pl.ds(48, 56)
    remote(wb, gb.at[slot_d], sb, by.at[0], y=yd).wait_recv()
    remote(gb.at[slot_d, blo], gb.at[slot_d, blo], sb, bh.at[0], y=yu).start()
    b_up(gb.at[slot_d], slot_d, 1, yd).start()
    b_down(gb.at[slot_d], slot_d, 1, yd).start()
    remote(wb, gb.at[slot_u], sb, by.at[1], y=yd).wait_recv()
    remote(gb.at[slot_u, bhi], gb.at[slot_u, bhi], sb, bh.at[1], y=yd).start()
    b_up(gb.at[slot_u], slot_u, 1, yu).start()
    b_down(gb.at[slot_u], slot_u, 1, yu).start()
    a_side(wa, z)

    def opposite():
        remote(gb.at[slot_o, blo], gb.at[slot_o, blo], sb, bh.at[0], y=yd).wait_recv()
        remote(gb.at[slot_o, bhi], gb.at[slot_o, bhi], sb, bh.at[1], y=yd).wait_recv()
        b_up(gb.at[slot_o], slot_o, 1, yo).start()
        b_down(gb.at[slot_o], slot_o, 1, yo).start()

    def side_forward(zz):
        sd, su = zz * NY + yd, zz * NY + yu
        remote(ga.at[sd], ga.at[sd], sa, ay.at[0, zz], y=yd).wait_recv()
        remote(ga.at[sd, lo], ga.at[sd, lo], sa, ah.at[0, zz], y=yu).start()
        remote(ga.at[su], ga.at[su], sa, ay.at[1, zz], y=yd).wait_recv()
        remote(ga.at[su, hi], ga.at[su, hi], sa, ah.at[1, zz], y=yd).start()

    spread = lax.broadcasted_iota(jnp.int32, (32, 128), 0) == lax.rem(
        lax.broadcasted_iota(jnp.int32, (32, 128), 1), 32
    )

    def stacked(ref, zz, at):
        return jnp.concatenate([ref[zz * NY + j, at : at + 32] for j in range(NY)], axis=0)

    def level_a(zz):
        so = zz * NY + yo
        remote(ga.at[so, lo], ga.at[so, lo], sa, ah.at[0, zz], y=yd).wait_recv()
        remote(ga.at[so, hi], ga.at[so, hi], sa, ah.at[1, zz], y=yd).wait_recv()
        rows = normed[zz]
        w = jnp.concatenate([stacked(ga, zz, 0), stacked(ga, zz, 32)], axis=1)
        acc_a[:, 0:256] += jnp.dot(rows, w, preferred_element_type=F32)
        acc_a[:, 256:384] += jnp.dot(rows, stacked(ga, zz, 64), preferred_element_type=F32)

    def level_b(zz):
        rows = normed[zz]
        w = jnp.concatenate([stacked(gb, zz, 0), stacked(gb, zz, 32)], axis=1)
        acc_b[:, 0:256] += jnp.dot(rows, w, preferred_element_type=F32)
        g = jnp.concatenate(
            [
                jnp.where(
                    spread, gb[zz * NY + j, 96:104].astype(F32)[0:1], 0.0
                ).astype(BF16)
                for j in range(NY)
            ],
            axis=0,
        )
        w = jnp.concatenate([stacked(gb, zz, 64), g], axis=1)
        acc_b[:, 256:512] += jnp.dot(rows, w, preferred_element_type=F32)

    def both(d, what):
        what(mod(z - d, NZ))

        @pl.when((d > 0) & (d < HALF))
        def _():
            what(mod(z + d, NZ))

    def b_step(s, j, far_up):
        sl, sl2 = mod(z - s, NZ) * NY + j, mod(z + s, NZ) * NY + j
        up_from, down_from = (HALF, HALF - 1) if far_up else (HALF - 1, HALF)

        @pl.when(s <= up_from)
        def _():
            b_up(gb.at[sl], sl, s, j).wait_recv()

            @pl.when(s < up_from)
            def _():
                b_up(gb.at[sl], sl, s + 1, j).start()

        @pl.when(s <= down_from)
        def _():
            b_down(gb.at[sl2], sl2, s, j).wait_recv()

            @pl.when(s < down_from)
            def _():
                b_down(gb.at[sl2], sl2, s + 1, j).start()

    def a_step(s):
        z_lo, z_hi = mod(z - s, NZ), mod(z + s, NZ)
        slot, slot2 = z_lo * NY + y, z_hi * NY + y
        for h in (0, 1):
            a_up(ga.at[slot], slot, s, h).wait_recv()

            @pl.when(s < HALF)
            def _():
                a_up(ga.at[slot], slot, s + 1, h).start()
                a_down(ga.at[slot2], slot2, s, h).wait_recv()

                @pl.when(s < HALF - 1)
                def _():
                    a_down(ga.at[slot2], slot2, s + 1, h).start()

        a_side(ga.at[slot], z_lo)

        @pl.when(s < HALF)
        def _():
            a_side(ga.at[slot2], z_hi)

    def above(d, what):
        @pl.when(d > 0)
        def _():
            what(mod(z + d, NZ))

    b_step(1, y, True)
    opposite()
    a_step(1)
    b_step(1, yd, True)
    b_step(1, yu, False)

    def step(s, carry):
        b_step(s - 1, yo, False)
        b_step(s, y, True)
        level_b(mod(z - s + 2, NZ))
        a_step(s)
        above(s - 2, level_b)
        b_step(s, yd, True)

        @pl.when(s >= 4)
        def _():
            level_a(mod(z - s + 4, NZ))

        b_step(s, yu, False)
        both(s - 2, side_forward)
        above(s - 4, level_a)
        return carry

    lax.fori_loop(2, HALF, step, 0)
    b_step(HALF - 1, yo, False)
    b_step(HALF, y, True)
    both(HALF - 2, level_b)
    b_step(HALF, yd, True)
    b_step(HALF, yu, False)
    both(HALF - 2, side_forward)
    both(HALF - 1, level_b)
    b_step(HALF, yo, False)
    level_b(mod(z - HALF, NZ))

    kv[...] = acc_b[:, 256:384].astype(BF16)
    first, last = pl.ds(0, WINDOW), pl.ds(TOK - WINDOW, WINDOW)
    to_next = remote(kv.at[last], halo.at[0], sh.at[0], rh.at[0], z=zn, y=yn)
    to_prev = remote(kv.at[first], halo.at[1], sh.at[1], rh.at[1], z=zq, y=yq)
    gt = jnp.sum(jnp.transpose(acc_b[:, 384:512]).reshape(4, 32, TOK), axis=1)
    in_f, in_b = gt[0:1] + bias[0:1, 0:1], gt[2:3] + bias[0:1, 2:3]
    lf_f = log_sigmoid(gt[1:2] + bias[0:1, 1:2]) + decay[0]
    lf_b = log_sigmoid(gt[3:4] + bias[0:1, 3:4]) + decay[1]
    to_next.start()
    to_prev.start()
    lane = lax.broadcasted_iota(jnp.int32, (1, TOK), 1)
    cum, rev = lf_f, lf_b
    k = 1
    while k < TOK:
        cum = cum + jnp.where(lane >= k, pltpu.roll(cum, k, 1), 0.0)
        rev = rev + jnp.where(lane < TOK - k, pltpu.roll(rev, TOK - k, 1), 0.0)
        k *= 2
    tot_f = jnp.max(jnp.where(lane == TOK - 1, cum, -jnp.inf), axis=1, keepdims=True)
    tot_b = jnp.max(jnp.where(lane == 0, rev, -jnp.inf), axis=1, keepdims=True)
    end_f = tot_f - cum + in_f
    end_b = tot_b - rev + in_b
    m_f = jnp.max(end_f, axis=1, keepdims=True)
    m_b = jnp.max(end_b, axis=1, keepdims=True)
    w_f, w_b = jnp.exp(end_f - m_f), jnp.exp(end_b - m_b)
    rows = jnp.concatenate([in_f, cum, in_b, rev, w_f, w_b, jnp.zeros((2, TOK), F32)], axis=0)
    cols = jnp.transpose(jnp.concatenate([rows, jnp.zeros((120, TOK), F32)], axis=0))
    key, value = acc_b[:, 0:128].astype(BF16), acc_b[:, 128:256].astype(BF16)
    val = value.astype(F32)
    tail, mats = [], []
    norms = jnp.dot(rows.astype(BF16), key, preferred_element_type=F32)
    for i in (4, 5):
        wv = (cols[:, i : i + 1] * val).astype(BF16)
        mats.append(
            lax.dot_general(key, wv, (((0,), (0,)), ((), ())), preferred_element_type=F32)
        )
        tail.append(norms[i : i + 1])
    for v in (m_f, tot_f, m_b, tot_b):
        tail.extend(jnp.broadcast_to(p, (1, 128)) for p in split3(v))
    tail.append(jnp.zeros((2, 128), F32))
    summary_tail = jnp.concatenate(tail, axis=0).astype(BF16)
    for q in range(NY):
        pk[q, 0:32] = mats[0][q * 32 : q * 32 + 32].astype(BF16)
        pk[q, 32:64] = mats[1][q * 32 : q * 32 + 32].astype(BF16)
        pk[q, 64:80] = summary_tail

    for d in (2, 1, 3):
        j = mod(y + d, NY)
        remote(pk.at[j], p1.at[y], s1.at[d - 1], r1.at[y], y=j).start()
    p1[y] = pk[y]

    a_step(HALF)
    both(HALF - 4, level_a)
    both(HALF - 1, side_forward)
    both(HALF - 3, level_a)

    for d in range(1, NY):
        j = mod(y + d, NY)
        remote(p1.at[j], p1.at[j], s1.at[0], r1.at[j], y=j).wait_recv()

    def local_piece(j, back):
        ends = p1[j, 64:80].astype(F32)
        if back:
            return joined(ends, 8), joined(ends, 11), p1[j, 32:64].astype(F32), ends[1:2]
        return joined(ends, 2), joined(ends, 5), p1[j, 0:32].astype(F32), ends[0:1]

    for back in (0, 1):
        state, total_decay = empty_state(), jnp.zeros((1, 128), F32)
        for j in reversed(range(NY)) if back else range(NY):
            piece = local_piece(j, back)
            state = step_state(state, piece)
            total_decay = total_decay + piece[1]
        zp[back, 0:32] = state[1].astype(BF16)
        zp[back, 32:40] = jnp.concatenate(
            [state[2], *split3(state[0]), *split3(total_decay), jnp.zeros((1, 128), F32)],
            axis=0,
        ).astype(BF16)
    for d in (8, 7, 9, 6, 10, 5, 11, 4, 12, 3, 13, 2, 14, 1, 15):
        remote(
            zp.at[lax.div(z + d, NZ)],
            p2.at[z],
            s2.at[d - 1],
            r2.at[z],
            z=mod(z + d, NZ),
        ).start()

    side_forward(mod(z - HALF, NZ))
    both(HALF - 2, level_a)
    both(HALF - 1, level_a)
    level_a(mod(z - HALF, NZ))
    query = acc_a[:, 0:128].astype(BF16)
    gate_in = acc_a[:, 128:256].astype(BF16)
    a_query = acc_a[:, 256:384].astype(BF16).astype(F32)

    mid, end = pl.ds(0, TOK // 2), pl.ds(TOK // 2, TOK // 2)

    def heads_start(i):
        mix, dst = mixes.at[i], full.at[i]
        for n, part in enumerate((mid, end)):
            remote(mix.at[part], dst.at[t, part], hs.at[i], hh.at[i, n], tp=t_far).start()
        remote(mix, dst.at[t], hs.at[i], hx.at[i, 0], tp=t_up).start()
        remote(mix, dst.at[t], hs.at[i], hx.at[i, 1], tp=t_down).start()
        remote(mix, dst.at[t], hs.at[i], hc.at[i, 0], tp=partner).start()
        full[i, t] = mixes[i]

    def heads_end(i):
        mix, dst = mixes.at[i], full.at[i]
        for n, part in enumerate((mid, end)):
            src = dst.at[t_far, part]
            remote(src, src, hs.at[i], hh.at[i, n], tp=t_up).wait_recv()
            remote(src, src, hs.at[i], hc.at[i, 3 + n], tp=partner).start()
        for n, slot in enumerate((t_down, t_up)):
            src = dst.at[slot]
            remote(mix, src, hs.at[i], hx.at[i, n], tp=t_up).wait_recv()
            remote(src, src, hs.at[i], hc.at[i, 1 + n], tp=partner).start()
        for n, part in enumerate((mid, end)):
            src = dst.at[2 * xo + o, part]
            remote(src, src, hs.at[i], hc.at[i, 3 + n], tp=partner).wait_recv()
        remote(mix, dst.at[partner], hs.at[i], hc.at[i, 0], tp=partner).wait_recv()
        remote(mix, dst.at[2 * xd + o], hs.at[i], hc.at[i, 1], tp=partner).wait_recv()
        remote(mix, dst.at[2 * xu + o], hs.at[i], hc.at[i, 2], tp=partner).wait_recv()

    def heads_product(i):
        total = None
        for n in range(NT):
            w = jnp.concatenate(
                [
                    ga[8 * n : 8 * n + 8, at : at + 16].reshape(128, 128)
                    for at in (96 + 32 * i, 112 + 32 * i)
                ],
                axis=1,
            )
            term = jnp.dot(full[i, n], w, preferred_element_type=F32)
            total = term if total is None else total + term
        return total

    to_next.wait_recv()
    to_prev.wait_recv()
    win[0:WINDOW] = halo[0]
    win[WINDOW : WINDOW + TOK] = kv[...]
    win[WINDOW + TOK :] = halo[1]
    low = lax.broadcasted_iota(jnp.int32, (WINDOW, 128), 1) < W_DIM
    two = lax.broadcasted_iota(jnp.int32, (2 * WINDOW, 3 * WINDOW), 0)
    col = lax.broadcasted_iota(jnp.int32, (2 * WINDOW, 3 * WINDOW), 1)
    off = col - jnp.where(two >= WINDOW, two - WINDOW, two)
    in_window = (off >= 0) & (off <= 2 * WINDOW)
    second = lax.broadcasted_iota(jnp.int32, (2 * WINDOW, 1), 0) >= WINDOW
    sink_col = jnp.where(second, sink[0:1, 1:2], sink[0:1, 0:1])
    for b in range(2):
        block = pl.ds(b * WINDOW, WINDOW)
        qb = a_query[b * WINDOW : b * WINDOW + WINDOW]
        q0 = jnp.where(low, qb, 0.0)
        q1 = jnp.where(low, pltpu.roll(qb, W_DIM, 1), 0.0)
        qq = jnp.concatenate([q0, q1], axis=0).astype(BF16)
        keys = win[b * WINDOW : b * WINDOW + 3 * WINDOW]
        scores = lax.dot_general(qq, keys, ACROSS, preferred_element_type=F32) * W_DIM**-0.5
        place = me * TOK + (b - 1) * WINDOW + col
        usable = in_window & (place >= 0) & (place < NZ * NY * TOK)
        scores = jnp.where(usable, scores, -jnp.inf)
        peak = jnp.maximum(sink_col, jnp.max(scores, axis=1, keepdims=True))
        weights = jnp.exp(scores - peak)
        tot = jnp.exp(sink_col - peak) + jnp.sum(weights, axis=1, keepdims=True)
        res = jnp.dot(weights.astype(BF16), keys, preferred_element_type=F32) / tot
        mixes[1, block] = jnp.where(
            low, pltpu.roll(res[0:WINDOW], W_DIM, 1), res[WINDOW:]
        ).astype(BF16)
        logt = jnp.transpose(jnp.broadcast_to(peak + jnp.log(tot), (2 * WINDOW, 128)))
        logs[0:1, block] = logt[0:1, 0:WINDOW]
        logs[1:2, block] = logt[0:1, WINDOW:]
    heads_start(1)
    gate_open = 1.0 / (1.0 + jnp.exp(-gate_in.astype(F32)))

    scale = M_DIM**-0.5
    dots = lax.dot_general(query, key, ACROSS, preferred_element_type=F32) * scale
    ti = lax.broadcasted_iota(jnp.int32, (TOK, TOK), 0)
    si = lax.broadcasted_iota(jnp.int32, (TOK, TOK), 1)
    inside = []
    for back in (0, 1):
        cum_t = cols[:, 2 * back + 1 : 2 * back + 2]
        log_in = rows[2 * back : 2 * back + 1] - rows[2 * back + 1 : 2 * back + 2]
        usable = (si >= ti) if back else (si <= ti)
        log_w = jnp.where(usable, cum_t + log_in, -jnp.inf)
        top = jnp.max(log_w, axis=1, keepdims=True)
        scores = dots * jnp.exp(log_w - top)
        numer = jnp.dot(scores.astype(BF16), value, preferred_element_type=F32)
        denom = jnp.sum(scores, axis=1, keepdims=True)
        inside.append((cum_t, top, numer, denom))


    for d in range(1, NZ):
        j = mod(z + d, NZ)
        remote(p2.at[j], p2.at[j], s2.at[0], r2.at[j], z=j).wait_recv()

    def far(i, state):
        ends = p2[i, 32:40].astype(F32)
        return step_state(
            state, (joined(ends, 1), joined(ends, 4), p2[i, 0:32].astype(F32), ends[0:1])
        )

    fwd = lax.fori_loop(0, z, far, empty_state())
    bwd = lax.fori_loop(0, NZ - 1 - z, lambda i, s: far(NZ - 1 - i, s), empty_state())
    for j in range(NY):
        p3[j, 0:32] = fwd[1].astype(BF16)
        keep[j, 0:1] = fwd[2]
        keep[j, 2:3] = fwd[0]
        fwd = step_state(fwd, local_piece(j, 0))
    for j in reversed(range(NY)):
        p3[j, 32:64] = bwd[1].astype(BF16)
        keep[j, 1:2] = bwd[2]
        keep[j, 3:4] = bwd[0]
        bwd = step_state(bwd, local_piece(j, 1))
    for d in (2, 1, 3):
        j = mod(y + d, NY)
        remote(p3.at[j], st.at[y], s3.at[d - 1], r3.at[y], y=j).start()
    st[y] = p3[y]
    nm = keep[y]
    heads_end(1)
    acc_b[:, 0:256] = heads_product(1)
    qf = query.astype(F32) * scale
    for d in range(1, NY):
        j = mod(y + d, NY)
        remote(st.at[j], st.at[j], s3.at[0], r3.at[j], y=j).wait_recv()

    cell = None
    for back in (0, 1):
        cum_t, top_in, numer, denom = inside[back]
        inter = cum_t + nm[2 + back : 3 + back, 0:1]
        top = jnp.maximum(inter, top_in)
        w_in, w_inter = jnp.exp(top_in - top), jnp.exp(inter - top)
        mat = st[:, 32 * back : 32 * back + 32].reshape(128, 128)
        numer = w_in * numer + (w_inter * scale) * jnp.dot(
            query, mat, preferred_element_type=F32
        )
        denom = w_in * denom + w_inter * jnp.sum(
            qf * nm[back : back + 1], axis=1, keepdims=True
        )
        part = numer / jnp.maximum(jnp.abs(denom), jnp.exp(-top))
        cell = part if cell is None else cell + part
    u = cell * gate_open
    norm = lax.rsqrt(jnp.mean(u * u, axis=1, keepdims=True) + EPS)
    mixes[0] = (u * norm * mgain[...]).astype(BF16)
    heads_start(0)
    heads_end(0)
    out[...] = (acc_b[:, 0:256] + heads_product(0)).astype(BF16)

    n = NZ * NY - 1
    every = pl.ds(0, n)
    remote(ga.at[every], ga.at[every], sa, ah.at[0, 0], y=yd).wait_send()
    remote(gb.at[every], gb.at[every], sb, ah.at[0, 0], y=yd).wait_send()
    for d in range(1, NY):
        remote(pk.at[0], p1.at[0], s1.at[d - 1], r1.at[0], y=yd).wait_send()
        remote(p3.at[0], st.at[0], s3.at[d - 1], r3.at[0], y=yd).wait_send()
    for d in range(1, NZ):
        remote(zp.at[0], p2.at[0], s2.at[d - 1], r2.at[0], z=zd).wait_send()
    to_next.wait_send()
    to_prev.wait_send()
    most = pl.ds(0, NT - 1)
    for i in (0, 1):
        src = full.at[i, most]
        remote(src, src, hs.at[i], hc.at[i, 0], tp=partner).wait_send()


def on_device(
    tokens,
    input_norm_gain,
    mq_weight,
    mk_weight,
    mv_weight,
    mo_weight,
    gate_weight,
    gate_bias,
    decay_extra,
    m_gain,
    aq_weight,
    ak_weight,
    av_weight,
    sink_logit,
    out_m_weight,
    out_a_weight,
):
    sds = jax.ShapeDtypeStruct
    dma = pltpu.SemaphoreType.DMA
    vm = pltpu.VMEM
    hbm = pl.BlockSpec(memory_space=pl.ANY)
    local = pl.BlockSpec(memory_space=pltpu.VMEM)
    n = NZ * NY
    return pl.pallas_call(
        layer_body,
        name="layer",
        out_shape=(sds((TOK, 256), BF16), sds((2, TOK), F32)),
        in_specs=[hbm, local, hbm, hbm, hbm, hbm, local, local, local, local]
        + [hbm, local, local, local, hbm, hbm],
        out_specs=[local] * 2,
        scratch_shapes=[
            vm((TOK, D), BF16),
            vm((A_ROWS, 128), BF16),
            vm((B_ROWS, 128), BF16),
            vm((n, A_ROWS, 128), BF16),
            vm((n, B_ROWS, 128), BF16),
            vm((NZ, TOK, 128), BF16),
            vm((TOK, 384), F32),
            vm((TOK, 512), F32),
            vm((TOK, 128), BF16),
            vm((2, WINDOW, 128), BF16),
            vm((TOK + 2 * WINDOW, 128), BF16),
            vm((NY, 80, 128), BF16),
            vm((NY, 80, 128), BF16),
            vm((2, 40, 128), BF16),
            vm((NZ, 40, 128), BF16),
            vm((NY, 64, 128), BF16),
            vm((NY, 64, 128), BF16),
            vm((NY, 8, 128), F32),
            vm((2, TOK, 128), BF16),
            vm((2, NT, TOK, 128), BF16),
            dma((10,)),
            dma((2,)),
            dma((2, HALF + 1, 2)),
            dma((2, NZ)),
            dma((2, NZ)),
            dma((2, HALF + 1, NY)),
            dma((2,)),
            dma((2,)),
            dma((NY - 1,)),
            dma((NY,)),
            dma((NZ - 1,)),
            dma((NZ,)),
            dma((NY - 1,)),
            dma((NY,)),
            dma((2,)),
            dma((2,)),
            dma((2,)),
            dma((2, 2)),
            dma((2, 2)),
            dma((2, 5)),
        ],
        compiler_params=pltpu.CompilerParams(collective_id=0, has_side_effects=True),
    )(
        tokens,
        input_norm_gain[None],
        mq_weight,
        mk_weight,
        mv_weight,
        mo_weight,
        gate_weight[:, :, 0].T,
        gate_bias.T,
        decay_extra,
        m_gain[None],
        aq_weight,
        ak_weight,
        av_weight,
        sink_logit[None],
        out_m_weight,
        out_a_weight,
    )


def solution(mesh):
    split = Mesh(mesh.devices.reshape(NZ, NY, NT), ("z", "y", "tp"))
    return jax.shard_map(
        on_device,
        mesh=split,
        in_specs=(
            P(SP, None),
            P(),
            P(SP, "tp"),
            P(SP, "tp"),
            P(SP, "tp"),
            P(SP, "tp"),
            P(SP, None, "tp"),
            P(None, "tp"),
            P(None, "tp", SP),
            P("tp"),
            P(SP, "tp"),
            P(SP, "tp"),
            P(SP, "tp"),
            P("tp"),
            P(SP, "tp"),
            P(SP, "tp"),
        ),
        out_specs=(P(SP, "tp"), P("tp", SP)),
        check_vma=False,
    )
```

```python
import jax
import jax.numpy as jnp
from jax import lax
from jax.experimental import pallas as pl
from jax.experimental.pallas import tpu as pltpu
from jax.sharding import Mesh
from jax.sharding import PartitionSpec as P

M_DIM = 128
W_DIM = 64
WINDOW = 128
EPS = 1e-06
FLOOR_LOG = -1e30
NZ = 16
NY = 4
NX = 4
NT = 8
TOK = 256
D = 2048
HALF = NZ // 2
A_ROWS = 160
B_ROWS = 104
SP = ("z", "y")
MESH = pl.DeviceIdType.MESH
F32 = jnp.float32
BF16 = jnp.bfloat16
ACROSS = (((1,), (1,)), ((), ()))


def mod(a, n):
    return lax.rem(a + n, n)


def remote(src, dst, ssem, rsem, **where):
    return pltpu.make_async_remote_copy(
        src_ref=src,
        dst_ref=dst,
        send_sem=ssem,
        recv_sem=rsem,
        device_id=where,
        device_id_type=MESH,
    )


def log1p_of(e):
    poly = e * (
        1.0
        + e * (-0.5 + e * (1 / 3 + e * (-0.25 + e * (0.2 + e * (-1 / 6 + e * (1 / 7))))))
    )
    return jnp.where(e < 0.0625, poly, jnp.log(1.0 + e))


def log_sigmoid(x):
    return jnp.minimum(x, 0.0) - log1p_of(jnp.exp(-jnp.abs(x)))


def split3(x):
    hi = x.astype(BF16).astype(F32)
    mid = (x - hi).astype(BF16).astype(F32)
    return hi, mid, x - hi - mid


def joined(tail, at):
    return tail[at : at + 1] + tail[at + 1 : at + 2] + tail[at + 2 : at + 3]


def step_state(state, piece):
    peak, mat, norm = state
    p_peak, p_decay, p_mat, p_norm = piece
    new = jnp.maximum(peak + p_decay, p_peak)
    old_s, new_s = jnp.exp(peak + p_decay - new), jnp.exp(p_peak - new)
    return new, mat * old_s + p_mat * new_s, norm * old_s + p_norm * new_s


def empty_state():
    return (
        jnp.full((1, 128), FLOOR_LOG, F32),
        jnp.zeros((32, 128), F32),
        jnp.zeros((1, 128), F32),
    )


def layer_body(
    tok_hbm,
    gain_hbm,
    mq,
    mk,
    mv,
    mo,
    gate_hbm,
    bias_hbm,
    decay_hbm,
    mgain_hbm,
    aq_w,
    ak_hbm,
    av_hbm,
    sink_hbm,
    om,
    oa,
    out,
    logs,
    gain,
    gate_t,
    bias,
    decay,
    mgain,
    ak_w,
    av_w,
    sink,
    tok,
    wa,
    wb,
    ga,
    gb,
    normed,
    acc_a,
    acc_b,
    kv,
    halo,
    win,
    pk,
    p1,
    zp,
    p2,
    p3,
    st,
    keep,
    mixes,
    full,
    local_sem,
    ssem,
    az,
    ay,
    ah,
    bz,
    by,
    bh,
    s1,
    r1,
    s2,
    r2,
    s3,
    r3,
    sh,
    rh,
    hs,
    hx,
    hh,
    hc,
):
    z = lax.axis_index("z")
    y = lax.axis_index("y")
    t = lax.axis_index("tp")
    me = z * NY + y
    zu, zd = mod(z + 1, NZ), mod(z - 1, NZ)
    yu, yd = mod(y + 1, NY), mod(y - 1, NY)
    yo = mod(y + 2, NY)
    nxt, prv = mod(me + 1, NZ * NY), mod(me - 1, NZ * NY)
    zn, yn = lax.div(nxt, NY), lax.rem(nxt, NY)
    zq, yq = lax.div(prv, NY), lax.rem(prv, NY)
    x, c = lax.div(t, 2), lax.rem(t, 2)
    o = 1 - c
    xu, xd, xo = mod(x + 1, NX), mod(x - 1, NX), mod(x + 2, NX)
    partner, t_up, t_down, t_far = 2 * x + o, 2 * xu + c, 2 * xd + c, 2 * xo + c

    loads = []

    def load(src, dst):
        copy = pltpu.make_async_copy(src, dst, local_sem.at[2 + len(loads)])
        copy.start()
        loads.append(copy)
        return copy

    early = [load(ak_hbm, ak_w), load(av_hbm, av_w), load(gate_hbm, gate_t)]
    for i, w in enumerate((mk, mv)):
        pltpu.make_async_copy(w, wb.at[32 * i : 32 * i + 32], local_sem.at[0]).start()
    for i, w in enumerate((mq, mo, aq_w)):
        pltpu.make_async_copy(w, wa.at[32 * i : 32 * i + 32], local_sem.at[1]).start()
    for i, w in enumerate((om, oa)):
        for part in (0, 1):
            at = 96 + 32 * i + 16 * part
            src = w.at[:, 128 * part : 128 * part + 128]
            pltpu.make_async_copy(src, wa.at[at : at + 16], local_sem.at[1]).start()
    late = [load(tok_hbm, tok), load(gain_hbm, gain), load(bias_hbm, bias)]
    late += [load(decay_hbm, decay), load(mgain_hbm, mgain), load(sink_hbm, sink)]
    barrier = pltpu.get_barrier_semaphore()
    hello = [{"z": zu}, {"z": zd}, {"y": yu}, {"y": yd}, {"y": yo}]
    hello += [{"z": zn, "y": yn}, {"z": zq, "y": yq}]
    hello += [{"tp": partner}, {"tp": t_up}, {"tp": t_down}, {"tp": t_far}]
    for where in hello:
        pl.semaphore_signal(barrier, inc=1, device_id=where, device_id_type=MESH)
    for copy in early:
        copy.wait()
    wb[64:96] = jnp.concatenate([ak_w[...], av_w[...]], axis=1)
    gate_rows = jnp.concatenate([gate_t[...].astype(F32), jnp.zeros((4, 96), F32)], axis=1)
    gate_row = gate_rows[0:1]
    for g in range(1, 4):
        gate_row = gate_row + pltpu.roll(gate_rows[g : g + 1], 32 * g, 1)
    wb[96:104] = jnp.concatenate([gate_row, jnp.zeros((7, 128), F32)], axis=0).astype(BF16)
    two_weights = wb.at[0:64]
    pltpu.make_async_copy(two_weights, two_weights, local_sem.at[0]).wait()
    pltpu.make_async_copy(wa, wa, local_sem.at[1]).wait()
    pl.semaphore_wait(barrier, len(hello))

    sa, sb = ssem.at[0], ssem.at[1]

    parts = (pl.ds(0, A_ROWS // 2), pl.ds(A_ROWS // 2, A_ROWS // 2))

    def a_up(ref, slot, s, h):
        return remote(ref.at[parts[h]], ga.at[slot, parts[h]], sa, az.at[0, s - 1, h], z=zu)

    def a_down(ref, slot, s, h):
        return remote(ref.at[parts[h]], ga.at[slot, parts[h]], sa, az.at[1, s - 1, h], z=zd)

    def a_side(src, zz):
        slot = zz * NY + y
        remote(src, ga.at[slot], sa, ay.at[0, zz], y=yu).start()
        remote(src, ga.at[slot], sa, ay.at[1, zz], y=yd).start()

    def b_up(src, slot, s, j):
        return remote(src, gb.at[slot], sb, bz.at[0, s - 1, j], z=zu)

    def b_down(src, slot, s, j):
        return remote(src, gb.at[slot], sb, bz.at[1, s - 1, j], z=zd)

    remote(wb, gb.at[me], sb, bh.at[0], y=yo).start()
    remote(wb, gb.at[me], sb, by.at[0], y=yu).start()
    remote(wb, gb.at[me], sb, by.at[1], y=yd).start()
    b_up(wb, me, 1, y).start()
    b_down(wb, me, 1, y).start()
    for h in (0, 1):
        a_up(wa, me, 1, h).start()
        a_down(wa, me, 1, h).start()
    ga[me] = wa[...]
    gb[me] = wb[...]

    for copy in late:
        copy.wait()
    xs = tok[...].astype(F32)
    xs = xs * lax.rsqrt(jnp.mean(xs * xs, axis=-1, keepdims=True) + EPS) * gain[...]
    for i in range(NZ):
        normed[i] = xs[:, 128 * i : 128 * i + 128].astype(BF16)
    acc_a[...] = jnp.zeros_like(acc_a)
    acc_b[...] = jnp.zeros_like(acc_b)

    slot_d, slot_u, slot_o = z * NY + yd, z * NY + yu, z * NY + yo
    lo, hi = pl.ds(0, A_ROWS // 2), pl.ds(A_ROWS // 2, A_ROWS // 2)
    remote(wb, gb.at[slot_d], sb, by.at[0], y=yd).wait_recv()
    b_up(gb.at[slot_d], slot_d, 1, yd).start()
    b_down(gb.at[slot_d], slot_d, 1, yd).start()
    remote(wb, gb.at[slot_u], sb, by.at[1], y=yd).wait_recv()
    b_up(gb.at[slot_u], slot_u, 1, yu).start()
    b_down(gb.at[slot_u], slot_u, 1, yu).start()
    a_side(wa, z)

    def opposite():
        remote(wb, gb.at[slot_o], sb, bh.at[0], y=yd).wait_recv()
        b_up(gb.at[slot_o], slot_o, 1, yo).start()
        b_down(gb.at[slot_o], slot_o, 1, yo).start()

    def side_forward(zz):
        sd, su = zz * NY + yd, zz * NY + yu
        remote(ga.at[sd], ga.at[sd], sa, ay.at[0, zz], y=yd).wait_recv()
        remote(ga.at[sd, lo], ga.at[sd, lo], sa, ah.at[zz], y=yu).start()
        remote(ga.at[su], ga.at[su], sa, ay.at[1, zz], y=yd).wait_recv()
        remote(ga.at[su, hi], ga.at[su, hi], sa, ah.at[zz], y=yd).start()

    spread = lax.broadcasted_iota(jnp.int32, (32, 128), 0) == lax.rem(
        lax.broadcasted_iota(jnp.int32, (32, 128), 1), 32
    )

    def stacked(ref, zz, at):
        return jnp.concatenate([ref[zz * NY + j, at : at + 32] for j in range(NY)], axis=0)

    def level_a(zz):
        so = zz * NY + yo
        remote(ga.at[so], ga.at[so], sa, ah.at[zz], y=yd).wait_recv()
        rows = normed[zz]
        w = jnp.concatenate([stacked(ga, zz, 0), stacked(ga, zz, 32)], axis=1)
        acc_a[:, 0:256] += jnp.dot(rows, w, preferred_element_type=F32)
        acc_a[:, 256:384] += jnp.dot(rows, stacked(ga, zz, 64), preferred_element_type=F32)

    def level_b(zz):
        rows = normed[zz]
        w = jnp.concatenate([stacked(gb, zz, 0), stacked(gb, zz, 32)], axis=1)
        acc_b[:, 0:256] += jnp.dot(rows, w, preferred_element_type=F32)
        g = jnp.concatenate(
            [
                jnp.where(
                    spread, gb[zz * NY + j, 96:104].astype(F32)[0:1], 0.0
                ).astype(BF16)
                for j in range(NY)
            ],
            axis=0,
        )
        w = jnp.concatenate([stacked(gb, zz, 64), g], axis=1)
        acc_b[:, 256:512] += jnp.dot(rows, w, preferred_element_type=F32)

    def both(d, what):
        what(mod(z - d, NZ))

        @pl.when((d > 0) & (d < HALF))
        def _():
            what(mod(z + d, NZ))

    def b_step(s, j, far_up):
        sl, sl2 = mod(z - s, NZ) * NY + j, mod(z + s, NZ) * NY + j
        up_from, down_from = (HALF, HALF - 1) if far_up else (HALF - 1, HALF)

        @pl.when(s <= up_from)
        def _():
            b_up(gb.at[sl], sl, s, j).wait_recv()

            @pl.when(s < up_from)
            def _():
                b_up(gb.at[sl], sl, s + 1, j).start()

        @pl.when(s <= down_from)
        def _():
            b_down(gb.at[sl2], sl2, s, j).wait_recv()

            @pl.when(s < down_from)
            def _():
                b_down(gb.at[sl2], sl2, s + 1, j).start()

    def a_step(s):
        z_lo, z_hi = mod(z - s, NZ), mod(z + s, NZ)
        slot, slot2 = z_lo * NY + y, z_hi * NY + y
        for h in (0, 1):
            a_up(ga.at[slot], slot, s, h).wait_recv()

            @pl.when(s < HALF)
            def _():
                a_up(ga.at[slot], slot, s + 1, h).start()
                a_down(ga.at[slot2], slot2, s, h).wait_recv()

                @pl.when(s < HALF - 1)
                def _():
                    a_down(ga.at[slot2], slot2, s + 1, h).start()

        a_side(ga.at[slot], z_lo)

        @pl.when(s < HALF)
        def _():
            a_side(ga.at[slot2], z_hi)

    def above(d, what):
        @pl.when(d > 0)
        def _():
            what(mod(z + d, NZ))

    b_step(1, y, True)
    opposite()
    a_step(1)
    b_step(1, yd, True)
    b_step(1, yu, False)

    def step(s, carry):
        b_step(s - 1, yo, False)
        b_step(s, y, True)
        level_b(mod(z - s + 2, NZ))
        a_step(s)
        above(s - 2, level_b)
        b_step(s, yd, True)

        @pl.when(s >= 4)
        def _():
            level_a(mod(z - s + 4, NZ))

        b_step(s, yu, False)
        both(s - 2, side_forward)
        above(s - 4, level_a)
        return carry

    lax.fori_loop(2, HALF, step, 0)
    b_step(HALF - 1, yo, False)
    b_step(HALF, y, True)
    both(HALF - 2, level_b)
    b_step(HALF, yd, True)
    b_step(HALF, yu, False)
    both(HALF - 2, side_forward)
    both(HALF - 1, level_b)
    b_step(HALF, yo, False)
    level_b(mod(z - HALF, NZ))

    kv[...] = acc_b[:, 256:384].astype(BF16)
    first, last = pl.ds(0, WINDOW), pl.ds(TOK - WINDOW, WINDOW)
    to_next = remote(kv.at[last], halo.at[0], sh, rh, z=zn, y=yn)
    to_prev = remote(kv.at[first], halo.at[1], sh, rh, z=zq, y=yq)
    gt = jnp.sum(jnp.transpose(acc_b[:, 384:512]).reshape(4, 32, TOK), axis=1)
    in_f, in_b = gt[0:1] + bias[0:1, 0:1], gt[2:3] + bias[0:1, 2:3]
    lf_f = log_sigmoid(gt[1:2] + bias[0:1, 1:2]) + decay[0]
    lf_b = log_sigmoid(gt[3:4] + bias[0:1, 3:4]) + decay[1]
    to_next.start()
    to_prev.start()
    lane = lax.broadcasted_iota(jnp.int32, (1, TOK), 1)
    cum, rev = lf_f, lf_b
    k = 1
    while k < TOK:
        cum = cum + jnp.where(lane >= k, pltpu.roll(cum, k, 1), 0.0)
        rev = rev + jnp.where(lane < TOK - k, pltpu.roll(rev, TOK - k, 1), 0.0)
        k *= 2
    tot_f = jnp.max(jnp.where(lane == TOK - 1, cum, -jnp.inf), axis=1, keepdims=True)
    tot_b = jnp.max(jnp.where(lane == 0, rev, -jnp.inf), axis=1, keepdims=True)
    end_f = tot_f - cum + in_f
    end_b = tot_b - rev + in_b
    m_f = jnp.max(end_f, axis=1, keepdims=True)
    m_b = jnp.max(end_b, axis=1, keepdims=True)
    w_f, w_b = jnp.exp(end_f - m_f), jnp.exp(end_b - m_b)
    rows = jnp.concatenate([in_f, cum, in_b, rev, w_f, w_b, jnp.zeros((2, TOK), F32)], axis=0)
    cols = jnp.transpose(jnp.concatenate([rows, jnp.zeros((120, TOK), F32)], axis=0))
    key, value = acc_b[:, 0:128].astype(BF16), acc_b[:, 128:256].astype(BF16)
    val = value.astype(F32)
    tail, mats = [], []
    norms = jnp.dot(rows.astype(BF16), key, preferred_element_type=F32)
    for i in (4, 5):
        wv = (cols[:, i : i + 1] * val).astype(BF16)
        mats.append(
            lax.dot_general(key, wv, (((0,), (0,)), ((), ())), preferred_element_type=F32)
        )
        tail.append(norms[i : i + 1])
    for v in (m_f, tot_f, m_b, tot_b):
        tail.extend(jnp.broadcast_to(p, (1, 128)) for p in split3(v))
    tail.append(jnp.zeros((2, 128), F32))
    summary_tail = jnp.concatenate(tail, axis=0).astype(BF16)
    for q in range(NY):
        pk[q, 0:32] = mats[0][q * 32 : q * 32 + 32].astype(BF16)
        pk[q, 32:64] = mats[1][q * 32 : q * 32 + 32].astype(BF16)
        pk[q, 64:80] = summary_tail

    for d in (2, 1, 3):
        j = mod(y + d, NY)
        remote(pk.at[j], p1.at[y], s1, r1, y=j).start()
    p1[y] = pk[y]

    a_step(HALF)
    both(HALF - 4, level_a)
    both(HALF - 1, side_forward)
    both(HALF - 3, level_a)

    others_y, others_z = pl.ds(0, NY - 1), pl.ds(0, NZ - 1)
    remote(pk.at[others_y], p1.at[others_y], s1, r1, y=yd).wait_recv()

    def local_piece(j, back):
        ends = p1[j, 64:80].astype(F32)
        if back:
            return joined(ends, 8), joined(ends, 11), p1[j, 32:64].astype(F32), ends[1:2]
        return joined(ends, 2), joined(ends, 5), p1[j, 0:32].astype(F32), ends[0:1]

    for back in (0, 1):
        state, total_decay = empty_state(), jnp.zeros((1, 128), F32)
        for j in reversed(range(NY)) if back else range(NY):
            piece = local_piece(j, back)
            state = step_state(state, piece)
            total_decay = total_decay + piece[1]
        zp[back, 0:32] = state[1].astype(BF16)
        zp[back, 32:40] = jnp.concatenate(
            [state[2], *split3(state[0]), *split3(total_decay), jnp.zeros((1, 128), F32)],
            axis=0,
        ).astype(BF16)
    for d in (8, 7, 9, 6, 10, 5, 11, 4, 12, 3, 13, 2, 14, 1, 15):
        remote(
            zp.at[lax.div(z + d, NZ)],
            p2.at[z],
            s2,
            r2,
            z=mod(z + d, NZ),
        ).start()

    side_forward(mod(z - HALF, NZ))
    both(HALF - 2, level_a)
    both(HALF - 1, level_a)
    level_a(mod(z - HALF, NZ))
    query = acc_a[:, 0:128].astype(BF16)
    gate_in = acc_a[:, 128:256].astype(BF16)
    a_query = acc_a[:, 256:384].astype(BF16).astype(F32)

    mid, end = pl.ds(0, TOK // 2), pl.ds(TOK // 2, TOK // 2)

    def heads_start(i):
        mix, dst = mixes.at[i], full.at[i]
        for n, part in enumerate((mid, end)):
            remote(mix.at[part], dst.at[t, part], hs.at[i], hh.at[i, n], tp=t_far).start()
        remote(mix, dst.at[t], hs.at[i], hx.at[i, 0], tp=t_up).start()
        remote(mix, dst.at[t], hs.at[i], hx.at[i, 1], tp=t_down).start()
        remote(mix, dst.at[t], hs.at[i], hc.at[i], tp=partner).start()
        full[i, t] = mixes[i]

    def heads_end(i):
        mix, dst = mixes.at[i], full.at[i]
        for n, part in enumerate((mid, end)):
            src = dst.at[t_far, part]
            remote(src, src, hs.at[i], hh.at[i, n], tp=t_up).wait_recv()
            remote(src, src, hs.at[i], hc.at[i], tp=partner).start()
        for n, slot in enumerate((t_down, t_up)):
            src = dst.at[slot]
            remote(mix, src, hs.at[i], hx.at[i, n], tp=t_up).wait_recv()
            remote(src, src, hs.at[i], hc.at[i], tp=partner).start()
        half = pl.ds(0, NT // 2)
        remote(dst.at[half], dst.at[half], hs.at[i], hc.at[i], tp=partner).wait_recv()

    def heads_product(i):
        total = None
        for n in range(NT):
            w = jnp.concatenate(
                [
                    ga[8 * n : 8 * n + 8, at : at + 16].reshape(128, 128)
                    for at in (96 + 32 * i, 112 + 32 * i)
                ],
                axis=1,
            )
            term = jnp.dot(full[i, n], w, preferred_element_type=F32)
            total = term if total is None else total + term
        return total

    remote(halo, halo, sh, rh, y=yd).wait_recv()
    win[0:WINDOW] = halo[0]
    win[WINDOW : WINDOW + TOK] = kv[...]
    win[WINDOW + TOK :] = halo[1]
    low = lax.broadcasted_iota(jnp.int32, (WINDOW, 128), 1) < W_DIM
    two = lax.broadcasted_iota(jnp.int32, (2 * WINDOW, 3 * WINDOW), 0)
    col = lax.broadcasted_iota(jnp.int32, (2 * WINDOW, 3 * WINDOW), 1)
    off = col - jnp.where(two >= WINDOW, two - WINDOW, two)
    in_window = (off >= 0) & (off <= 2 * WINDOW)
    second = lax.broadcasted_iota(jnp.int32, (2 * WINDOW, 1), 0) >= WINDOW
    sink_col = jnp.where(second, sink[0:1, 1:2], sink[0:1, 0:1])
    for b in range(2):
        block = pl.ds(b * WINDOW, WINDOW)
        qb = a_query[b * WINDOW : b * WINDOW + WINDOW]
        q0 = jnp.where(low, qb, 0.0)
        q1 = jnp.where(low, pltpu.roll(qb, W_DIM, 1), 0.0)
        qq = jnp.concatenate([q0, q1], axis=0).astype(BF16)
        keys = win[b * WINDOW : b * WINDOW + 3 * WINDOW]
        scores = lax.dot_general(qq, keys, ACROSS, preferred_element_type=F32) * W_DIM**-0.5
        place = me * TOK + (b - 1) * WINDOW + col
        usable = in_window & (place >= 0) & (place < NZ * NY * TOK)
        scores = jnp.where(usable, scores, -jnp.inf)
        peak = jnp.maximum(sink_col, jnp.max(scores, axis=1, keepdims=True))
        weights = jnp.exp(scores - peak)
        tot = jnp.exp(sink_col - peak) + jnp.sum(weights, axis=1, keepdims=True)
        res = jnp.dot(weights.astype(BF16), keys, preferred_element_type=F32) / tot
        mixes[1, block] = jnp.where(
            low, pltpu.roll(res[0:WINDOW], W_DIM, 1), res[WINDOW:]
        ).astype(BF16)
        logt = jnp.transpose(jnp.broadcast_to(peak + jnp.log(tot), (2 * WINDOW, 128)))
        logs[0:1, block] = logt[0:1, 0:WINDOW]
        logs[1:2, block] = logt[0:1, WINDOW:]
    heads_start(1)
    gate_open = 1.0 / (1.0 + jnp.exp(-gate_in.astype(F32)))

    scale = M_DIM**-0.5
    dots = lax.dot_general(query, key, ACROSS, preferred_element_type=F32) * scale
    ti = lax.broadcasted_iota(jnp.int32, (TOK, TOK), 0)
    si = lax.broadcasted_iota(jnp.int32, (TOK, TOK), 1)
    inside = []
    for back in (0, 1):
        cum_t = cols[:, 2 * back + 1 : 2 * back + 2]
        log_in = rows[2 * back : 2 * back + 1] - rows[2 * back + 1 : 2 * back + 2]
        usable = (si >= ti) if back else (si <= ti)
        log_w = jnp.where(usable, cum_t + log_in, -jnp.inf)
        top = jnp.max(log_w, axis=1, keepdims=True)
        scores = dots * jnp.exp(log_w - top)
        numer = jnp.dot(scores.astype(BF16), value, preferred_element_type=F32)
        denom = jnp.sum(scores, axis=1, keepdims=True)
        inside.append((cum_t, top, numer, denom))


    remote(p2.at[others_z], p2.at[others_z], s2, r2, z=zd).wait_recv()

    def far(i, state):
        ends = p2[i, 32:40].astype(F32)
        return step_state(
            state, (joined(ends, 1), joined(ends, 4), p2[i, 0:32].astype(F32), ends[0:1])
        )

    fwd = lax.fori_loop(0, z, far, empty_state())
    bwd = lax.fori_loop(0, NZ - 1 - z, lambda i, s: far(NZ - 1 - i, s), empty_state())
    for j in range(NY):
        p3[j, 0:32] = fwd[1].astype(BF16)
        keep[j, 0:1] = fwd[2]
        keep[j, 2:3] = fwd[0]
        fwd = step_state(fwd, local_piece(j, 0))
    for j in reversed(range(NY)):
        p3[j, 32:64] = bwd[1].astype(BF16)
        keep[j, 1:2] = bwd[2]
        keep[j, 3:4] = bwd[0]
        bwd = step_state(bwd, local_piece(j, 1))
    for d in (2, 1, 3):
        j = mod(y + d, NY)
        remote(p3.at[j], st.at[y], s3, r3, y=j).start()
    st[y] = p3[y]
    nm = keep[y]
    qf = query.astype(F32) * scale
    remote(p3.at[others_y], st.at[others_y], s3, r3, y=yd).wait_recv()

    cell = None
    for back in (0, 1):
        cum_t, top_in, numer, denom = inside[back]
        inter = cum_t + nm[2 + back : 3 + back, 0:1]
        top = jnp.maximum(inter, top_in)
        w_in, w_inter = jnp.exp(top_in - top), jnp.exp(inter - top)
        mat = st[:, 32 * back : 32 * back + 32].reshape(128, 128)
        numer = w_in * numer + (w_inter * scale) * jnp.dot(
            query, mat, preferred_element_type=F32
        )
        denom = w_in * denom + w_inter * jnp.sum(
            qf * nm[back : back + 1], axis=1, keepdims=True
        )
        part = numer / jnp.maximum(jnp.abs(denom), jnp.exp(-top))
        cell = part if cell is None else cell + part
    u = cell * gate_open
    norm = lax.rsqrt(jnp.mean(u * u, axis=1, keepdims=True) + EPS)
    mixes[0] = (u * norm * mgain[...]).astype(BF16)
    heads_start(0)
    heads_end(1)
    acc_b[:, 0:256] = heads_product(1)
    heads_end(0)
    out[...] = (acc_b[:, 0:256] + heads_product(0)).astype(BF16)

    n = NZ * NY - 1
    every = pl.ds(0, n)
    remote(ga.at[every], ga.at[every], sa, ah.at[0], y=yd).wait_send()
    remote(gb.at[every], gb.at[every], sb, ah.at[0], y=yd).wait_send()
    remote(pk.at[others_y], p1.at[others_y], s1, r1, y=yd).wait_send()
    remote(p3.at[others_y], st.at[others_y], s3, r3, y=yd).wait_send()
    remote(p2.at[others_z], p2.at[others_z], s2, r2, z=zd).wait_send()
    remote(halo, halo, sh, rh, y=yd).wait_send()
    most = pl.ds(0, NT - 1)
    for i in (0, 1):
        src = full.at[i, most]
        remote(src, src, hs.at[i], hc.at[i], tp=partner).wait_send()


def on_device(
    tokens,
    input_norm_gain,
    mq_weight,
    mk_weight,
    mv_weight,
    mo_weight,
    gate_weight,
    gate_bias,
    decay_extra,
    m_gain,
    aq_weight,
    ak_weight,
    av_weight,
    sink_logit,
    out_m_weight,
    out_a_weight,
):
    sds = jax.ShapeDtypeStruct
    dma = pltpu.SemaphoreType.DMA
    vm = pltpu.VMEM
    hbm = pl.BlockSpec(memory_space=pl.ANY)
    local = pl.BlockSpec(memory_space=pltpu.VMEM)
    n = NZ * NY
    return pl.pallas_call(
        layer_body,
        name="layer",
        out_shape=(vm((TOK, 256), BF16), vm((2, TOK), F32)),
        in_specs=[hbm] * 16,
        out_specs=[local] * 2,
        scratch_shapes=[
            vm((1, D), F32),
            vm((4, 32), BF16),
            vm((1, 4), F32),
            vm((2, 1, TOK), F32),
            vm((1, 128), F32),
            vm((32, 64), BF16),
            vm((32, 64), BF16),
            vm((1, 2), F32),
            vm((TOK, D), BF16),
            vm((A_ROWS, 128), BF16),
            vm((B_ROWS, 128), BF16),
            vm((n, A_ROWS, 128), BF16),
            vm((n, B_ROWS, 128), BF16),
            vm((NZ, TOK, 128), BF16),
            vm((TOK, 384), F32),
            vm((TOK, 512), F32),
            vm((TOK, 128), BF16),
            vm((2, WINDOW, 128), BF16),
            vm((TOK + 2 * WINDOW, 128), BF16),
            vm((NY, 80, 128), BF16),
            vm((NY, 80, 128), BF16),
            vm((2, 40, 128), BF16),
            vm((NZ, 40, 128), BF16),
            vm((NY, 64, 128), BF16),
            vm((NY, 64, 128), BF16),
            vm((NY, 8, 128), F32),
            vm((2, TOK, 128), BF16),
            vm((2, NT, TOK, 128), BF16),
            dma((11,)),
            dma((2,)),
            dma((2, HALF, 2)),
            dma((2, NZ)),
            dma((NZ,)),
            dma((2, HALF, NY)),
            dma((2,)),
            dma((2,)),
            dma,
            dma,
            dma,
            dma,
            dma,
            dma,
            dma,
            dma,
            dma((2,)),
            dma((2, 2)),
            dma((2, 2)),
            dma((2,)),
        ],
        compiler_params=pltpu.CompilerParams(collective_id=0, has_side_effects=True),
    )(
        tokens,
        input_norm_gain[None],
        mq_weight,
        mk_weight,
        mv_weight,
        mo_weight,
        gate_weight[:, :, 0].T,
        gate_bias.T,
        decay_extra,
        m_gain[None],
        aq_weight,
        ak_weight,
        av_weight,
        sink_logit[None],
        out_m_weight,
        out_a_weight,
    )


def solution(mesh):
    split = Mesh(mesh.devices.reshape(NZ, NY, NT), ("z", "y", "tp"))
    return jax.shard_map(
        on_device,
        mesh=split,
        in_specs=(
            P(SP, None),
            P(),
            P(SP, "tp"),
            P(SP, "tp"),
            P(SP, "tp"),
            P(SP, "tp"),
            P(SP, None, "tp"),
            P(None, "tp"),
            P(None, "tp", SP),
            P("tp"),
            P(SP, "tp"),
            P(SP, "tp"),
            P(SP, "tp"),
            P("tp"),
            P(SP, "tp"),
            P(SP, "tp"),
        ),
        out_specs=(P(SP, "tp"), P("tp", SP)),
        check_vma=False,
    )
```

```python
import jax
import jax.numpy as jnp
from jax import lax
from jax.experimental import pallas as pl
from jax.experimental.pallas import tpu as pltpu
from jax.sharding import Mesh
from jax.sharding import PartitionSpec as P

M_DIM = 128
W_DIM = 64
WINDOW = 128
EPS = 1e-06
FLOOR_LOG = -1e30
NZ = 16
NY = 4
NX = 4
NT = 8
TOK = 256
D = 2048
HALF = NZ // 2
A_ROWS = 160
B_ROWS = 104
SP = ("z", "y")
MESH = pl.DeviceIdType.MESH
F32 = jnp.float32
BF16 = jnp.bfloat16
ACROSS = (((1,), (1,)), ((), ()))


def mod(a, n):
    return lax.rem(a + n, n)


def remote(src, dst, ssem, rsem, **where):
    return pltpu.make_async_remote_copy(
        src_ref=src,
        dst_ref=dst,
        send_sem=ssem,
        recv_sem=rsem,
        device_id=where,
        device_id_type=MESH,
    )


def log1p_of(e):
    poly = e * (
        1.0
        + e * (-0.5 + e * (1 / 3 + e * (-0.25 + e * (0.2 + e * (-1 / 6 + e * (1 / 7))))))
    )
    return jnp.where(e < 0.0625, poly, jnp.log(1.0 + e))


def log_sigmoid(x):
    return jnp.minimum(x, 0.0) - log1p_of(jnp.exp(-jnp.abs(x)))


def split3(x):
    hi = x.astype(BF16).astype(F32)
    mid = (x - hi).astype(BF16).astype(F32)
    return hi, mid, x - hi - mid


def joined(tail, at):
    return tail[at : at + 1] + tail[at + 1 : at + 2] + tail[at + 2 : at + 3]


def step_state(state, piece):
    peak, mat, norm = state
    p_peak, p_decay, p_mat, p_norm = piece
    new = jnp.maximum(peak + p_decay, p_peak)
    old_s, new_s = jnp.exp(peak + p_decay - new), jnp.exp(p_peak - new)
    return new, mat * old_s + p_mat * new_s, norm * old_s + p_norm * new_s


def empty_state():
    return (
        jnp.full((1, 128), FLOOR_LOG, F32),
        jnp.zeros((32, 128), F32),
        jnp.zeros((1, 128), F32),
    )


def layer_body(
    tok_hbm,
    gain_hbm,
    mq,
    mk,
    mv,
    mo,
    gate_hbm,
    bias_hbm,
    decay_hbm,
    mgain_hbm,
    aq_w,
    ak_hbm,
    av_hbm,
    sink_hbm,
    om,
    oa,
    out,
    logs,
    gain,
    gate_t,
    bias,
    decay,
    mgain,
    ak_w,
    av_w,
    sink,
    tok,
    wa,
    wb,
    ga,
    gb,
    normed,
    tri,
    acc_a,
    acc_b,
    kv,
    halo,
    win,
    pk,
    p1,
    zp,
    p2,
    p3,
    st,
    keep,
    mixes,
    full,
    local_sem,
    ssem,
    az,
    ay,
    ah,
    bz,
    by,
    bh,
    s1,
    r1,
    s2,
    r2,
    s3,
    r3,
    sh,
    rh,
    hs,
    hx,
    hh,
    hc,
):
    z = lax.axis_index("z")
    y = lax.axis_index("y")
    t = lax.axis_index("tp")
    me = z * NY + y
    zu, zd = mod(z + 1, NZ), mod(z - 1, NZ)
    yu, yd = mod(y + 1, NY), mod(y - 1, NY)
    yo = mod(y + 2, NY)
    nxt, prv = mod(me + 1, NZ * NY), mod(me - 1, NZ * NY)
    zn, yn = lax.div(nxt, NY), lax.rem(nxt, NY)
    zq, yq = lax.div(prv, NY), lax.rem(prv, NY)
    x, c = lax.div(t, 2), lax.rem(t, 2)
    o = 1 - c
    xu, xd, xo = mod(x + 1, NX), mod(x - 1, NX), mod(x + 2, NX)
    partner, t_up, t_down, t_far = 2 * x + o, 2 * xu + c, 2 * xd + c, 2 * xo + c

    loads = []

    def load(src, dst):
        copy = pltpu.make_async_copy(src, dst, local_sem.at[2 + len(loads)])
        copy.start()
        loads.append(copy)
        return copy

    early = [load(ak_hbm, ak_w), load(av_hbm, av_w), load(gate_hbm, gate_t)]
    for i, w in enumerate((mk, mv)):
        pltpu.make_async_copy(w, wb.at[32 * i : 32 * i + 32], local_sem.at[0]).start()
    for i, w in enumerate((mq, mo, aq_w)):
        pltpu.make_async_copy(w, wa.at[32 * i : 32 * i + 32], local_sem.at[1]).start()
    for i, w in enumerate((om, oa)):
        for part in (0, 1):
            at = 96 + 32 * i + 16 * part
            src = w.at[:, 128 * part : 128 * part + 128]
            pltpu.make_async_copy(src, wa.at[at : at + 16], local_sem.at[1]).start()
    late = [load(tok_hbm, tok), load(gain_hbm, gain), load(bias_hbm, bias)]
    late += [load(decay_hbm, decay), load(mgain_hbm, mgain), load(sink_hbm, sink)]
    barrier = pltpu.get_barrier_semaphore()
    hello = [{"z": zu}, {"z": zd}, {"y": yu}, {"y": yd}, {"y": yo}]
    hello += [{"z": zn, "y": yn}, {"z": zq, "y": yq}]
    hello += [{"tp": partner}, {"tp": t_up}, {"tp": t_down}, {"tp": t_far}]
    for where in hello:
        pl.semaphore_signal(barrier, inc=1, device_id=where, device_id_type=MESH)
    for copy in early:
        copy.wait()
    wb[64:96] = jnp.concatenate([ak_w[...], av_w[...]], axis=1)
    gate_rows = jnp.concatenate([gate_t[...].astype(F32), jnp.zeros((4, 96), F32)], axis=1)
    gate_row = gate_rows[0:1]
    for g in range(1, 4):
        gate_row = gate_row + pltpu.roll(gate_rows[g : g + 1], 32 * g, 1)
    wb[96:104] = jnp.concatenate([gate_row, jnp.zeros((7, 128), F32)], axis=0).astype(BF16)
    two_weights = wb.at[0:64]
    pltpu.make_async_copy(two_weights, two_weights, local_sem.at[0]).wait()
    pltpu.make_async_copy(wa, wa, local_sem.at[1]).wait()
    pl.semaphore_wait(barrier, len(hello))

    sa, sb = ssem.at[0], ssem.at[1]

    parts = (pl.ds(0, A_ROWS // 2), pl.ds(A_ROWS // 2, A_ROWS // 2))

    def a_up(ref, slot, s, h):
        return remote(ref.at[parts[h]], ga.at[slot, parts[h]], sa, az.at[s - 1, h], z=zu)

    def a_down(ref, slot, s, h):
        return remote(ref.at[parts[h]], ga.at[slot, parts[h]], sa, az.at[s - 1, h], z=zd)

    def a_side(src, zz):
        slot = zz * NY + y
        remote(src, ga.at[slot], sa, ay.at[zz], y=yu).start()
        remote(src, ga.at[slot], sa, ay.at[zz], y=yd).start()

    def b_up(src, slot, s, j):
        return remote(src, gb.at[slot], sb, bz.at[0, s - 1, j], z=zu)

    def b_down(src, slot, s, j):
        return remote(src, gb.at[slot], sb, bz.at[1, s - 1, j], z=zd)

    remote(wb, gb.at[me], sb, bh.at[0], y=yo).start()
    remote(wb, gb.at[me], sb, by.at[0], y=yu).start()
    remote(wb, gb.at[me], sb, by.at[1], y=yd).start()
    b_up(wb, me, 1, y).start()
    b_down(wb, me, 1, y).start()
    for h in (0, 1):
        a_up(wa, me, 1, h).start()
        a_down(wa, me, 1, h).start()
    ga[me] = wa[...]
    gb[me] = wb[...]

    for copy in late:
        copy.wait()
    xs = tok[...].astype(F32)
    xs = xs * lax.rsqrt(jnp.mean(xs * xs, axis=-1, keepdims=True) + EPS) * gain[...]
    for i in range(NZ):
        normed[i] = xs[:, 128 * i : 128 * i + 128].astype(BF16)
    acc_a[...] = jnp.zeros_like(acc_a)
    acc_b[...] = jnp.zeros_like(acc_b)
    down_at = lax.broadcasted_iota(jnp.int32, (TOK, 2 * TOK), 0)
    across_at = lax.broadcasted_iota(jnp.int32, (TOK, 2 * TOK), 1)
    upper = (across_at < TOK) & (down_at <= across_at)
    lower = (across_at >= TOK) & (down_at >= across_at - TOK)
    tri[...] = jnp.where(upper | lower, 1.0, 0.0).astype(BF16)

    slot_d, slot_u, slot_o = z * NY + yd, z * NY + yu, z * NY + yo
    lo, hi = pl.ds(0, A_ROWS // 2), pl.ds(A_ROWS // 2, A_ROWS // 2)
    remote(wb, gb.at[slot_d], sb, by.at[0], y=yd).wait_recv()
    b_up(gb.at[slot_d], slot_d, 1, yd).start()
    b_down(gb.at[slot_d], slot_d, 1, yd).start()
    remote(wb, gb.at[slot_u], sb, by.at[1], y=yd).wait_recv()
    b_up(gb.at[slot_u], slot_u, 1, yu).start()
    b_down(gb.at[slot_u], slot_u, 1, yu).start()
    a_side(wa, z)

    def opposite():
        remote(wb, gb.at[slot_o], sb, bh.at[0], y=yd).wait_recv()
        b_up(gb.at[slot_o], slot_o, 1, yo).start()
        b_down(gb.at[slot_o], slot_o, 1, yo).start()

    def side_forward(zz):
        sd, su = zz * NY + yd, zz * NY + yu
        two_blocks = ga.at[pl.ds(0, 2)]
        remote(two_blocks, two_blocks, sa, ay.at[zz], y=yd).wait_recv()
        remote(ga.at[sd, lo], ga.at[sd, lo], sa, ah.at[zz], y=yu).start()
        remote(ga.at[su, hi], ga.at[su, hi], sa, ah.at[zz], y=yd).start()

    spread = lax.broadcasted_iota(jnp.int32, (32, 128), 0) == lax.rem(
        lax.broadcasted_iota(jnp.int32, (32, 128), 1), 32
    )

    def stacked(ref, zz, at):
        return jnp.concatenate([ref[zz * NY + j, at : at + 32] for j in range(NY)], axis=0)

    def level_a(zz):
        so = zz * NY + yo
        remote(ga.at[so], ga.at[so], sa, ah.at[zz], y=yd).wait_recv()
        rows = normed[zz]
        w = jnp.concatenate([stacked(ga, zz, 0), stacked(ga, zz, 32)], axis=1)
        acc_a[:, 0:256] += jnp.dot(rows, w, preferred_element_type=F32)
        acc_a[:, 256:384] += jnp.dot(rows, stacked(ga, zz, 64), preferred_element_type=F32)

    def level_b(zz):
        rows = normed[zz]
        w = jnp.concatenate([stacked(gb, zz, 0), stacked(gb, zz, 32)], axis=1)
        acc_b[:, 0:256] += jnp.dot(rows, w, preferred_element_type=F32)
        g = jnp.concatenate(
            [
                jnp.where(
                    spread, gb[zz * NY + j, 96:104].astype(F32)[0:1], 0.0
                ).astype(BF16)
                for j in range(NY)
            ],
            axis=0,
        )
        w = jnp.concatenate([stacked(gb, zz, 64), g], axis=1)
        acc_b[:, 256:512] += jnp.dot(rows, w, preferred_element_type=F32)

    def both(d, what):
        what(mod(z - d, NZ))

        @pl.when((d > 0) & (d < HALF))
        def _():
            what(mod(z + d, NZ))

    def b_step(s, j, far_up):
        sl, sl2 = mod(z - s, NZ) * NY + j, mod(z + s, NZ) * NY + j
        up_from, down_from = (HALF, HALF - 1) if far_up else (HALF - 1, HALF)

        @pl.when(s <= up_from)
        def _():
            b_up(gb.at[sl], sl, s, j).wait_recv()

            @pl.when(s < up_from)
            def _():
                b_up(gb.at[sl], sl, s + 1, j).start()

        @pl.when(s <= down_from)
        def _():
            b_down(gb.at[sl2], sl2, s, j).wait_recv()

            @pl.when(s < down_from)
            def _():
                b_down(gb.at[sl2], sl2, s + 1, j).start()

    def a_step(s):
        s = jnp.int32(s)
        z_lo, z_hi = mod(z - s, NZ), mod(z + s, NZ)
        slot, slot2 = z_lo * NY + y, z_hi * NY + y
        for h in (0, 1):

            @pl.when(s < HALF)
            def _():
                two_halves = ga.at[slot]
                remote(two_halves, two_halves, sa, az.at[s - 1, h], z=zu).wait_recv()
                a_up(ga.at[slot], slot, s + 1, h).start()

                @pl.when(s < HALF - 1)
                def _():
                    a_down(ga.at[slot2], slot2, s + 1, h).start()

            @pl.when(s == HALF)
            def _():
                a_up(ga.at[slot], slot, s, h).wait_recv()

        a_side(ga.at[slot], z_lo)

        @pl.when(s < HALF)
        def _():
            a_side(ga.at[slot2], z_hi)

    def above(d, what):
        @pl.when(d > 0)
        def _():
            what(mod(z + d, NZ))

    b_step(1, y, True)
    opposite()
    a_step(1)
    b_step(1, yd, True)
    b_step(1, yu, False)

    def step(s, carry):
        b_step(s - 1, yo, False)
        b_step(s, y, True)
        level_b(mod(z - s + 2, NZ))
        a_step(s)
        above(s - 2, level_b)
        b_step(s, yd, True)

        @pl.when(s >= 4)
        def _():
            level_a(mod(z - s + 4, NZ))

        b_step(s, yu, False)
        both(s - 2, side_forward)
        above(s - 4, level_a)
        return carry

    lax.fori_loop(2, HALF, step, 0)
    b_step(HALF - 1, yo, False)
    b_step(HALF, y, True)
    both(HALF - 2, level_b)
    b_step(HALF, yd, True)
    b_step(HALF, yu, False)
    both(HALF - 2, side_forward)
    both(HALF - 1, level_b)
    b_step(HALF, yo, False)
    level_b(mod(z - HALF, NZ))

    kv[...] = acc_b[:, 256:384].astype(BF16)
    first, last = pl.ds(0, WINDOW), pl.ds(TOK - WINDOW, WINDOW)
    to_next = remote(kv.at[last], halo.at[0], sh, rh, z=zn, y=yn)
    to_prev = remote(kv.at[first], halo.at[1], sh, rh, z=zq, y=yq)
    gt = jnp.sum(jnp.transpose(acc_b[:, 384:512]).reshape(4, 32, TOK), axis=1)
    in_f, in_b = gt[0:1] + bias[0:1, 0:1], gt[2:3] + bias[0:1, 2:3]
    lf_f = log_sigmoid(gt[1:2] + bias[0:1, 1:2]) + decay[0]
    lf_b = log_sigmoid(gt[3:4] + bias[0:1, 3:4]) + decay[1]
    to_next.start()
    to_prev.start()
    lane = lax.broadcasted_iota(jnp.int32, (1, TOK), 1)
    terms = jnp.concatenate([*split3(lf_f), *split3(lf_b), jnp.zeros((2, TOK), F32)], axis=0)
    sums = jnp.dot(terms.astype(BF16), tri[...], preferred_element_type=F32)
    cum = joined(sums[:, 0:TOK], 0)
    rev = joined(sums[:, TOK:], 3)
    tot_f = jnp.max(jnp.where(lane == TOK - 1, cum, -jnp.inf), axis=1, keepdims=True)
    tot_b = jnp.max(jnp.where(lane == 0, rev, -jnp.inf), axis=1, keepdims=True)
    end_f = tot_f - cum + in_f
    end_b = tot_b - rev + in_b
    m_f = jnp.max(end_f, axis=1, keepdims=True)
    m_b = jnp.max(end_b, axis=1, keepdims=True)
    w_f, w_b = jnp.exp(end_f - m_f), jnp.exp(end_b - m_b)
    rows = jnp.concatenate([in_f, cum, in_b, rev, w_f, w_b, jnp.zeros((2, TOK), F32)], axis=0)
    cols = jnp.transpose(jnp.concatenate([rows, jnp.zeros((120, TOK), F32)], axis=0))
    key, value = acc_b[:, 0:128].astype(BF16), acc_b[:, 128:256].astype(BF16)
    val = value.astype(F32)
    tail, mats = [], []
    norms = jnp.dot(rows.astype(BF16), key, preferred_element_type=F32)
    for i in (4, 5):
        wv = (cols[:, i : i + 1] * val).astype(BF16)
        mats.append(
            lax.dot_general(key, wv, (((0,), (0,)), ((), ())), preferred_element_type=F32)
        )
        tail.append(norms[i : i + 1])
    for v in (m_f, tot_f, m_b, tot_b):
        tail.extend(jnp.broadcast_to(p, (1, 128)) for p in split3(v))
    tail.append(jnp.zeros((2, 128), F32))
    summary_tail = jnp.concatenate(tail, axis=0).astype(BF16)
    for q in range(NY):
        pk[q, 0:32] = mats[0][q * 32 : q * 32 + 32].astype(BF16)
        pk[q, 32:64] = mats[1][q * 32 : q * 32 + 32].astype(BF16)
        pk[q, 64:80] = summary_tail

    for d in (2, 1, 3):
        j = mod(y + d, NY)
        remote(pk.at[j], p1.at[y], s1, r1, y=j).start()
    p1[y] = pk[y]

    a_step(HALF)
    both(HALF - 4, level_a)
    both(HALF - 1, side_forward)
    both(HALF - 3, level_a)

    others_y, others_z = pl.ds(0, NY - 1), pl.ds(0, NZ - 1)
    remote(pk.at[others_y], p1.at[others_y], s1, r1, y=yd).wait_recv()

    def local_piece(j, back):
        ends = p1[j, 64:80].astype(F32)
        if back:
            return joined(ends, 8), joined(ends, 11), p1[j, 32:64].astype(F32), ends[1:2]
        return joined(ends, 2), joined(ends, 5), p1[j, 0:32].astype(F32), ends[0:1]

    for back in (0, 1):
        state, total_decay = empty_state(), jnp.zeros((1, 128), F32)
        for j in reversed(range(NY)) if back else range(NY):
            piece = local_piece(j, back)
            state = step_state(state, piece)
            total_decay = total_decay + piece[1]
        zp[back, 0:32] = state[1].astype(BF16)
        zp[back, 32:40] = jnp.concatenate(
            [state[2], *split3(state[0]), *split3(total_decay), jnp.zeros((1, 128), F32)],
            axis=0,
        ).astype(BF16)
    for d in (8, 7, 9, 6, 10, 5, 11, 4, 12, 3, 13, 2, 14, 1, 15):
        remote(
            zp.at[lax.div(z + d, NZ)],
            p2.at[z],
            s2,
            r2,
            z=mod(z + d, NZ),
        ).start()

    side_forward(mod(z - HALF, NZ))
    both(HALF - 2, level_a)
    both(HALF - 1, level_a)
    level_a(mod(z - HALF, NZ))
    query = acc_a[:, 0:128].astype(BF16)
    gate_in = acc_a[:, 128:256].astype(BF16)
    a_query = acc_a[:, 256:384].astype(BF16).astype(F32)

    mid, end = pl.ds(0, TOK // 2), pl.ds(TOK // 2, TOK // 2)

    def heads_start(i):
        mix, dst = mixes.at[i], full.at[i]
        for n, part in enumerate((mid, end)):
            remote(mix.at[part], dst.at[t, part], hs.at[i], hh.at[i, n], tp=t_far).start()
        remote(mix, dst.at[t], hs.at[i], hx.at[i, 0], tp=t_up).start()
        remote(mix, dst.at[t], hs.at[i], hx.at[i, 1], tp=t_down).start()
        remote(mix, dst.at[t], hs.at[i], hc.at[i], tp=partner).start()
        full[i, t] = mixes[i]

    def heads_end(i):
        mix, dst = mixes.at[i], full.at[i]
        for n, part in enumerate((mid, end)):
            src = dst.at[t_far, part]
            remote(src, src, hs.at[i], hh.at[i, n], tp=t_up).wait_recv()
            remote(src, src, hs.at[i], hc.at[i], tp=partner).start()
        for n, slot in enumerate((t_down, t_up)):
            src = dst.at[slot]
            remote(mix, src, hs.at[i], hx.at[i, n], tp=t_up).wait_recv()
            remote(src, src, hs.at[i], hc.at[i], tp=partner).start()
        half = pl.ds(0, NT // 2)
        remote(dst.at[half], dst.at[half], hs.at[i], hc.at[i], tp=partner).wait_recv()

    def heads_product(i):
        total = None
        for n in range(NT):
            w = jnp.concatenate(
                [
                    ga[8 * n : 8 * n + 8, at : at + 16].reshape(128, 128)
                    for at in (96 + 32 * i, 112 + 32 * i)
                ],
                axis=1,
            )
            term = jnp.dot(full[i, n], w, preferred_element_type=F32)
            total = term if total is None else total + term
        return total

    remote(halo, halo, sh, rh, y=yd).wait_recv()
    win[0:WINDOW] = halo[0]
    win[WINDOW : WINDOW + TOK] = kv[...]
    win[WINDOW + TOK :] = halo[1]
    low = lax.broadcasted_iota(jnp.int32, (WINDOW, 128), 1) < W_DIM
    two = lax.broadcasted_iota(jnp.int32, (2 * WINDOW, 3 * WINDOW), 0)
    col = lax.broadcasted_iota(jnp.int32, (2 * WINDOW, 3 * WINDOW), 1)
    off = col - jnp.where(two >= WINDOW, two - WINDOW, two)
    in_window = (off >= 0) & (off <= 2 * WINDOW)
    second = lax.broadcasted_iota(jnp.int32, (2 * WINDOW, 1), 0) >= WINDOW
    sink_col = jnp.where(second, sink[0:1, 1:2], sink[0:1, 0:1])
    for b in range(2):
        block = pl.ds(b * WINDOW, WINDOW)
        qb = a_query[b * WINDOW : b * WINDOW + WINDOW]
        q0 = jnp.where(low, qb, 0.0)
        q1 = jnp.where(low, pltpu.roll(qb, W_DIM, 1), 0.0)
        qq = jnp.concatenate([q0, q1], axis=0).astype(BF16)
        keys = win[b * WINDOW : b * WINDOW + 3 * WINDOW]
        scores = lax.dot_general(qq, keys, ACROSS, preferred_element_type=F32) * W_DIM**-0.5
        place = me * TOK + (b - 1) * WINDOW + col
        usable = in_window & (place >= 0) & (place < NZ * NY * TOK)
        scores = jnp.where(usable, scores, -jnp.inf)
        peak = jnp.maximum(sink_col, jnp.max(scores, axis=1, keepdims=True))
        weights = jnp.exp(scores - peak)
        tot = jnp.exp(sink_col - peak) + jnp.sum(weights, axis=1, keepdims=True)
        res = jnp.dot(weights.astype(BF16), keys, preferred_element_type=F32) / tot
        mixes[1, block] = jnp.where(
            low, pltpu.roll(res[0:WINDOW], W_DIM, 1), res[WINDOW:]
        ).astype(BF16)
        logt = jnp.transpose(jnp.broadcast_to(peak + jnp.log(tot), (2 * WINDOW, 128)))
        logs[0:1, block] = logt[0:1, 0:WINDOW]
        logs[1:2, block] = logt[0:1, WINDOW:]
    heads_start(1)
    gate_open = 1.0 / (1.0 + jnp.exp(-gate_in.astype(F32)))

    scale = M_DIM**-0.5
    dots = lax.dot_general(query, key, ACROSS, preferred_element_type=F32) * scale
    ti = lax.broadcasted_iota(jnp.int32, (TOK, TOK), 0)
    si = lax.broadcasted_iota(jnp.int32, (TOK, TOK), 1)
    inside = []
    for back in (0, 1):
        cum_t = cols[:, 2 * back + 1 : 2 * back + 2]
        log_in = rows[2 * back : 2 * back + 1] - rows[2 * back + 1 : 2 * back + 2]
        usable = (si >= ti) if back else (si <= ti)
        log_w = jnp.where(usable, cum_t + log_in, -jnp.inf)
        top = jnp.max(log_w, axis=1, keepdims=True)
        scores = dots * jnp.exp(log_w - top)
        numer = jnp.dot(scores.astype(BF16), value, preferred_element_type=F32)
        denom = jnp.sum(scores, axis=1, keepdims=True)
        inside.append((cum_t, top, numer, denom))


    remote(p2.at[others_z], p2.at[others_z], s2, r2, z=zd).wait_recv()

    def far(i, state):
        ends = p2[i, 32:40].astype(F32)
        return step_state(
            state, (joined(ends, 1), joined(ends, 4), p2[i, 0:32].astype(F32), ends[0:1])
        )

    fwd = lax.fori_loop(0, z, far, empty_state())
    bwd = lax.fori_loop(0, NZ - 1 - z, lambda i, s: far(NZ - 1 - i, s), empty_state())
    for j in range(NY):
        p3[j, 0:32] = fwd[1].astype(BF16)
        keep[j, 0:1] = fwd[2]
        keep[j, 2:3] = fwd[0]
        fwd = step_state(fwd, local_piece(j, 0))
    for j in reversed(range(NY)):
        p3[j, 32:64] = bwd[1].astype(BF16)
        keep[j, 1:2] = bwd[2]
        keep[j, 3:4] = bwd[0]
        bwd = step_state(bwd, local_piece(j, 1))
    for d in (2, 1, 3):
        j = mod(y + d, NY)
        remote(p3.at[j], st.at[y], s3, r3, y=j).start()
    st[y] = p3[y]
    nm = keep[y]
    qf = query.astype(F32) * scale
    remote(p3.at[others_y], st.at[others_y], s3, r3, y=yd).wait_recv()

    cell = None
    for back in (0, 1):
        cum_t, top_in, numer, denom = inside[back]
        inter = cum_t + nm[2 + back : 3 + back, 0:1]
        top = jnp.maximum(inter, top_in)
        w_in, w_inter = jnp.exp(top_in - top), jnp.exp(inter - top)
        mat = st[:, 32 * back : 32 * back + 32].reshape(128, 128)
        numer = w_in * numer + (w_inter * scale) * jnp.dot(
            query, mat, preferred_element_type=F32
        )
        denom = w_in * denom + w_inter * jnp.sum(
            qf * nm[back : back + 1], axis=1, keepdims=True
        )
        part = numer / jnp.maximum(jnp.abs(denom), jnp.exp(-top))
        cell = part if cell is None else cell + part
    u = cell * gate_open
    norm = lax.rsqrt(jnp.mean(u * u, axis=1, keepdims=True) + EPS)
    mixes[0] = (u * norm * mgain[...]).astype(BF16)
    heads_start(0)
    heads_end(1)
    acc_b[:, 0:256] = heads_product(1)
    heads_end(0)
    out[...] = (acc_b[:, 0:256] + heads_product(0)).astype(BF16)

    n = NZ * NY - 1
    every = pl.ds(0, n)
    remote(ga.at[every], ga.at[every], sa, ah.at[0], y=yd).wait_send()
    remote(gb.at[every], gb.at[every], sb, ah.at[0], y=yd).wait_send()
    remote(pk.at[others_y], p1.at[others_y], s1, r1, y=yd).wait_send()
    remote(p3.at[others_y], st.at[others_y], s3, r3, y=yd).wait_send()
    remote(p2.at[others_z], p2.at[others_z], s2, r2, z=zd).wait_send()
    remote(halo, halo, sh, rh, y=yd).wait_send()
    most = pl.ds(0, NT - 1)
    for i in (0, 1):
        src = full.at[i, most]
        remote(src, src, hs.at[i], hc.at[i], tp=partner).wait_send()


def on_device(
    tokens,
    input_norm_gain,
    mq_weight,
    mk_weight,
    mv_weight,
    mo_weight,
    gate_weight,
    gate_bias,
    decay_extra,
    m_gain,
    aq_weight,
    ak_weight,
    av_weight,
    sink_logit,
    out_m_weight,
    out_a_weight,
):
    sds = jax.ShapeDtypeStruct
    dma = pltpu.SemaphoreType.DMA
    vm = pltpu.VMEM
    hbm = pl.BlockSpec(memory_space=pl.ANY)
    local = pl.BlockSpec(memory_space=pltpu.VMEM)
    n = NZ * NY
    return pl.pallas_call(
        layer_body,
        name="layer",
        out_shape=(vm((TOK, 256), BF16), vm((2, TOK), F32)),
        in_specs=[hbm] * 16,
        out_specs=[local] * 2,
        scratch_shapes=[
            vm((1, D), F32),
            vm((4, 32), BF16),
            vm((1, 4), F32),
            vm((2, 1, TOK), F32),
            vm((1, 128), F32),
            vm((32, 64), BF16),
            vm((32, 64), BF16),
            vm((1, 2), F32),
            vm((TOK, D), BF16),
            vm((A_ROWS, 128), BF16),
            vm((B_ROWS, 128), BF16),
            vm((n, A_ROWS, 128), BF16),
            vm((n, B_ROWS, 128), BF16),
            vm((NZ, TOK, 128), BF16),
            vm((TOK, 2 * TOK), BF16),
            vm((TOK, 384), F32),
            vm((TOK, 512), F32),
            vm((TOK, 128), BF16),
            vm((2, WINDOW, 128), BF16),
            vm((TOK + 2 * WINDOW, 128), BF16),
            vm((NY, 80, 128), BF16),
            vm((NY, 80, 128), BF16),
            vm((2, 40, 128), BF16),
            vm((NZ, 40, 128), BF16),
            vm((NY, 64, 128), BF16),
            vm((NY, 64, 128), BF16),
            vm((NY, 8, 128), F32),
            vm((2, TOK, 128), BF16),
            vm((2, NT, TOK, 128), BF16),
            dma((11,)),
            dma((2,)),
            dma((HALF, 2)),
            dma((NZ,)),
            dma((NZ,)),
            dma((2, HALF, NY)),
            dma((2,)),
            dma((2,)),
            dma,
            dma,
            dma,
            dma,
            dma,
            dma,
            dma,
            dma,
            dma((2,)),
            dma((2, 2)),
            dma((2, 2)),
            dma((2,)),
        ],
        compiler_params=pltpu.CompilerParams(collective_id=0, has_side_effects=True),
    )(
        tokens,
        input_norm_gain[None],
        mq_weight,
        mk_weight,
        mv_weight,
        mo_weight,
        gate_weight[:, :, 0].T,
        gate_bias.T,
        decay_extra,
        m_gain[None],
        aq_weight,
        ak_weight,
        av_weight,
        sink_logit[None],
        out_m_weight,
        out_a_weight,
    )


def solution(mesh):
    split = Mesh(mesh.devices.reshape(NZ, NY, NT), ("z", "y", "tp"))
    return jax.shard_map(
        on_device,
        mesh=split,
        in_specs=(
            P(SP, None),
            P(),
            P(SP, "tp"),
            P(SP, "tp"),
            P(SP, "tp"),
            P(SP, "tp"),
            P(SP, None, "tp"),
            P(None, "tp"),
            P(None, "tp", SP),
            P("tp"),
            P(SP, "tp"),
            P(SP, "tp"),
            P(SP, "tp"),
            P("tp"),
            P(SP, "tp"),
            P(SP, "tp"),
        ),
        out_specs=(P(SP, "tp"), P("tp", SP)),
        check_vma=False,
    )
```

```python
import jax
import jax.numpy as jnp
from jax import lax
from jax.experimental import pallas as pl
from jax.experimental.pallas import tpu as pltpu
from jax.sharding import Mesh
from jax.sharding import PartitionSpec as P

M_DIM = 128
W_DIM = 64
WINDOW = 128
EPS = 1e-06
FLOOR_LOG = -1e30
NZ = 16
NY = 4
NX = 4
NT = 8
TOK = 256
D = 2048
HALF = NZ // 2
A_ROWS = 160
B_ROWS = 104
SP = ("z", "y")
MESH = pl.DeviceIdType.MESH
F32 = jnp.float32
BF16 = jnp.bfloat16
ACROSS = (((1,), (1,)), ((), ()))


def mod(a, n):
    return lax.rem(a + n, n)


def remote(src, dst, ssem, rsem, **where):
    return pltpu.make_async_remote_copy(
        src_ref=src,
        dst_ref=dst,
        send_sem=ssem,
        recv_sem=rsem,
        device_id=where,
        device_id_type=MESH,
    )


def log1p_of(e):
    poly = e * (
        1.0
        + e * (-0.5 + e * (1 / 3 + e * (-0.25 + e * (0.2 + e * (-1 / 6 + e * (1 / 7))))))
    )
    return jnp.where(e < 0.0625, poly, jnp.log(1.0 + e))


def log_sigmoid(x):
    return jnp.minimum(x, 0.0) - log1p_of(jnp.exp(-jnp.abs(x)))


def split3(x):
    hi = x.astype(BF16).astype(F32)
    mid = (x - hi).astype(BF16).astype(F32)
    return hi, mid, x - hi - mid


def joined(tail, at):
    return tail[at : at + 1] + tail[at + 1 : at + 2] + tail[at + 2 : at + 3]


def step_state(state, piece):
    peak, mat, norm = state
    p_peak, p_decay, p_mat, p_norm = piece
    new = jnp.maximum(peak + p_decay, p_peak)
    old_s, new_s = jnp.exp(peak + p_decay - new), jnp.exp(p_peak - new)
    return new, mat * old_s + p_mat * new_s, norm * old_s + p_norm * new_s


def empty_state():
    return (
        jnp.full((1, 128), FLOOR_LOG, F32),
        jnp.zeros((32, 128), F32),
        jnp.zeros((1, 128), F32),
    )


def layer_body(
    tok_hbm,
    gain_hbm,
    mq,
    mk,
    mv,
    mo,
    gate_hbm,
    bias_hbm,
    decay_hbm,
    mgain_hbm,
    aq_w,
    ak_hbm,
    av_hbm,
    sink_hbm,
    om,
    oa,
    out,
    logs,
    gain,
    gate_t,
    bias,
    decay,
    mgain,
    ak_w,
    av_w,
    sink,
    tok,
    wa,
    wb,
    ga,
    gb,
    normed,
    tri,
    acc_a,
    acc_b,
    kv,
    halo,
    win,
    pk,
    p1,
    zp,
    p2,
    p3,
    st,
    keep,
    mixes,
    full,
    local_sem,
    ssem,
    az,
    ay,
    ah,
    bz,
    by,
    bh,
    s1,
    r1,
    s2,
    r2,
    s3,
    r3,
    sh,
    rh,
    hs,
    hx,
    hh,
    hc,
):
    z = lax.axis_index("z")
    y = lax.axis_index("y")
    t = lax.axis_index("tp")
    me = z * NY + y
    zu, zd = mod(z + 1, NZ), mod(z - 1, NZ)
    yu, yd = mod(y + 1, NY), mod(y - 1, NY)
    yo = mod(y + 2, NY)
    nxt, prv = mod(me + 1, NZ * NY), mod(me - 1, NZ * NY)
    zn, yn = lax.div(nxt, NY), lax.rem(nxt, NY)
    zq, yq = lax.div(prv, NY), lax.rem(prv, NY)
    x, c = lax.div(t, 2), lax.rem(t, 2)
    o = 1 - c
    xu, xd, xo = mod(x + 1, NX), mod(x - 1, NX), mod(x + 2, NX)
    partner, t_up, t_down, t_far = 2 * x + o, 2 * xu + c, 2 * xd + c, 2 * xo + c

    barrier = pltpu.get_barrier_semaphore()
    hello = [{"z": zu}, {"z": zd}, {"y": yu}, {"y": yd}, {"y": yo}]
    hello += [{"z": zn, "y": yn}, {"z": zq, "y": yq}]
    hello += [{"tp": partner}, {"tp": t_up}, {"tp": t_down}, {"tp": t_far}]
    hello += [{"tp": 2 * xu + o}, {"tp": 2 * xd + o}]
    for where in hello:
        pl.semaphore_signal(barrier, inc=1, device_id=where, device_id_type=MESH)
    loads = []

    def load(src, dst):
        copy = pltpu.make_async_copy(src, dst, local_sem.at[2 + len(loads)])
        copy.start()
        loads.append(copy)
        return copy

    early = [load(ak_hbm, ak_w), load(av_hbm, av_w), load(gate_hbm, gate_t)]
    for i, w in enumerate((mk, mv)):
        pltpu.make_async_copy(w, wb.at[32 * i : 32 * i + 32], local_sem.at[0]).start()
    for i, w in enumerate((mq, mo, aq_w)):
        pltpu.make_async_copy(w, wa.at[32 * i : 32 * i + 32], local_sem.at[1]).start()
    for i, w in enumerate((om, oa)):
        for part in (0, 1):
            at = 96 + 32 * i + 16 * part
            src = w.at[:, 128 * part : 128 * part + 128]
            pltpu.make_async_copy(src, wa.at[at : at + 16], local_sem.at[1]).start()
    late = [load(tok_hbm, tok), load(gain_hbm, gain), load(bias_hbm, bias)]
    late += [load(decay_hbm, decay), load(mgain_hbm, mgain), load(sink_hbm, sink)]
    for copy in early:
        copy.wait()
    wb[64:96] = jnp.concatenate([ak_w[...], av_w[...]], axis=1)
    gate_rows = jnp.concatenate([gate_t[...].astype(F32), jnp.zeros((4, 96), F32)], axis=1)
    gate_row = gate_rows[0:1]
    for g in range(1, 4):
        gate_row = gate_row + pltpu.roll(gate_rows[g : g + 1], 32 * g, 1)
    wb[96:104] = jnp.concatenate([gate_row, jnp.zeros((7, 128), F32)], axis=0).astype(BF16)
    two_weights = wb.at[0:64]
    pltpu.make_async_copy(two_weights, two_weights, local_sem.at[0]).wait()
    pltpu.make_async_copy(wa, wa, local_sem.at[1]).wait()
    pl.semaphore_wait(barrier, len(hello))

    sa, sb = ssem.at[0], ssem.at[1]

    parts = (pl.ds(0, A_ROWS // 2), pl.ds(A_ROWS // 2, A_ROWS // 2))

    def a_up(ref, slot, s, h):
        return remote(ref.at[parts[h]], ga.at[slot, parts[h]], sa, az.at[s - 1, h], z=zu)

    def a_down(ref, slot, s, h):
        return remote(ref.at[parts[h]], ga.at[slot, parts[h]], sa, az.at[s - 1, h], z=zd)

    def a_side(src, zz):
        slot = zz * NY + y
        remote(src, ga.at[slot], sa, ay.at[zz], y=yu).start()
        remote(src, ga.at[slot], sa, ay.at[zz], y=yd).start()

    def b_up(src, slot, s, j):
        return remote(src, gb.at[slot], sb, bz.at[0, s - 1, j], z=zu)

    def b_down(src, slot, s, j):
        return remote(src, gb.at[slot], sb, bz.at[1, s - 1, j], z=zd)

    remote(wb, gb.at[me], sb, bh.at[0], y=yo).start()
    remote(wb, gb.at[me], sb, by.at[0], y=yu).start()
    remote(wb, gb.at[me], sb, by.at[1], y=yd).start()
    b_up(wb, me, 1, y).start()
    b_down(wb, me, 1, y).start()
    def a_first():
        for h in (0, 1):
            a_up(wa, me, 1, h).start()
            a_down(wa, me, 1, h).start()

    a_first()
    ga[me] = wa[...]
    gb[me] = wb[...]

    for copy in late:
        copy.wait()
    xs = tok[...].astype(F32)
    xs = xs * lax.rsqrt(jnp.mean(xs * xs, axis=-1, keepdims=True) + EPS) * gain[...]
    for i in range(NZ):
        normed[i] = xs[:, 128 * i : 128 * i + 128].astype(BF16)
    acc_a[...] = jnp.zeros_like(acc_a)
    acc_b[...] = jnp.zeros_like(acc_b)
    down_at = lax.broadcasted_iota(jnp.int32, (TOK, 2 * TOK), 0)
    across_at = lax.broadcasted_iota(jnp.int32, (TOK, 2 * TOK), 1)
    upper = (across_at < TOK) & (down_at <= across_at)
    lower = (across_at >= TOK) & (down_at >= across_at - TOK)
    tri[...] = jnp.where(upper | lower, 1.0, 0.0).astype(BF16)

    slot_d, slot_u, slot_o = z * NY + yd, z * NY + yu, z * NY + yo
    lo, hi = pl.ds(0, A_ROWS // 2), pl.ds(A_ROWS // 2, A_ROWS // 2)
    remote(wb, gb.at[slot_d], sb, by.at[0], y=yd).wait_recv()
    b_up(gb.at[slot_d], slot_d, 1, yd).start()
    b_down(gb.at[slot_d], slot_d, 1, yd).start()
    remote(wb, gb.at[slot_u], sb, by.at[1], y=yd).wait_recv()
    b_up(gb.at[slot_u], slot_u, 1, yu).start()
    b_down(gb.at[slot_u], slot_u, 1, yu).start()
    a_side(wa, z)

    def opposite():
        remote(wb, gb.at[slot_o], sb, bh.at[0], y=yd).wait_recv()
        b_up(gb.at[slot_o], slot_o, 1, yo).start()
        b_down(gb.at[slot_o], slot_o, 1, yo).start()

    def side_forward(zz):
        sd, su = zz * NY + yd, zz * NY + yu
        two_blocks = ga.at[pl.ds(0, 2)]
        remote(two_blocks, two_blocks, sa, ay.at[zz], y=yd).wait_recv()
        remote(ga.at[sd, lo], ga.at[sd, lo], sa, ah.at[zz], y=yu).start()
        remote(ga.at[su, hi], ga.at[su, hi], sa, ah.at[zz], y=yd).start()

    spread = lax.broadcasted_iota(jnp.int32, (32, 128), 0) == lax.rem(
        lax.broadcasted_iota(jnp.int32, (32, 128), 1), 32
    )

    def stacked(ref, zz, at):
        return jnp.concatenate([ref[zz * NY + j, at : at + 32] for j in range(NY)], axis=0)

    def level_a(zz):
        so = zz * NY + yo
        remote(ga.at[so], ga.at[so], sa, ah.at[zz], y=yd).wait_recv()
        rows = normed[zz]
        w = jnp.concatenate([stacked(ga, zz, 0), stacked(ga, zz, 32)], axis=1)
        acc_a[:, 0:256] += jnp.dot(rows, w, preferred_element_type=F32)
        acc_a[:, 256:384] += jnp.dot(rows, stacked(ga, zz, 64), preferred_element_type=F32)

    def level_b(zz):
        rows = normed[zz]
        w = jnp.concatenate([stacked(gb, zz, 0), stacked(gb, zz, 32)], axis=1)
        acc_b[:, 0:256] += jnp.dot(rows, w, preferred_element_type=F32)
        g = jnp.concatenate(
            [
                jnp.where(
                    spread, gb[zz * NY + j, 96:104].astype(F32)[0:1], 0.0
                ).astype(BF16)
                for j in range(NY)
            ],
            axis=0,
        )
        w = jnp.concatenate([stacked(gb, zz, 64), g], axis=1)
        acc_b[:, 256:512] += jnp.dot(rows, w, preferred_element_type=F32)

    def both(d, what):
        what(mod(z - d, NZ))

        @pl.when((d > 0) & (d < HALF))
        def _():
            what(mod(z + d, NZ))

    def b_step(s, j, far_up):
        sl, sl2 = mod(z - s, NZ) * NY + j, mod(z + s, NZ) * NY + j
        up_from, down_from = (HALF, HALF - 1) if far_up else (HALF - 1, HALF)

        @pl.when(s <= up_from)
        def _():
            b_up(gb.at[sl], sl, s, j).wait_recv()

            @pl.when(s < up_from)
            def _():
                b_up(gb.at[sl], sl, s + 1, j).start()

        @pl.when(s <= down_from)
        def _():
            b_down(gb.at[sl2], sl2, s, j).wait_recv()

            @pl.when(s < down_from)
            def _():
                b_down(gb.at[sl2], sl2, s + 1, j).start()

    def a_step(s):
        s = jnp.int32(s)
        z_lo, z_hi = mod(z - s, NZ), mod(z + s, NZ)
        slot, slot2 = z_lo * NY + y, z_hi * NY + y
        for h in (0, 1):

            @pl.when(s < HALF)
            def _():
                two_halves = ga.at[slot]
                remote(two_halves, two_halves, sa, az.at[s - 1, h], z=zu).wait_recv()
                a_up(ga.at[slot], slot, s + 1, h).start()

                @pl.when(s < HALF - 1)
                def _():
                    a_down(ga.at[slot2], slot2, s + 1, h).start()

            @pl.when(s == HALF)
            def _():
                a_up(ga.at[slot], slot, s, h).wait_recv()

        a_side(ga.at[slot], z_lo)

        @pl.when(s < HALF)
        def _():
            a_side(ga.at[slot2], z_hi)

    def above(d, what):
        @pl.when(d > 0)
        def _():
            what(mod(z + d, NZ))

    b_step(1, y, True)
    opposite()
    a_step(1)
    b_step(1, yd, True)
    b_step(1, yu, False)

    def step(s, carry):
        b_step(s - 1, yo, False)
        b_step(s, y, True)
        level_b(mod(z - s + 2, NZ))
        a_step(s)
        above(s - 2, level_b)
        b_step(s, yd, True)

        @pl.when(s >= 4)
        def _():
            level_a(mod(z - s + 4, NZ))

        b_step(s, yu, False)
        both(s - 2, side_forward)
        above(s - 4, level_a)
        return carry

    lax.fori_loop(2, HALF, step, 0)
    b_step(HALF - 1, yo, False)
    b_step(HALF, y, True)
    both(HALF - 2, level_b)
    b_step(HALF, yd, True)
    b_step(HALF, yu, False)
    both(HALF - 2, side_forward)
    both(HALF - 1, level_b)
    b_step(HALF, yo, False)
    level_b(mod(z - HALF, NZ))

    kv[...] = acc_b[:, 256:384].astype(BF16)
    first, last = pl.ds(0, WINDOW), pl.ds(TOK - WINDOW, WINDOW)
    to_next = remote(kv.at[last], halo.at[0], sh, rh, z=zn, y=yn)
    to_prev = remote(kv.at[first], halo.at[1], sh, rh, z=zq, y=yq)
    gt = jnp.sum(jnp.transpose(acc_b[:, 384:512]).reshape(4, 32, TOK), axis=1)
    in_f, in_b = gt[0:1] + bias[0:1, 0:1], gt[2:3] + bias[0:1, 2:3]
    lf_f = log_sigmoid(gt[1:2] + bias[0:1, 1:2]) + decay[0]
    lf_b = log_sigmoid(gt[3:4] + bias[0:1, 3:4]) + decay[1]
    to_next.start()
    to_prev.start()
    lane = lax.broadcasted_iota(jnp.int32, (1, TOK), 1)
    terms = jnp.concatenate([*split3(lf_f), *split3(lf_b), jnp.zeros((2, TOK), F32)], axis=0)
    sums = jnp.dot(terms.astype(BF16), tri[...], preferred_element_type=F32)
    cum = joined(sums[:, 0:TOK], 0)
    rev = joined(sums[:, TOK:], 3)
    tot_f = jnp.max(jnp.where(lane == TOK - 1, cum, -jnp.inf), axis=1, keepdims=True)
    tot_b = jnp.max(jnp.where(lane == 0, rev, -jnp.inf), axis=1, keepdims=True)
    end_f = tot_f - cum + in_f
    end_b = tot_b - rev + in_b
    m_f = jnp.max(end_f, axis=1, keepdims=True)
    m_b = jnp.max(end_b, axis=1, keepdims=True)
    w_f, w_b = jnp.exp(end_f - m_f), jnp.exp(end_b - m_b)
    rows = jnp.concatenate([in_f, cum, in_b, rev, w_f, w_b, jnp.zeros((2, TOK), F32)], axis=0)
    cols = jnp.transpose(jnp.concatenate([rows, jnp.zeros((120, TOK), F32)], axis=0))
    key, value = acc_b[:, 0:128].astype(BF16), acc_b[:, 128:256].astype(BF16)
    val = value.astype(F32)
    tail, mats = [], []
    norms = jnp.dot(rows.astype(BF16), key, preferred_element_type=F32)
    for i in (4, 5):
        wv = (cols[:, i : i + 1] * val).astype(BF16)
        mats.append(
            lax.dot_general(key, wv, (((0,), (0,)), ((), ())), preferred_element_type=F32)
        )
        tail.append(norms[i : i + 1])
    for v in (m_f, tot_f, m_b, tot_b):
        tail.extend(jnp.broadcast_to(p, (1, 128)) for p in split3(v))
    tail.append(jnp.zeros((2, 128), F32))
    summary_tail = jnp.concatenate(tail, axis=0).astype(BF16)
    for q in range(NY):
        pk[q, 0:32] = mats[0][q * 32 : q * 32 + 32].astype(BF16)
        pk[q, 32:64] = mats[1][q * 32 : q * 32 + 32].astype(BF16)
        pk[q, 64:80] = summary_tail

    for d in (2, 1, 3):
        j = mod(y + d, NY)
        remote(pk.at[j], p1.at[y], s1, r1, y=j).start()
    p1[y] = pk[y]

    a_step(HALF)
    both(HALF - 4, level_a)
    both(HALF - 1, side_forward)
    both(HALF - 3, level_a)

    others_y, others_z = pl.ds(0, NY - 1), pl.ds(0, NZ - 1)
    remote(pk.at[others_y], p1.at[others_y], s1, r1, y=yd).wait_recv()

    def local_piece(j, back):
        ends = p1[j, 64:80].astype(F32)
        if back:
            return joined(ends, 8), joined(ends, 11), p1[j, 32:64].astype(F32), ends[1:2]
        return joined(ends, 2), joined(ends, 5), p1[j, 0:32].astype(F32), ends[0:1]

    for back in (0, 1):
        state, total_decay = empty_state(), jnp.zeros((1, 128), F32)
        for j in reversed(range(NY)) if back else range(NY):
            piece = local_piece(j, back)
            state = step_state(state, piece)
            total_decay = total_decay + piece[1]
        zp[back, 0:32] = state[1].astype(BF16)
        zp[back, 32:40] = jnp.concatenate(
            [state[2], *split3(state[0]), *split3(total_decay), jnp.zeros((1, 128), F32)],
            axis=0,
        ).astype(BF16)
    for d in (8, 7, 9, 6, 10, 5, 11, 4, 12, 3, 13, 2, 14, 1, 15):
        remote(
            zp.at[lax.div(z + d, NZ)],
            p2.at[z],
            s2,
            r2,
            z=mod(z + d, NZ),
        ).start()

    side_forward(mod(z - HALF, NZ))
    both(HALF - 2, level_a)
    both(HALF - 1, level_a)
    level_a(mod(z - HALF, NZ))
    query = acc_a[:, 0:128].astype(BF16)
    gate_in = acc_a[:, 128:256].astype(BF16)
    a_query = acc_a[:, 256:384].astype(BF16).astype(F32)

    mid, end = pl.ds(0, TOK // 2), pl.ds(TOK // 2, TOK // 2)

    def heads_start(i):
        mix, dst = mixes.at[i], full.at[i]
        for n, part in enumerate((mid, end)):
            remote(mix.at[part], dst.at[t, part], hs.at[i], hh.at[i, n], tp=t_far).start()
        remote(mix, dst.at[t], hs.at[i], hx.at[i, 0], tp=t_up).start()
        remote(mix, dst.at[t], hs.at[i], hx.at[i, 1], tp=t_down).start()
        remote(mix, dst.at[t], hs.at[i], hc.at[i], tp=2 * xu + o).start()
        remote(mix, dst.at[t], hs.at[i], hc.at[i], tp=2 * xd + o).start()
        remote(mix, dst.at[t], hs.at[i], hc.at[i], tp=partner).start()
        full[i, t] = mixes[i]

    def heads_end(i):
        mix, dst = mixes.at[i], full.at[i]
        for n, part in enumerate((mid, end)):
            src = dst.at[t_far, part]
            remote(src, src, hs.at[i], hh.at[i, n], tp=t_up).wait_recv()
            remote(src, src, hs.at[i], hc.at[i], tp=partner).start()
        for n, slot in enumerate((t_down, t_up)):
            remote(mix, dst.at[slot], hs.at[i], hx.at[i, n], tp=t_up).wait_recv()
        half = pl.ds(0, NT // 2)
        remote(dst.at[half], dst.at[half], hs.at[i], hc.at[i], tp=partner).wait_recv()

    def heads_product(i):
        total = None
        for n in range(NT):
            w = jnp.concatenate(
                [
                    ga[8 * n : 8 * n + 8, at : at + 16].reshape(128, 128)
                    for at in (96 + 32 * i, 112 + 32 * i)
                ],
                axis=1,
            )
            term = jnp.dot(full[i, n], w, preferred_element_type=F32)
            total = term if total is None else total + term
        return total

    remote(halo, halo, sh, rh, y=yd).wait_recv()
    win[0:WINDOW] = halo[0]
    win[WINDOW : WINDOW + TOK] = kv[...]
    win[WINDOW + TOK :] = halo[1]
    low = lax.broadcasted_iota(jnp.int32, (WINDOW, 128), 1) < W_DIM
    two = lax.broadcasted_iota(jnp.int32, (2 * WINDOW, 3 * WINDOW), 0)
    col = lax.broadcasted_iota(jnp.int32, (2 * WINDOW, 3 * WINDOW), 1)
    off = col - jnp.where(two >= WINDOW, two - WINDOW, two)
    in_window = (off >= 0) & (off <= 2 * WINDOW)
    second = lax.broadcasted_iota(jnp.int32, (2 * WINDOW, 1), 0) >= WINDOW
    sink_col = jnp.where(second, sink[0:1, 1:2], sink[0:1, 0:1])
    for b in range(2):
        block = pl.ds(b * WINDOW, WINDOW)
        qb = a_query[b * WINDOW : b * WINDOW + WINDOW]
        q0 = jnp.where(low, qb, 0.0)
        q1 = jnp.where(low, pltpu.roll(qb, W_DIM, 1), 0.0)
        qq = jnp.concatenate([q0, q1], axis=0).astype(BF16)
        keys = win[b * WINDOW : b * WINDOW + 3 * WINDOW]
        scores = lax.dot_general(qq, keys, ACROSS, preferred_element_type=F32) * W_DIM**-0.5
        place = me * TOK + (b - 1) * WINDOW + col
        usable = in_window & (place >= 0) & (place < NZ * NY * TOK)
        scores = jnp.where(usable, scores, -jnp.inf)
        peak = jnp.maximum(sink_col, jnp.max(scores, axis=1, keepdims=True))
        weights = jnp.exp(scores - peak)
        tot = jnp.exp(sink_col - peak) + jnp.sum(weights, axis=1, keepdims=True)
        res = jnp.dot(weights.astype(BF16), keys, preferred_element_type=F32) / tot
        mixes[1, block] = jnp.where(
            low, pltpu.roll(res[0:WINDOW], W_DIM, 1), res[WINDOW:]
        ).astype(BF16)
        logt = jnp.transpose(jnp.broadcast_to(peak + jnp.log(tot), (2 * WINDOW, 128)))
        logs[0:1, block] = logt[0:1, 0:WINDOW]
        logs[1:2, block] = logt[0:1, WINDOW:]
    heads_start(1)
    gate_open = 1.0 / (1.0 + jnp.exp(-gate_in.astype(F32)))

    scale = M_DIM**-0.5
    dots = lax.dot_general(query, key, ACROSS, preferred_element_type=F32) * scale
    ti = lax.broadcasted_iota(jnp.int32, (TOK, TOK), 0)
    si = lax.broadcasted_iota(jnp.int32, (TOK, TOK), 1)
    inside = []
    for back in (0, 1):
        cum_t = cols[:, 2 * back + 1 : 2 * back + 2]
        log_in = rows[2 * back : 2 * back + 1] - rows[2 * back + 1 : 2 * back + 2]
        usable = (si >= ti) if back else (si <= ti)
        log_w = jnp.where(usable, cum_t + log_in, -jnp.inf)
        top = jnp.max(log_w, axis=1, keepdims=True)
        scores = dots * jnp.exp(log_w - top)
        numer = jnp.dot(scores.astype(BF16), value, preferred_element_type=F32)
        denom = jnp.sum(scores, axis=1, keepdims=True)
        inside.append((cum_t, top, numer, denom))


    remote(p2.at[others_z], p2.at[others_z], s2, r2, z=zd).wait_recv()

    def far(i, state):
        ends = p2[i, 32:40].astype(F32)
        return step_state(
            state, (joined(ends, 1), joined(ends, 4), p2[i, 0:32].astype(F32), ends[0:1])
        )

    fwd = lax.fori_loop(0, z, far, empty_state())
    bwd = lax.fori_loop(0, NZ - 1 - z, lambda i, s: far(NZ - 1 - i, s), empty_state())
    for j in range(NY):
        p3[j, 0:32] = fwd[1].astype(BF16)
        keep[j, 0:1] = fwd[2]
        keep[j, 2:3] = fwd[0]
        fwd = step_state(fwd, local_piece(j, 0))
    for j in reversed(range(NY)):
        p3[j, 32:64] = bwd[1].astype(BF16)
        keep[j, 1:2] = bwd[2]
        keep[j, 3:4] = bwd[0]
        bwd = step_state(bwd, local_piece(j, 1))
    for d in (2, 1, 3):
        j = mod(y + d, NY)
        remote(p3.at[j], st.at[y], s3, r3, y=j).start()
    st[y] = p3[y]
    nm = keep[y]
    qf = query.astype(F32) * scale
    remote(p3.at[others_y], st.at[others_y], s3, r3, y=yd).wait_recv()

    cell = None
    for back in (0, 1):
        cum_t, top_in, numer, denom = inside[back]
        inter = cum_t + nm[2 + back : 3 + back, 0:1]
        top = jnp.maximum(inter, top_in)
        w_in, w_inter = jnp.exp(top_in - top), jnp.exp(inter - top)
        mat = st[:, 32 * back : 32 * back + 32].reshape(128, 128)
        numer = w_in * numer + (w_inter * scale) * jnp.dot(
            query, mat, preferred_element_type=F32
        )
        denom = w_in * denom + w_inter * jnp.sum(
            qf * nm[back : back + 1], axis=1, keepdims=True
        )
        part = numer / jnp.maximum(jnp.abs(denom), jnp.exp(-top))
        cell = part if cell is None else cell + part
    u = cell * gate_open
    norm = lax.rsqrt(jnp.mean(u * u, axis=1, keepdims=True) + EPS)
    mixes[0] = (u * norm * mgain[...]).astype(BF16)
    heads_start(0)
    heads_end(1)
    acc_b[:, 0:256] = heads_product(1)
    heads_end(0)
    out[...] = (acc_b[:, 0:256] + heads_product(0)).astype(BF16)

    n = NZ * NY - 1
    every = pl.ds(0, n)
    remote(ga.at[every], ga.at[every], sa, ah.at[0], y=yd).wait_send()
    remote(gb.at[every], gb.at[every], sb, ah.at[0], y=yd).wait_send()
    remote(pk.at[others_y], p1.at[others_y], s1, r1, y=yd).wait_send()
    remote(p3.at[others_y], st.at[others_y], s3, r3, y=yd).wait_send()
    remote(p2.at[others_z], p2.at[others_z], s2, r2, z=zd).wait_send()
    remote(halo, halo, sh, rh, y=yd).wait_send()
    most = pl.ds(0, NT - 1)
    for i in (0, 1):
        src = full.at[i, most]
        remote(src, src, hs.at[i], hc.at[i], tp=partner).wait_send()


def on_device(
    tokens,
    input_norm_gain,
    mq_weight,
    mk_weight,
    mv_weight,
    mo_weight,
    gate_weight,
    gate_bias,
    decay_extra,
    m_gain,
    aq_weight,
    ak_weight,
    av_weight,
    sink_logit,
    out_m_weight,
    out_a_weight,
):
    sds = jax.ShapeDtypeStruct
    dma = pltpu.SemaphoreType.DMA
    vm = pltpu.VMEM
    hbm = pl.BlockSpec(memory_space=pl.ANY)
    local = pl.BlockSpec(memory_space=pltpu.VMEM)
    n = NZ * NY
    return pl.pallas_call(
        layer_body,
        name="layer",
        out_shape=(vm((TOK, 256), BF16), vm((2, TOK), F32)),
        in_specs=[hbm] * 16,
        out_specs=[local] * 2,
        scratch_shapes=[
            vm((1, D), F32),
            vm((4, 32), BF16),
            vm((1, 4), F32),
            vm((2, 1, TOK), F32),
            vm((1, 128), F32),
            vm((32, 64), BF16),
            vm((32, 64), BF16),
            vm((1, 2), F32),
            vm((TOK, D), BF16),
            vm((A_ROWS, 128), BF16),
            vm((B_ROWS, 128), BF16),
            vm((n, A_ROWS, 128), BF16),
            vm((n, B_ROWS, 128), BF16),
            vm((NZ, TOK, 128), BF16),
            vm((TOK, 2 * TOK), BF16),
            vm((TOK, 384), F32),
            vm((TOK, 512), F32),
            vm((TOK, 128), BF16),
            vm((2, WINDOW, 128), BF16),
            vm((TOK + 2 * WINDOW, 128), BF16),
            vm((NY, 80, 128), BF16),
            vm((NY, 80, 128), BF16),
            vm((2, 40, 128), BF16),
            vm((NZ, 40, 128), BF16),
            vm((NY, 64, 128), BF16),
            vm((NY, 64, 128), BF16),
            vm((NY, 8, 128), F32),
            vm((2, TOK, 128), BF16),
            vm((2, NT, TOK, 128), BF16),
            dma((11,)),
            dma((2,)),
            dma((HALF, 2)),
            dma((NZ,)),
            dma((NZ,)),
            dma((2, HALF, NY)),
            dma((2,)),
            dma((2,)),
            dma,
            dma,
            dma,
            dma,
            dma,
            dma,
            dma,
            dma,
            dma((2,)),
            dma((2, 2)),
            dma((2, 2)),
            dma((2,)),
        ],
        compiler_params=pltpu.CompilerParams(collective_id=0, has_side_effects=True),
    )(
        tokens,
        input_norm_gain[None],
        mq_weight,
        mk_weight,
        mv_weight,
        mo_weight,
        gate_weight[:, :, 0].T,
        gate_bias.T,
        decay_extra,
        m_gain[None],
        aq_weight,
        ak_weight,
        av_weight,
        sink_logit[None],
        out_m_weight,
        out_a_weight,
    )


def solution(mesh):
    split = Mesh(mesh.devices.reshape(NZ, NY, NT), ("z", "y", "tp"))
    return jax.shard_map(
        on_device,
        mesh=split,
        in_specs=(
            P(SP, None),
            P(),
            P(SP, "tp"),
            P(SP, "tp"),
            P(SP, "tp"),
            P(SP, "tp"),
            P(SP, None, "tp"),
            P(None, "tp"),
            P(None, "tp", SP),
            P("tp"),
            P(SP, "tp"),
            P(SP, "tp"),
            P(SP, "tp"),
            P("tp"),
            P(SP, "tp"),
            P(SP, "tp"),
        ),
        out_specs=(P(SP, "tp"), P("tp", SP)),
        check_vma=False,
    )
```

```python
import jax
import jax.numpy as jnp
from jax import lax
from jax.experimental import pallas as pl
from jax.experimental.pallas import tpu as pltpu
from jax.sharding import Mesh
from jax.sharding import PartitionSpec as P

M_DIM = 128
W_DIM = 64
WINDOW = 128
EPS = 1e-06
FLOOR_LOG = -1e30
NZ = 16
NY = 4
NX = 4
NT = 8
TOK = 256
D = 2048
HALF = NZ // 2
A_ROWS = 160
B_ROWS = 104
SP = ("z", "y")
MESH = pl.DeviceIdType.MESH
F32 = jnp.float32
BF16 = jnp.bfloat16
ACROSS = (((1,), (1,)), ((), ()))


def mod(a, n):
    return lax.rem(a + n, n)


def remote(src, dst, ssem, rsem, **where):
    return pltpu.make_async_remote_copy(
        src_ref=src,
        dst_ref=dst,
        send_sem=ssem,
        recv_sem=rsem,
        device_id=where,
        device_id_type=MESH,
    )


def log1p_of(e):
    poly = e * (
        1.0
        + e * (-0.5 + e * (1 / 3 + e * (-0.25 + e * (0.2 + e * (-1 / 6 + e * (1 / 7))))))
    )
    return jnp.where(e < 0.0625, poly, jnp.log(1.0 + e))


def log_sigmoid(x):
    return jnp.minimum(x, 0.0) - log1p_of(jnp.exp(-jnp.abs(x)))


def split3(x):
    hi = x.astype(BF16).astype(F32)
    mid = (x - hi).astype(BF16).astype(F32)
    return hi, mid, x - hi - mid


def joined(tail, at):
    return tail[at : at + 1] + tail[at + 1 : at + 2] + tail[at + 2 : at + 3]


def step_state(state, piece):
    peak, mat, norm = state
    p_peak, p_decay, p_mat, p_norm = piece
    new = jnp.maximum(peak + p_decay, p_peak)
    old_s, new_s = jnp.exp(peak + p_decay - new), jnp.exp(p_peak - new)
    return new, mat * old_s + p_mat * new_s, norm * old_s + p_norm * new_s


def empty_state():
    return (
        jnp.full((1, 128), FLOOR_LOG, F32),
        jnp.zeros((32, 128), F32),
        jnp.zeros((1, 128), F32),
    )


def layer_body(
    tok_hbm,
    gain_hbm,
    mq,
    mk,
    mv,
    mo,
    gate_hbm,
    bias_hbm,
    decay_hbm,
    mgain_hbm,
    aq_w,
    ak_hbm,
    av_hbm,
    sink_hbm,
    om,
    oa,
    out,
    logs,
    gain,
    gate_t,
    bias,
    decay,
    mgain,
    ak_w,
    av_w,
    sink,
    tok,
    wa,
    wb,
    ga,
    gb,
    normed,
    tri,
    acc_a,
    acc_b,
    kv,
    halo,
    win,
    pk,
    p1,
    zp,
    p2,
    p3,
    st,
    keep,
    mixes,
    full,
    local_sem,
    ssem,
    az,
    ay,
    ah,
    bz,
    by,
    bh,
    s1,
    r1,
    s2,
    r2,
    s3,
    r3,
    sh,
    rh,
    hs,
    hx,
    hh,
    hc,
):
    z = lax.axis_index("z")
    y = lax.axis_index("y")
    t = lax.axis_index("tp")
    me = z * NY + y
    zu, zd = mod(z + 1, NZ), mod(z - 1, NZ)
    yu, yd = mod(y + 1, NY), mod(y - 1, NY)
    yo = mod(y + 2, NY)
    nxt, prv = mod(me + 1, NZ * NY), mod(me - 1, NZ * NY)
    zn, yn = lax.div(nxt, NY), lax.rem(nxt, NY)
    zq, yq = lax.div(prv, NY), lax.rem(prv, NY)
    x, c = lax.div(t, 2), lax.rem(t, 2)
    o = 1 - c
    xu, xd, xo = mod(x + 1, NX), mod(x - 1, NX), mod(x + 2, NX)
    partner, t_up, t_down, t_far = 2 * x + o, 2 * xu + c, 2 * xd + c, 2 * xo + c

    barrier = pltpu.get_barrier_semaphore()
    hello = [{"z": zu}, {"z": zd}, {"y": yu}, {"y": yd}, {"y": yo}]
    hello += [{"z": zn, "y": yn}, {"z": zq, "y": yq}]
    hello += [{"tp": partner}, {"tp": t_up}, {"tp": t_down}, {"tp": t_far}]
    hello += [{"tp": 2 * xu + o}, {"tp": 2 * xd + o}]
    for where in hello:
        pl.semaphore_signal(barrier, inc=1, device_id=where, device_id_type=MESH)
    loads = []

    def load(src, dst):
        copy = pltpu.make_async_copy(src, dst, local_sem.at[2 + len(loads)])
        copy.start()
        loads.append(copy)
        return copy

    early = [load(ak_hbm, ak_w), load(av_hbm, av_w), load(gate_hbm, gate_t)]
    for i, w in enumerate((mk, mv)):
        pltpu.make_async_copy(w, wb.at[32 * i : 32 * i + 32], local_sem.at[0]).start()
    for i, w in enumerate((mq, mo, aq_w)):
        pltpu.make_async_copy(w, wa.at[32 * i : 32 * i + 32], local_sem.at[1]).start()
    for i, w in enumerate((om, oa)):
        for part in (0, 1):
            at = 96 + 32 * i + 16 * part
            src = w.at[:, 128 * part : 128 * part + 128]
            pltpu.make_async_copy(src, wa.at[at : at + 16], local_sem.at[1]).start()
    late = [load(tok_hbm, tok), load(gain_hbm, gain), load(bias_hbm, bias)]
    late += [load(decay_hbm, decay), load(mgain_hbm, mgain), load(sink_hbm, sink)]
    for copy in early:
        copy.wait()
    wb[64:96] = jnp.concatenate([ak_w[...], av_w[...]], axis=1)
    gate_rows = jnp.concatenate([gate_t[...].astype(F32), jnp.zeros((4, 96), F32)], axis=1)
    gate_row = gate_rows[0:1]
    for g in range(1, 4):
        gate_row = gate_row + pltpu.roll(gate_rows[g : g + 1], 32 * g, 1)
    wb[96:104] = jnp.concatenate([gate_row, jnp.zeros((7, 128), F32)], axis=0).astype(BF16)
    two_weights = wb.at[0:64]
    pltpu.make_async_copy(two_weights, two_weights, local_sem.at[0]).wait()
    pltpu.make_async_copy(wa, wa, local_sem.at[1]).wait()
    pl.semaphore_wait(barrier, len(hello))

    sa, sb = ssem.at[0], ssem.at[1]

    parts = (pl.ds(0, A_ROWS // 2), pl.ds(A_ROWS // 2, A_ROWS // 2))

    def a_up(ref, slot, s, h):
        return remote(ref.at[parts[h]], ga.at[slot, parts[h]], sa, az.at[s - 1, h], z=zu)

    def a_down(ref, slot, s, h):
        return remote(ref.at[parts[h]], ga.at[slot, parts[h]], sa, az.at[s - 1, h], z=zd)

    def a_side(src, zz):
        slot = zz * NY + y
        remote(src, ga.at[slot], sa, ay.at[zz], y=yu).start()
        remote(src, ga.at[slot], sa, ay.at[zz], y=yd).start()

    def b_up(src, slot, s, j):
        return remote(src, gb.at[slot], sb, bz.at[0, s - 1, j], z=zu)

    def b_down(src, slot, s, j):
        return remote(src, gb.at[slot], sb, bz.at[1, s - 1, j], z=zd)

    remote(wb, gb.at[me], sb, bh.at[0], y=yo).start()
    remote(wb, gb.at[me], sb, by.at[0], y=yu).start()
    remote(wb, gb.at[me], sb, by.at[1], y=yd).start()
    b_up(wb, me, 1, y).start()
    b_down(wb, me, 1, y).start()
    def a_first():
        for h in (0, 1):
            a_up(wa, me, 1, h).start()
            a_down(wa, me, 1, h).start()

    a_first()
    ga[me] = wa[...]
    gb[me] = wb[...]

    for copy in late:
        copy.wait()
    xs = tok[...].astype(F32)
    xs = xs * lax.rsqrt(jnp.mean(xs * xs, axis=-1, keepdims=True) + EPS) * gain[...]
    for i in range(NZ):
        normed[i] = xs[:, 128 * i : 128 * i + 128].astype(BF16)
    acc_a[...] = jnp.zeros_like(acc_a)
    acc_b[...] = jnp.zeros_like(acc_b)
    down_at = lax.broadcasted_iota(jnp.int32, (TOK, 2 * TOK), 0)
    across_at = lax.broadcasted_iota(jnp.int32, (TOK, 2 * TOK), 1)
    upper = (across_at < TOK) & (down_at <= across_at)
    lower = (across_at >= TOK) & (down_at >= across_at - TOK)
    tri[...] = jnp.where(upper | lower, 1.0, 0.0).astype(BF16)

    slot_d, slot_u, slot_o = z * NY + yd, z * NY + yu, z * NY + yo
    lo, hi = pl.ds(0, A_ROWS // 2), pl.ds(A_ROWS // 2, A_ROWS // 2)
    remote(wb, gb.at[slot_d], sb, by.at[0], y=yd).wait_recv()
    b_up(gb.at[slot_d], slot_d, 1, yd).start()
    b_down(gb.at[slot_d], slot_d, 1, yd).start()
    remote(wb, gb.at[slot_u], sb, by.at[1], y=yd).wait_recv()
    b_up(gb.at[slot_u], slot_u, 1, yu).start()
    b_down(gb.at[slot_u], slot_u, 1, yu).start()
    a_side(wa, z)

    def opposite():
        remote(wb, gb.at[slot_o], sb, bh.at[0], y=yd).wait_recv()
        b_up(gb.at[slot_o], slot_o, 1, yo).start()
        b_down(gb.at[slot_o], slot_o, 1, yo).start()

    def side_forward(zz):
        sd, su = zz * NY + yd, zz * NY + yu
        two_blocks = ga.at[pl.ds(0, 2)]
        remote(two_blocks, two_blocks, sa, ay.at[zz], y=yd).wait_recv()
        remote(ga.at[sd, lo], ga.at[sd, lo], sa, ah.at[zz], y=yu).start()
        remote(ga.at[su, hi], ga.at[su, hi], sa, ah.at[zz], y=yd).start()

    spread = lax.broadcasted_iota(jnp.int32, (32, 128), 0) == lax.rem(
        lax.broadcasted_iota(jnp.int32, (32, 128), 1), 32
    )

    def stacked(ref, zz, at):
        return jnp.concatenate([ref[zz * NY + j, at : at + 32] for j in range(NY)], axis=0)

    def level_a(zz):
        so = zz * NY + yo
        remote(ga.at[so], ga.at[so], sa, ah.at[zz], y=yd).wait_recv()
        rows = normed[zz]
        w = jnp.concatenate([stacked(ga, zz, 0), stacked(ga, zz, 32)], axis=1)
        acc_a[:, 0:256] += jnp.dot(rows, w, preferred_element_type=F32)
        acc_a[:, 256:384] += jnp.dot(rows, stacked(ga, zz, 64), preferred_element_type=F32)

    def level_b(zz):
        rows = normed[zz]
        w = jnp.concatenate([stacked(gb, zz, 0), stacked(gb, zz, 32)], axis=1)
        acc_b[:, 0:256] += jnp.dot(rows, w, preferred_element_type=F32)
        g = jnp.concatenate(
            [
                jnp.where(
                    spread, gb[zz * NY + j, 96:104].astype(F32)[0:1], 0.0
                ).astype(BF16)
                for j in range(NY)
            ],
            axis=0,
        )
        w = jnp.concatenate([stacked(gb, zz, 64), g], axis=1)
        acc_b[:, 256:512] += jnp.dot(rows, w, preferred_element_type=F32)

    def both(d, what):
        what(mod(z - d, NZ))

        @pl.when((d > 0) & (d < HALF))
        def _():
            what(mod(z + d, NZ))

    def b_step(s, j, far_up):
        sl, sl2 = mod(z - s, NZ) * NY + j, mod(z + s, NZ) * NY + j
        up_from, down_from = (HALF, HALF - 1) if far_up else (HALF - 1, HALF)

        @pl.when(s <= up_from)
        def _():
            b_up(gb.at[sl], sl, s, j).wait_recv()

            @pl.when(s < up_from)
            def _():
                b_up(gb.at[sl], sl, s + 1, j).start()

        @pl.when(s <= down_from)
        def _():
            b_down(gb.at[sl2], sl2, s, j).wait_recv()

            @pl.when(s < down_from)
            def _():
                b_down(gb.at[sl2], sl2, s + 1, j).start()

    def a_step(s):
        s = jnp.int32(s)
        z_lo, z_hi = mod(z - s, NZ), mod(z + s, NZ)
        slot, slot2 = z_lo * NY + y, z_hi * NY + y
        for h in (0, 1):

            @pl.when(s < HALF)
            def _():
                two_halves = ga.at[slot]
                remote(two_halves, two_halves, sa, az.at[s - 1, h], z=zu).wait_recv()
                a_up(ga.at[slot], slot, s + 1, h).start()

                @pl.when(s < HALF - 1)
                def _():
                    a_down(ga.at[slot2], slot2, s + 1, h).start()

            @pl.when(s == HALF)
            def _():
                a_up(ga.at[slot], slot, s, h).wait_recv()

        a_side(ga.at[slot], z_lo)

        @pl.when(s < HALF)
        def _():
            a_side(ga.at[slot2], z_hi)

    def above(d, what):
        @pl.when(d > 0)
        def _():
            what(mod(z + d, NZ))

    b_step(1, y, True)
    opposite()
    a_step(1)
    b_step(1, yd, True)
    b_step(1, yu, False)

    def step(s, carry):
        b_step(s - 1, yo, False)
        b_step(s, y, True)
        level_b(mod(z - s + 2, NZ))
        a_step(s)
        above(s - 2, level_b)
        b_step(s, yd, True)

        @pl.when(s >= 4)
        def _():
            level_a(mod(z - s + 4, NZ))

        b_step(s, yu, False)
        both(s - 2, side_forward)
        above(s - 4, level_a)
        return carry

    lax.fori_loop(2, HALF, step, 0)
    b_step(HALF - 1, yo, False)
    b_step(HALF, y, True)
    both(HALF - 2, level_b)
    b_step(HALF, yd, True)
    b_step(HALF, yu, False)
    both(HALF - 2, side_forward)
    both(HALF - 1, level_b)
    b_step(HALF, yo, False)
    level_b(mod(z - HALF, NZ))

    kv[...] = acc_b[:, 256:384].astype(BF16)
    first, last = pl.ds(0, WINDOW), pl.ds(TOK - WINDOW, WINDOW)
    to_next = remote(kv.at[last], halo.at[0], sh, rh, z=zn, y=yn)
    to_prev = remote(kv.at[first], halo.at[1], sh, rh, z=zq, y=yq)
    gt = jnp.sum(jnp.transpose(acc_b[:, 384:512]).reshape(4, 32, TOK), axis=1)
    in_f, in_b = gt[0:1] + bias[0:1, 0:1], gt[2:3] + bias[0:1, 2:3]
    lf_f = log_sigmoid(gt[1:2] + bias[0:1, 1:2]) + decay[0]
    lf_b = log_sigmoid(gt[3:4] + bias[0:1, 3:4]) + decay[1]
    to_next.start()
    to_prev.start()
    lane = lax.broadcasted_iota(jnp.int32, (1, TOK), 1)
    terms = jnp.concatenate([*split3(lf_f), *split3(lf_b), jnp.zeros((2, TOK), F32)], axis=0)
    sums = jnp.dot(terms.astype(BF16), tri[...], preferred_element_type=F32)
    cum = joined(sums[:, 0:TOK], 0)
    rev = joined(sums[:, TOK:], 3)
    tot_f = jnp.max(jnp.where(lane == TOK - 1, cum, -jnp.inf), axis=1, keepdims=True)
    tot_b = jnp.max(jnp.where(lane == 0, rev, -jnp.inf), axis=1, keepdims=True)
    end_f = tot_f - cum + in_f
    end_b = tot_b - rev + in_b
    m_f = jnp.max(end_f, axis=1, keepdims=True)
    m_b = jnp.max(end_b, axis=1, keepdims=True)
    w_f, w_b = jnp.exp(end_f - m_f), jnp.exp(end_b - m_b)
    rows = jnp.concatenate([in_f, cum, in_b, rev, w_f, w_b, jnp.zeros((2, TOK), F32)], axis=0)
    cols = jnp.transpose(jnp.concatenate([rows, jnp.zeros((120, TOK), F32)], axis=0))
    key, value = acc_b[:, 0:128].astype(BF16), acc_b[:, 128:256].astype(BF16)
    val = value.astype(F32)
    tail, mats = [], []
    norms = jnp.dot(rows.astype(BF16), key, preferred_element_type=F32)
    for i in (4, 5):
        wv = (cols[:, i : i + 1] * val).astype(BF16)
        mats.append(
            lax.dot_general(key, wv, (((0,), (0,)), ((), ())), preferred_element_type=F32)
        )
        tail.append(norms[i : i + 1])
    for v in (m_f, tot_f, m_b, tot_b):
        tail.extend(jnp.broadcast_to(p, (1, 128)) for p in split3(v))
    tail.append(jnp.zeros((2, 128), F32))
    summary_tail = jnp.concatenate(tail, axis=0).astype(BF16)
    for q in range(NY):
        pk[q, 0:32] = mats[0][q * 32 : q * 32 + 32].astype(BF16)
        pk[q, 32:64] = mats[1][q * 32 : q * 32 + 32].astype(BF16)
        pk[q, 64:80] = summary_tail

    for d in (2, 1, 3):
        j = mod(y + d, NY)
        remote(pk.at[j], p1.at[y], s1, r1, y=j).start()
    p1[y] = pk[y]

    a_step(HALF)
    both(HALF - 4, level_a)
    both(HALF - 1, side_forward)
    both(HALF - 3, level_a)

    others_y, others_z = pl.ds(0, NY - 1), pl.ds(0, NZ - 1)
    remote(pk.at[others_y], p1.at[others_y], s1, r1, y=yd).wait_recv()

    def local_piece(j, back):
        ends = p1[j, 64:80].astype(F32)
        if back:
            return joined(ends, 8), joined(ends, 11), p1[j, 32:64].astype(F32), ends[1:2]
        return joined(ends, 2), joined(ends, 5), p1[j, 0:32].astype(F32), ends[0:1]

    for back in (0, 1):
        state, total_decay = empty_state(), jnp.zeros((1, 128), F32)
        for j in reversed(range(NY)) if back else range(NY):
            piece = local_piece(j, back)
            state = step_state(state, piece)
            total_decay = total_decay + piece[1]
        zp[back, 0:32] = state[1].astype(BF16)
        zp[back, 32:40] = jnp.concatenate(
            [state[2], *split3(state[0]), *split3(total_decay), jnp.zeros((1, 128), F32)],
            axis=0,
        ).astype(BF16)
    for d in (8, 7, 9, 6, 10, 5, 11, 4, 12, 3, 13, 2, 14, 1, 15):
        remote(
            zp.at[lax.div(z + d, NZ)],
            p2.at[z],
            s2,
            r2,
            z=mod(z + d, NZ),
        ).start()

    side_forward(mod(z - HALF, NZ))
    both(HALF - 2, level_a)
    both(HALF - 1, level_a)
    level_a(mod(z - HALF, NZ))
    query = acc_a[:, 0:128].astype(BF16)
    gate_in = acc_a[:, 128:256].astype(BF16)
    a_query = acc_a[:, 256:384].astype(BF16).astype(F32)

    mid, end = pl.ds(0, TOK // 2), pl.ds(TOK // 2, TOK // 2)

    def heads_start(i):
        mix, dst = mixes.at[i], full.at[i]
        for n, part in enumerate((mid, end)):
            remote(mix.at[part], dst.at[t, part], hs.at[i], hh.at[i, n], tp=t_far).start()
        remote(mix, dst.at[t], hs.at[i], hx.at[i, 0], tp=t_up).start()
        remote(mix, dst.at[t], hs.at[i], hx.at[i, 1], tp=t_down).start()
        remote(mix, dst.at[t], hs.at[i], hc.at[i], tp=2 * xu + o).start()
        remote(mix, dst.at[t], hs.at[i], hc.at[i], tp=2 * xd + o).start()
        remote(mix, dst.at[t], hs.at[i], hc.at[i], tp=partner).start()
        full[i, t] = mixes[i]

    def heads_end(i):
        mix, dst = mixes.at[i], full.at[i]
        for n, part in enumerate((mid, end)):
            src = dst.at[t_far, part]
            remote(src, src, hs.at[i], hh.at[i, n], tp=t_up).wait_recv()
            remote(src, src, hs.at[i], hc.at[i], tp=partner).start()
        for n, slot in enumerate((t_down, t_up)):
            remote(mix, dst.at[slot], hs.at[i], hx.at[i, n], tp=t_up).wait_recv()

    def heads_other(i):
        dst = full.at[i]
        half = pl.ds(0, NT // 2)
        remote(dst.at[half], dst.at[half], hs.at[i], hc.at[i], tp=partner).wait_recv()

    def heads_product(i, slots):
        total = None
        for n in slots:
            w = jnp.concatenate(
                [
                    ga[pl.ds(8 * n, 8), at : at + 16].reshape(128, 128)
                    for at in (96 + 32 * i, 112 + 32 * i)
                ],
                axis=1,
            )
            term = jnp.dot(full[i, n], w, preferred_element_type=F32)
            total = term if total is None else total + term
        return total

    remote(halo, halo, sh, rh, y=yd).wait_recv()
    win[0:WINDOW] = halo[0]
    win[WINDOW : WINDOW + TOK] = kv[...]
    win[WINDOW + TOK :] = halo[1]
    low = lax.broadcasted_iota(jnp.int32, (WINDOW, 128), 1) < W_DIM
    two = lax.broadcasted_iota(jnp.int32, (2 * WINDOW, 3 * WINDOW), 0)
    col = lax.broadcasted_iota(jnp.int32, (2 * WINDOW, 3 * WINDOW), 1)
    off = col - jnp.where(two >= WINDOW, two - WINDOW, two)
    in_window = (off >= 0) & (off <= 2 * WINDOW)
    second = lax.broadcasted_iota(jnp.int32, (2 * WINDOW, 1), 0) >= WINDOW
    sink_col = jnp.where(second, sink[0:1, 1:2], sink[0:1, 0:1])
    for b in range(2):
        block = pl.ds(b * WINDOW, WINDOW)
        qb = a_query[b * WINDOW : b * WINDOW + WINDOW]
        q0 = jnp.where(low, qb, 0.0)
        q1 = jnp.where(low, pltpu.roll(qb, W_DIM, 1), 0.0)
        qq = jnp.concatenate([q0, q1], axis=0).astype(BF16)
        keys = win[b * WINDOW : b * WINDOW + 3 * WINDOW]
        scores = lax.dot_general(qq, keys, ACROSS, preferred_element_type=F32) * W_DIM**-0.5
        place = me * TOK + (b - 1) * WINDOW + col
        usable = in_window & (place >= 0) & (place < NZ * NY * TOK)
        scores = jnp.where(usable, scores, -jnp.inf)
        peak = jnp.maximum(sink_col, jnp.max(scores, axis=1, keepdims=True))
        weights = jnp.exp(scores - peak)
        tot = jnp.exp(sink_col - peak) + jnp.sum(weights, axis=1, keepdims=True)
        res = jnp.dot(weights.astype(BF16), keys, preferred_element_type=F32) / tot
        mixes[1, block] = jnp.where(
            low, pltpu.roll(res[0:WINDOW], W_DIM, 1), res[WINDOW:]
        ).astype(BF16)
        logt = jnp.transpose(jnp.broadcast_to(peak + jnp.log(tot), (2 * WINDOW, 128)))
        logs[0:1, block] = logt[0:1, 0:WINDOW]
        logs[1:2, block] = logt[0:1, WINDOW:]
    heads_start(1)
    gate_open = 1.0 / (1.0 + jnp.exp(-gate_in.astype(F32)))

    scale = M_DIM**-0.5
    dots = lax.dot_general(query, key, ACROSS, preferred_element_type=F32) * scale
    ti = lax.broadcasted_iota(jnp.int32, (TOK, TOK), 0)
    si = lax.broadcasted_iota(jnp.int32, (TOK, TOK), 1)
    inside = []
    for back in (0, 1):
        cum_t = cols[:, 2 * back + 1 : 2 * back + 2]
        log_in = rows[2 * back : 2 * back + 1] - rows[2 * back + 1 : 2 * back + 2]
        usable = (si >= ti) if back else (si <= ti)
        log_w = jnp.where(usable, cum_t + log_in, -jnp.inf)
        top = jnp.max(log_w, axis=1, keepdims=True)
        scores = dots * jnp.exp(log_w - top)
        numer = jnp.dot(scores.astype(BF16), value, preferred_element_type=F32)
        denom = jnp.sum(scores, axis=1, keepdims=True)
        inside.append((cum_t, top, numer, denom))


    remote(p2.at[others_z], p2.at[others_z], s2, r2, z=zd).wait_recv()

    def far(i, state):
        ends = p2[i, 32:40].astype(F32)
        return step_state(
            state, (joined(ends, 1), joined(ends, 4), p2[i, 0:32].astype(F32), ends[0:1])
        )

    fwd = lax.fori_loop(0, z, far, empty_state())
    bwd = lax.fori_loop(0, NZ - 1 - z, lambda i, s: far(NZ - 1 - i, s), empty_state())
    for j in range(NY):
        p3[j, 0:32] = fwd[1].astype(BF16)
        keep[j, 0:1] = fwd[2]
        keep[j, 2:3] = fwd[0]
        fwd = step_state(fwd, local_piece(j, 0))
    for j in reversed(range(NY)):
        p3[j, 32:64] = bwd[1].astype(BF16)
        keep[j, 1:2] = bwd[2]
        keep[j, 3:4] = bwd[0]
        bwd = step_state(bwd, local_piece(j, 1))
    for d in (2, 1, 3):
        j = mod(y + d, NY)
        remote(p3.at[j], st.at[y], s3, r3, y=j).start()
    st[y] = p3[y]
    nm = keep[y]
    qf = query.astype(F32) * scale
    remote(p3.at[others_y], st.at[others_y], s3, r3, y=yd).wait_recv()

    cell = None
    for back in (0, 1):
        cum_t, top_in, numer, denom = inside[back]
        inter = cum_t + nm[2 + back : 3 + back, 0:1]
        top = jnp.maximum(inter, top_in)
        w_in, w_inter = jnp.exp(top_in - top), jnp.exp(inter - top)
        mat = st[:, 32 * back : 32 * back + 32].reshape(128, 128)
        numer = w_in * numer + (w_inter * scale) * jnp.dot(
            query, mat, preferred_element_type=F32
        )
        denom = w_in * denom + w_inter * jnp.sum(
            qf * nm[back : back + 1], axis=1, keepdims=True
        )
        part = numer / jnp.maximum(jnp.abs(denom), jnp.exp(-top))
        cell = part if cell is None else cell + part
    u = cell * gate_open
    norm = lax.rsqrt(jnp.mean(u * u, axis=1, keepdims=True) + EPS)
    mixes[0] = (u * norm * mgain[...]).astype(BF16)
    heads_start(0)
    heads_end(1)
    heads_other(1)
    acc_b[:, 0:256] = heads_product(1, range(NT))
    heads_end(0)
    mine = heads_product(0, (t, t_up, t_down, t_far)) + acc_b[:, 0:256]
    heads_other(0)
    others = (partner, 2 * xu + o, 2 * xd + o, 2 * xo + o)
    out[...] = (mine + heads_product(0, others)).astype(BF16)

    n = NZ * NY - 1
    every = pl.ds(0, n)
    remote(ga.at[every], ga.at[every], sa, ah.at[0], y=yd).wait_send()
    remote(gb.at[every], gb.at[every], sb, ah.at[0], y=yd).wait_send()
    remote(pk.at[others_y], p1.at[others_y], s1, r1, y=yd).wait_send()
    remote(p3.at[others_y], st.at[others_y], s3, r3, y=yd).wait_send()
    remote(p2.at[others_z], p2.at[others_z], s2, r2, z=zd).wait_send()
    remote(halo, halo, sh, rh, y=yd).wait_send()
    most = pl.ds(0, NT - 1)
    for i in (0, 1):
        src = full.at[i, most]
        remote(src, src, hs.at[i], hc.at[i], tp=partner).wait_send()


def on_device(
    tokens,
    input_norm_gain,
    mq_weight,
    mk_weight,
    mv_weight,
    mo_weight,
    gate_weight,
    gate_bias,
    decay_extra,
    m_gain,
    aq_weight,
    ak_weight,
    av_weight,
    sink_logit,
    out_m_weight,
    out_a_weight,
):
    sds = jax.ShapeDtypeStruct
    dma = pltpu.SemaphoreType.DMA
    vm = pltpu.VMEM
    hbm = pl.BlockSpec(memory_space=pl.ANY)
    local = pl.BlockSpec(memory_space=pltpu.VMEM)
    n = NZ * NY
    return pl.pallas_call(
        layer_body,
        name="layer",
        out_shape=(vm((TOK, 256), BF16), vm((2, TOK), F32)),
        in_specs=[hbm] * 16,
        out_specs=[local] * 2,
        scratch_shapes=[
            vm((1, D), F32),
            vm((4, 32), BF16),
            vm((1, 4), F32),
            vm((2, 1, TOK), F32),
            vm((1, 128), F32),
            vm((32, 64), BF16),
            vm((32, 64), BF16),
            vm((1, 2), F32),
            vm((TOK, D), BF16),
            vm((A_ROWS, 128), BF16),
            vm((B_ROWS, 128), BF16),
            vm((n, A_ROWS, 128), BF16),
            vm((n, B_ROWS, 128), BF16),
            vm((NZ, TOK, 128), BF16),
            vm((TOK, 2 * TOK), BF16),
            vm((TOK, 384), F32),
            vm((TOK, 512), F32),
            vm((TOK, 128), BF16),
            vm((2, WINDOW, 128), BF16),
            vm((TOK + 2 * WINDOW, 128), BF16),
            vm((NY, 80, 128), BF16),
            vm((NY, 80, 128), BF16),
            vm((2, 40, 128), BF16),
            vm((NZ, 40, 128), BF16),
            vm((NY, 64, 128), BF16),
            vm((NY, 64, 128), BF16),
            vm((NY, 8, 128), F32),
            vm((2, TOK, 128), BF16),
            vm((2, NT, TOK, 128), BF16),
            dma((11,)),
            dma((2,)),
            dma((HALF, 2)),
            dma((NZ,)),
            dma((NZ,)),
            dma((2, HALF, NY)),
            dma((2,)),
            dma((2,)),
            dma,
            dma,
            dma,
            dma,
            dma,
            dma,
            dma,
            dma,
            dma((2,)),
            dma((2, 2)),
            dma((2, 2)),
            dma((2,)),
        ],
        compiler_params=pltpu.CompilerParams(collective_id=0, has_side_effects=True),
    )(
        tokens,
        input_norm_gain[None],
        mq_weight,
        mk_weight,
        mv_weight,
        mo_weight,
        gate_weight[:, :, 0].T,
        gate_bias.T,
        decay_extra,
        m_gain[None],
        aq_weight,
        ak_weight,
        av_weight,
        sink_logit[None],
        out_m_weight,
        out_a_weight,
    )


def solution(mesh):
    split = Mesh(mesh.devices.reshape(NZ, NY, NT), ("z", "y", "tp"))
    return jax.shard_map(
        on_device,
        mesh=split,
        in_specs=(
            P(SP, None),
            P(),
            P(SP, "tp"),
            P(SP, "tp"),
            P(SP, "tp"),
            P(SP, "tp"),
            P(SP, None, "tp"),
            P(None, "tp"),
            P(None, "tp", SP),
            P("tp"),
            P(SP, "tp"),
            P(SP, "tp"),
            P(SP, "tp"),
            P("tp"),
            P(SP, "tp"),
            P(SP, "tp"),
        ),
        out_specs=(P(SP, "tp"), P("tp", SP)),
        check_vma=False,
    )
```
